256 devices in a mesh: sp: 32 (over z, x), tp: 8 (over y, core).
Axes of the slice: x: 4, y: 4, z: 8, core: 2. Of those that a mesh axis runs over, the one named last changes fastest.
Arguments:
- inputs: bfloat16 [32768, 2048], P('sp'), may hold values from -6 to 6
- w_query: bfloat16 [2048, 2048], P(None, 'tp'), may hold values from -0.125 to 0.125
- w_key: bfloat16 [2048, 2048], P(None, 'tp'), may hold values from -0.125 to 0.125
- w_value: bfloat16 [2048, 2048], P(None, 'tp'), may hold values from -0.125 to 0.125
- rel_table: float32 [16, 257], P('tp'), may hold values from -4 to 254
- out_grad: bfloat16 [32768, 2048], P('sp', 'tp'), may hold values from -6 to 6
Outputs:
- query_grad: bfloat16 [32768, 2048], P('sp', 'tp')
- key_grad: bfloat16 [32768, 2048], P('sp', 'tp')
- value_grad: bfloat16 [32768, 2048], P('sp', 'tp')
- query_weight_grad: float32 [2048, 2048], P('sp', 'tp')
- key_weight_grad: float32 [2048, 2048], P('sp', 'tp')
- value_weight_grad: float32 [2048, 2048], P('sp', 'tp')
- table_grad: float32 [16, 257], P('tp')
The draws below stay inside these ranges and needn't reach their ends.
All inputs are finite; a program needn't handle non-finite values.
Results may differ from the reference program's by a relative error of at most 0.017.
The reference program's roundings to bfloat16 on the way count: a program that leaves them out, or rounds other values in their place, can miss the bound.
Values may be sent and summed in bfloat16 or wider, within the bound.
No kernel may reach another device: no remote copies, remote signals or barrier semaphores. Data moves between devices by JAX's collectives and lax.ppermute only.
A program may use at most 128 MiB of HBM per device.

```python
import jax
import jax.numpy as jnp
from jax import lax

HEADS = 16
HDIM = 128
D = 2048
SEG = 64
PREV = 4
MAXREL = 128
TOKENS = 32768


def draw_rel_table(key, part):
    base_key = jax.random.fold_in(jax.random.fold_in(key, 7), 0)
    bias_table = jnp.clip(jax.random.normal(base_key, (HEADS, 2 * MAXREL + 1), jnp.float32), -4.0, 4.0)
    return bias_table


def strengthened(drawn, own_key, source, target, parts, factor):
    owner, partner = [(jnp.arange(drawn.shape[axis_at]) // (drawn.shape[axis_at] // parts)).reshape([-1 if axis == axis_at else 1 for axis in range(drawn.ndim)]) for axis_at in (source, target)]
    chosen = jax.random.permutation(own_key, parts)[partner]
    strong = (owner == chosen) | (owner == (partner + parts // 2) % parts)
    return jnp.where(strong, factor * drawn, drawn)


def block_scale(rng, extent, pieces, least, high):
    factor_of = 1.0
    for dim, parts in pieces:
        steps = jax.random.uniform(jax.random.fold_in(jax.random.fold_in(rng, 6), dim), (parts,), jnp.float32, least / len(pieces), high / len(pieces))
        factor_of = factor_of * jnp.repeat(jnp.exp(steps), extent[dim] // parts).reshape((-1,) + (1,) * (len(extent) - 1 - dim))
    return factor_of


def normal_values(key, shape, spread, most, cuts=(), kind=jnp.bfloat16):
    values = spread * jax.random.normal(key, shape, jnp.float32)
    if cuts:
        values = values * block_scale(key, shape, cuts, -0.22, 0.18)
    return jnp.clip(values, -most, most).astype(kind)


def bell_draw_with(rng, shape, spread, bound, shards, heavy, held_as=jnp.bfloat16):
    array = spread * jax.random.normal(rng, shape, jnp.float32)
    if shards:
        array = array * block_scale(rng, shape, shards, -0.22, 0.18)
    return jnp.clip(strengthened(array, jax.random.fold_in(rng, 3), *heavy), -bound, bound).astype(held_as)


def setup_inputs(seed: int = 0) -> dict:
    streams_of = jax.random.split(jax.random.key(seed), 7)
    return {
        "inputs": bell_draw_with(streams_of[0], (TOKENS, D), 1.0, 6.0, ((0, 32),), (0, 1, 32, 2.75)),
        "w_query": normal_values(streams_of[1], (D, D), D ** -0.5, 0.125, ((1, 8),)),
        "w_key": normal_values(streams_of[2], (D, D), D ** -0.5, 0.125, ((1, 8),)),
        "w_value": normal_values(streams_of[3], (D, D), D ** -0.5, 0.125, ((1, 8),)),
        "rel_table": draw_rel_table(jax.random.fold_in(streams_of[6], 71), 0),
        "out_grad": normal_values(streams_of[5], (TOKENS, D), 1.0, 6.0, ((0, 32), (1, 8))),
    }


def project(inputs, weight):
    return jnp.dot(inputs, weight, preferred_element_type=jnp.float32).astype(jnp.bfloat16)


def reference(inputs, w_query, w_key, w_value, rel_table, out_grad):
    reach = PREV * SEG
    band = reach + SEG
    score_scale = HDIM ** -0.5
    query = project(inputs, w_query).reshape(TOKENS, HEADS, HDIM)
    key_rows = project(inputs, w_key).reshape(TOKENS, HEADS, HDIM)
    value_rows = project(inputs, w_value).reshape(TOKENS, HEADS, HDIM)
    upstream = out_grad.reshape(TOKENS, HEADS, HDIM)
    key_pad = jnp.pad(key_rows, ((reach, 0), (0, 0), (0, 0)))
    value_pad = jnp.pad(value_rows, ((reach, 0), (0, 0), (0, 0)))
    row_index = jnp.arange(SEG, dtype=jnp.int32)[:, None]
    band_index = jnp.arange(band, dtype=jnp.int32)[None, :]
    buckets = jnp.clip(row_index + reach - band_index, -MAXREL, MAXREL) + MAXREL
    bias_pattern = rel_table[:, buckets].astype(jnp.float32)

    def one_segment(carry, segment):
        key_acc, value_acc, pattern = carry
        start = segment * SEG
        query_seg = lax.dynamic_slice_in_dim(query, start, SEG, 0).astype(jnp.float32)
        grad_seg = lax.dynamic_slice_in_dim(upstream, start, SEG, 0).astype(jnp.float32)
        key_band = lax.dynamic_slice_in_dim(key_pad, start, band, 0).astype(jnp.float32)
        value_band = lax.dynamic_slice_in_dim(value_pad, start, band, 0).astype(jnp.float32)
        visible = band_index[0] >= reach - start
        scores = jnp.einsum('qhd,khd->hqk', query_seg, key_band) * score_scale + bias_pattern
        scores = jnp.where(visible[None, None, :], scores, -jnp.inf)
        row_max = jnp.max(scores, axis=-1, keepdims=True)
        log_norm = row_max + jnp.log(jnp.sum(jnp.exp(scores - row_max), axis=-1, keepdims=True))
        probs_full = jnp.exp(scores - log_norm)
        probs_low = lax.optimization_barrier(probs_full.astype(jnp.bfloat16)).astype(jnp.float32)
        attn_out = jnp.einsum('hqk,khd->qhd', probs_low, value_band)
        attn_out = lax.optimization_barrier(attn_out.astype(jnp.bfloat16)).astype(jnp.float32)
        out_dot = jnp.sum(grad_seg * attn_out, axis=-1)
        value_part = jnp.einsum('hqk,qhd->khd', probs_low, grad_seg)
        prob_grad = jnp.einsum('qhd,khd->hqk', grad_seg, value_band)
        score_grad = probs_full * (prob_grad - jnp.transpose(out_dot)[:, :, None])
        score_low = lax.optimization_barrier(score_grad.astype(jnp.bfloat16)).astype(jnp.float32)
        query_part = score_scale * jnp.einsum('hqk,khd->qhd', score_low, key_band)
        key_part = score_scale * jnp.einsum('hqk,qhd->khd', score_low, query_seg)
        key_acc = lax.dynamic_update_slice_in_dim(
            key_acc, lax.dynamic_slice_in_dim(key_acc, start, band, 0) + key_part, start, 0)
        value_acc = lax.dynamic_update_slice_in_dim(
            value_acc, lax.dynamic_slice_in_dim(value_acc, start, band, 0) + value_part, start, 0)
        pattern = pattern + score_grad
        return (key_acc, value_acc, pattern), query_part.astype(jnp.bfloat16)

    initial = (jnp.zeros((TOKENS + reach, HEADS, HDIM), jnp.float32),
               jnp.zeros((TOKENS + reach, HEADS, HDIM), jnp.float32),
               jnp.zeros((HEADS, SEG, band), jnp.float32))
    (key_acc, value_acc, pattern), query_parts = lax.scan(
        one_segment, initial, jnp.arange(TOKENS // SEG, dtype=jnp.int32))
    query_grad = query_parts.reshape(TOKENS, D)
    key_grad = key_acc[reach:].reshape(TOKENS, D).astype(jnp.bfloat16)
    value_grad = value_acc[reach:].reshape(TOKENS, D).astype(jnp.bfloat16)
    one_hot = (buckets[:, :, None] == jnp.arange(2 * MAXREL + 1, dtype=jnp.int32)[None, None, :]).astype(jnp.float32)
    table_grad = jnp.einsum('hqk,qkr->hr', pattern, one_hot, precision=lax.Precision.HIGHEST)
    query_weight_grad = jnp.dot(inputs.T, query_grad, preferred_element_type=jnp.float32)
    key_weight_grad = jnp.dot(inputs.T, key_grad, preferred_element_type=jnp.float32)
    value_weight_grad = jnp.dot(inputs.T, value_grad, preferred_element_type=jnp.float32)
    return (query_grad, key_grad, value_grad, query_weight_grad, key_weight_grad, value_weight_grad, table_grad)
```

```python
import functools

import jax
import jax.numpy as jnp
import numpy as np
from jax import lax
from jax.experimental import pallas as pl
from jax.experimental.pallas import tpu as pltpu
from jax.sharding import Mesh
from jax.sharding import PartitionSpec as P

HDIM = 128
SEG = 64
PREV = 4
MAXREL = 128
REACH = PREV * SEG
TILE = 128
BAND = REACH + TILE
SP = ("sp_0", "sp_1")
NZ, NX = 8, 4
ROWS = 64
SCALE = HDIM ** (-0.5)
F32 = jnp.float32
BF16 = jnp.bfloat16


def odd_pair(i):
    return i ^ 1


def even_pair(i, n):
    return (i + 1) % n if i % 2 else (i - 1) % n


X0 = (("sp_1", odd_pair), ("sp_1", lambda i: even_pair(i, NX)))
X1 = (X0[1], X0[0])
ZF = ("sp_0", lambda i: (i + NZ // 2) % NZ)
Z0 = (("sp_0", odd_pair), ("sp_0", lambda i: even_pair(i, NZ)), ZF)
Z1 = (Z0[1], Z0[0], ZF)


def partner(level, device):
    axis, f = level
    z, x = divmod(device, NX)
    return f(z) * NX + x if axis == "sp_0" else z * NX + f(x)


def held_order(levels, device):
    if not levels:
        return [device]
    return held_order(levels[1:], partner(levels[0], device)) + held_order(levels[1:], device)


def place_table(levels):
    n = NZ * NX
    table = np.zeros((n, n), np.int32)
    for device in range(n):
        order = held_order(levels, device)
        assert sorted(order) == list(range(n))
        for at, unit in enumerate(order):
            table[device, unit] = at
    return table


def exchange(block, level):
    axis, f = level
    n = NZ if axis == "sp_0" else NX
    return lax.ppermute(block, axis, [(i, f(i)) for i in range(n)])


def reduced(send, keep, levels):
    for level in levels[:-1]:
        got = exchange(send, level)
        half = keep.shape[0] // 2
        send = (keep[:half].astype(F32) + got[:half].astype(F32)).astype(BF16)
        keep = (keep[half:].astype(F32) + got[half:].astype(F32)).astype(BF16)
    return keep.astype(F32) + exchange(send, levels[-1]).astype(F32)


def dot(a, b, contract=((1,), (0,))):
    return lax.dot_general(a, b, (contract, ((), ())), preferred_element_type=F32)


def tile_grads(query, grad, key, value, key_t, value_t, bias):
    scores = dot(key, query, ((1,), (1,))) * SCALE + bias
    top = jnp.max(scores, axis=0, keepdims=True)
    raised = jnp.exp(scores - top)
    probs = raised * (1.0 / jnp.sum(raised, axis=0, keepdims=True))
    probs_low = probs.astype(BF16)
    attn_out = dot(value_t, probs_low).astype(BF16).astype(F32)
    out_dot = jnp.sum(attn_out * grad.T.astype(F32), axis=0, keepdims=True)
    value_part = dot(probs_low, grad)
    score_grad = probs * (dot(value, grad, ((1,), (1,))) - out_dot)
    score_low = score_grad.astype(BF16)
    query_part = (dot(key_t, score_low) * SCALE).T
    key_part = dot(score_low, query) * SCALE
    return score_grad, query_part, key_part, value_part


def tail_kernel(x_ref, wk_ref, wv_ref, out_ref):
    x = x_ref[...]
    out_ref[:, :256] = dot(x, wk_ref[...]).astype(BF16)
    out_ref[:, 256:] = dot(x, wv_ref[...]).astype(BF16)


def main_kernel(
    x_ref, wq_ref, wk_ref, wv_ref, far_ref, og_ref,
    xt_ref, dq_ref, kg_ref, vg_ref, q0_ref, k0_ref, v0_ref, edge_ref, bias_ref, pat_ref,
    k_s, v_s, kt_s, vt_s, ka_s, va_s,
):
    b = pl.program_id(0)
    x = x_ref[...]
    query = dot(x, wq_ref[...]).astype(BF16)
    key = dot(x, wk_ref[...]).astype(BF16)
    value = dot(x, wv_ref[...]).astype(BF16)
    here = pl.ds(pl.multiple_of(b * REACH, REACH), REACH)
    k_s[here, :] = key
    v_s[here, :] = value
    kt_s[:, here] = key.T
    vt_s[:, here] = value.T
    xt_ref[...] = x.T

    @pl.when(b == 0)
    def _():
        q0_ref[...] = query
        k0_ref[...] = key
        v0_ref[...] = value
        ka_s[:REACH] = jnp.zeros((REACH, 256), F32)
        va_s[:REACH] = jnp.zeros((REACH, 256), F32)
        pat_ref[...] = jnp.zeros_like(pat_ref)
        u = lax.broadcasted_iota(jnp.int32, (BAND, TILE), 0)
        t = lax.broadcasted_iota(jnp.int32, (BAND, TILE), 1)
        low = jnp.where(t < SEG, 0, SEG)
        inside = (u >= low) & (u < low + REACH + SEG)
        for h in range(2):
            far = jnp.broadcast_to(far_ref[h : h + 1, :], (BAND, 512))
            skew = pltpu.roll(far, 0, 1, stride=1, stride_axis=0)[:, BAND:]
            bias_ref[h] = jnp.where(inside, skew, -jnp.inf)

    @pl.when(b > 0)
    def _():
        ka_s[here, :] = jnp.zeros((REACH, 256), F32)
        va_s[here, :] = jnp.zeros((REACH, 256), F32)
        for t in range(2):
            rows = slice(t * TILE, (t + 1) * TILE)
            band = pl.ds(pl.multiple_of((b - 1) * REACH + t * TILE, TILE), BAND)
            for h in range(2):
                cols = slice(h * HDIM, (h + 1) * HDIM)
                score_grad, query_part, key_part, value_part = tile_grads(
                    query[rows, cols], og_ref[rows, cols], k_s[band, cols], v_s[band, cols],
                    kt_s[cols, band], vt_s[cols, band], bias_ref[h],
                )
                pat_ref[h] += score_grad
                dq_ref[rows, cols] = query_part.astype(BF16)
                ka_s[band, cols] += key_part
                va_s[band, cols] += value_part

    @pl.when(b == 3)
    def _():
        kg_ref[256:768] = ka_s[256:768].astype(BF16)
        vg_ref[256:768] = va_s[256:768].astype(BF16)
        edge_ref[0, :, :256] = ka_s[:256]
        edge_ref[0, :, 256:] = va_s[:256]
        edge_ref[1, :, :256] = ka_s[768:]
        edge_ref[1, :, 256:] = va_s[768:]


def first_kernel(
    flag_ref, q_ref, k_ref, v_ref, halo_ref, og_ref, bias_ref, pat_ref, edge_ref, dq_in, kg_in, vg_in,
    dq_ref, kg_ref, vg_ref, back_ref, table_ref,
    k_s, v_s, kt_s, vt_s, ka_s, va_s, pat_s, diag_s,
):
    del dq_in, kg_in, vg_in
    k_s[:REACH] = halo_ref[:, :256]
    v_s[:REACH] = halo_ref[:, 256:]
    k_s[REACH:] = k_ref[...]
    v_s[REACH:] = v_ref[...]
    kt_s[...] = k_s[...].T
    vt_s[...] = v_s[...].T
    ka_s[:REACH] = jnp.zeros((REACH, 256), F32)
    va_s[:REACH] = jnp.zeros((REACH, 256), F32)
    ka_s[REACH:] = edge_ref[0, :, :256]
    va_s[REACH:] = edge_ref[0, :, 256:]
    pat_s[...] = pat_ref[...]
    outside = flag_ref[0] == 0
    u = lax.broadcasted_iota(jnp.int32, (BAND, TILE), 0)
    for t in range(2):
        rows = slice(t * TILE, (t + 1) * TILE)
        band = slice(t * TILE, t * TILE + BAND)
        for h in range(2):
            cols = slice(h * HDIM, (h + 1) * HDIM)
            bias = jnp.where(outside & (u < REACH - t * TILE), -jnp.inf, bias_ref[h])
            score_grad, query_part, key_part, value_part = tile_grads(
                q_ref[rows, cols], og_ref[rows, cols], k_s[band, cols], v_s[band, cols],
                kt_s[cols, band], vt_s[cols, band], bias,
            )
            pat_s[h] += score_grad
            dq_ref[rows, cols] = query_part.astype(BF16)
            ka_s[band, cols] += key_part
            va_s[band, cols] += value_part
    kg_ref[...] = ka_s[REACH:].astype(BF16)
    vg_ref[...] = va_s[REACH:].astype(BF16)
    back_ref[:, :256] = ka_s[:REACH].astype(BF16)
    back_ref[:, 256:] = va_s[:REACH].astype(BF16)
    for h in range(2):
        diag_s[...] = jnp.zeros_like(diag_s)
        for a in range(BAND // 8):
            off = BAND - 8 * a
            diag_s[:, off : off + TILE] += pat_s[h, 8 * a : 8 * a + 8, :]
        total = jnp.zeros((1, 512), F32)
        for s in range(8):
            total += diag_s[s : s + 1, s : s + 512]
        far = jnp.sum(total[:, 256:], axis=1, keepdims=True)
        table_ref[h : h + 1, :256] = total[:, :256]
        table_ref[h : h + 1, 256:] = jnp.broadcast_to(far, (1, 128))


def store_units(value, first_unit, place_ref, send_ref, keep_ref):
    for i in range(value.shape[0] // ROWS):
        at = place_ref[first_unit + i]
        rows = value[i * ROWS : (i + 1) * ROWS]

        @pl.when(at < 16)
        def _():
            send_ref[pl.ds(pl.multiple_of(at * ROWS, ROWS), ROWS), :] = rows

        @pl.when(at >= 16)
        def _():
            keep_ref[pl.ds(pl.multiple_of((at - 16) * ROWS, ROWS), ROWS), :] = rows


def query_weight_kernel(place_ref, xt_ref, dq_ref, send_ref, keep_ref):
    i = pl.program_id(0)
    value = dot(xt_ref[...], dq_ref[...]).astype(BF16)
    store_units(value, i * (value.shape[0] // ROWS), place_ref, send_ref, keep_ref)


def pair_weight_kernel(
    kplace_ref, vplace_ref, xt_ref, kg_in, vg_in, edge_ref, back_ref,
    kg_ref, vg_ref, ksend_ref, kkeep_ref, vsend_ref, vkeep_ref, k_s, v_s,
):
    i = pl.program_id(0)

    @pl.when(i == 0)
    def _():
        k_s[:768] = kg_in[:768]
        v_s[:768] = vg_in[:768]
        key = (edge_ref[0, :, :256] + back_ref[:, :256].astype(F32)).astype(BF16)
        value = (edge_ref[0, :, 256:] + back_ref[:, 256:].astype(F32)).astype(BF16)
        k_s[768:] = key
        v_s[768:] = value
        kg_ref[...] = key
        vg_ref[...] = value

    x = xt_ref[...]
    key = dot(x, k_s[...]).astype(BF16)
    value = dot(x, v_s[...]).astype(BF16)
    units = key.shape[0] // ROWS
    store_units(key, i * units, kplace_ref, ksend_ref, kkeep_ref)
    store_units(value, i * units, vplace_ref, vsend_ref, vkeep_ref)


def sds(shape, dtype):
    return jax.ShapeDtypeStruct(shape, dtype)


def whole(shape):
    return pl.BlockSpec(shape, lambda *_: (0,) * len(shape))


def once(shape):
    return pl.BlockSpec(shape, lambda *_: (0,) * len(shape), pipeline_mode=pl.Buffered(1))


def cost(flops, byte_count):
    return pl.CostEstimate(flops=flops, bytes_accessed=byte_count, transcendentals=0)


def params():
    return pltpu.CompilerParams(dimension_semantics=("arbitrary",))


def tail_call(inputs, w_key, w_value):
    return pl.pallas_call(
        tail_kernel,
        grid=(1,),
        in_specs=[pl.BlockSpec((REACH, 2048), lambda i: (3, 0)), whole((2048, 256)), whole((2048, 256))],
        out_specs=whole((REACH, 512)),
        out_shape=sds((REACH, 512), BF16),
        compiler_params=params(),
        cost_estimate=cost(2 * 256 * 2048 * 512, 3 << 20),
        name="tail",
    )(inputs, w_key, w_value)


def main_call(inputs, w_query, w_key, w_value, far, out_grad):
    block = lambda i: (i, 0)
    return pl.pallas_call(
        main_kernel,
        grid=(4,),
        in_specs=[
            pl.BlockSpec((REACH, 2048), block),
            once((2048, 256)), once((2048, 256)), once((2048, 256)),
            once((2, 512)),
            pl.BlockSpec((REACH, 256), block),
        ],
        out_specs=[
            pl.BlockSpec((2048, REACH), lambda i: (0, i)),
            pl.BlockSpec((REACH, 256), block),
            whole((1024, 256)), whole((1024, 256)),
            whole((REACH, 256)), whole((REACH, 256)), whole((REACH, 256)),
            whole((2, REACH, 512)),
            whole((2, BAND, TILE)), whole((2, BAND, TILE)),
        ],
        out_shape=[
            sds((2048, 1024), BF16),
            sds((1024, 256), BF16),
            sds((1024, 256), BF16), sds((1024, 256), BF16),
            sds((REACH, 256), BF16), sds((REACH, 256), BF16), sds((REACH, 256), BF16),
            sds((2, REACH, 512), F32),
            sds((2, BAND, TILE), F32), sds((2, BAND, TILE), F32),
        ],
        scratch_shapes=[
            pltpu.VMEM((1024, 256), BF16), pltpu.VMEM((1024, 256), BF16),
            pltpu.VMEM((256, 1024), BF16), pltpu.VMEM((256, 1024), BF16),
            pltpu.VMEM((1024, 256), F32), pltpu.VMEM((1024, 256), F32),
        ],
        compiler_params=params(),
        cost_estimate=cost(2 * 1024 * 2048 * 768 + 12 * 6 * 2 * 128 * 128 * 384, 12 << 20),
        name="main",
    )(inputs, w_query, w_key, w_value, far, out_grad)


def first_call(flag, q0, k0, v0, halo, out_grad, bias, pat, edge, dq, kg, vg):
    anyspec = pl.BlockSpec(memory_space=pl.ANY)
    spec = pltpu.PrefetchScalarGridSpec(
        num_scalar_prefetch=1,
        grid=(1,),
        in_specs=[
            whole((REACH, 256)), whole((REACH, 256)), whole((REACH, 256)),
            whole((REACH, 512)),
            whole((REACH, 256)),
            whole((2, BAND, TILE)), whole((2, BAND, TILE)),
            whole((1, REACH, 512)),
            anyspec, anyspec, anyspec,
        ],
        out_specs=[
            whole((REACH, 256)), whole((REACH, 256)), whole((REACH, 256)),
            whole((REACH, 512)),
            whole((2, 384)),
        ],
        scratch_shapes=[
            pltpu.VMEM((512, 256), BF16), pltpu.VMEM((512, 256), BF16),
            pltpu.VMEM((256, 512), BF16), pltpu.VMEM((256, 512), BF16),
            pltpu.VMEM((512, 256), F32), pltpu.VMEM((512, 256), F32),
            pltpu.VMEM((2, BAND, TILE), F32),
            pltpu.VMEM((8, 640), F32),
        ],
    )
    return pl.pallas_call(
        first_kernel,
        grid_spec=spec,
        out_shape=[
            sds((1024, 256), BF16), sds((1024, 256), BF16), sds((1024, 256), BF16),
            sds((REACH, 512), BF16),
            sds((2, 384), F32),
        ],
        input_output_aliases={9: 0, 10: 1, 11: 2},
        compiler_params=params(),
        cost_estimate=cost(4 * 6 * 2 * 128 * 128 * 384, 3 << 20),
        name="first",
    )(flag, q0, k0, v0, halo, out_grad, bias, pat, edge, dq, kg, vg)


def query_weight_call(place, xt, dq):
    spec = pltpu.PrefetchScalarGridSpec(
        num_scalar_prefetch=1,
        grid=(4,),
        in_specs=[pl.BlockSpec((512, 1024), lambda i, *_: (i, 0)), once((1024, 256))],
        out_specs=[whole((1024, 256)), whole((1024, 256))],
    )
    return pl.pallas_call(
        query_weight_kernel,
        grid_spec=spec,
        out_shape=[sds((1024, 256), BF16)] * 2,
        compiler_params=params(),
        cost_estimate=cost(2 * 1024 * 2048 * 256, 6 << 20),
        name="qweight",
    )(place, xt, dq)


def pair_weight_call(kplace, vplace, xt, kg, vg, edge, back):
    spec = pltpu.PrefetchScalarGridSpec(
        num_scalar_prefetch=2,
        grid=(4,),
        in_specs=[
            pl.BlockSpec((512, 1024), lambda i, *_: (i, 0)),
            once((1024, 256)), once((1024, 256)),
            pl.BlockSpec((1, REACH, 512), lambda i, *_: (1, 0, 0)),
            once((REACH, 512)),
        ],
        out_specs=[
            pl.BlockSpec((REACH, 256), lambda i, *_: (3, 0)),
            pl.BlockSpec((REACH, 256), lambda i, *_: (3, 0)),
        ] + [whole((1024, 256))] * 4,
        scratch_shapes=[pltpu.VMEM((1024, 256), BF16), pltpu.VMEM((1024, 256), BF16)],
    )
    return pl.pallas_call(
        pair_weight_kernel,
        grid_spec=spec,
        out_shape=[sds((1024, 256), BF16)] * 6,
        input_output_aliases={3: 0, 4: 1},
        compiler_params=params(),
        cost_estimate=cost(4 * 1024 * 2048 * 256, 9 << 20),
        name="pairweight",
    )(kplace, vplace, xt, kg, vg, edge, back)


def neighbour(block, distance):
    count = NZ * NX
    route = [(i, i + distance) for i in range(count) if 0 <= i + distance < count]
    return lax.ppermute(block, SP, route)


QLEVELS = X0 + Z0
KLEVELS = Z0 + X0
VLEVELS = X1 + Z1


def local(inputs, w_query, w_key, w_value, rel_table, out_grad):
    me = lax.axis_index(SP)
    places = [jnp.asarray(place_table(levels))[me] for levels in (QLEVELS, KLEVELS, VLEVELS)]
    flag = jnp.reshape(me, (1,)).astype(jnp.int32)
    halo = neighbour(tail_call(inputs, w_key, w_value), 1)
    far = jnp.pad(rel_table, ((0, 0), (0, 512 - rel_table.shape[1])), mode="edge")
    xt, dq, kg, vg, q0, k0, v0, edge, bias, pat = main_call(
        inputs, w_query, w_key, w_value, far, out_grad
    )
    dq, kg, vg, back, table = first_call(
        flag, q0, k0, v0, halo, out_grad, bias, pat, edge, dq, kg, vg
    )
    back = neighbour(back, -1)
    tables = jnp.broadcast_to(table, (NZ * NX, *table.shape))
    tables = lax.all_to_all(tables, SP, split_axis=0, concat_axis=0, tiled=True)
    table_grad = tables.sum(axis=0)[:, : rel_table.shape[1]]
    qsend, qkeep = query_weight_call(places[0], xt, dq)
    query_weight_grad = reduced(qsend, qkeep, QLEVELS)
    kg, vg, ksend, kkeep, vsend, vkeep = pair_weight_call(places[1], places[2], xt, kg, vg, edge, back)
    key_weight_grad = reduced(ksend, kkeep, KLEVELS)
    value_weight_grad = reduced(vsend, vkeep, VLEVELS)
    return (dq, kg, vg, query_weight_grad, key_weight_grad, value_weight_grad, table_grad)


def solution(mesh):
    torus = Mesh(mesh.devices.reshape(NZ, NX, mesh.shape["tp"]), ("sp_0", "sp_1", "tp"))
    in_specs = (P(SP, None), P(None, "tp"), P(None, "tp"), P(None, "tp"), P("tp", None), P(SP, "tp"))
    out_specs = (P(SP, "tp"),) * 6 + (P("tp", None),)
    return jax.shard_map(local, mesh=torus, in_specs=in_specs, out_specs=out_specs, check_vma=False)
```

```python
import jax
import jax.numpy as jnp
from jax import lax
from jax.experimental import pallas as pl
from jax.experimental.pallas import tpu as pltpu
from jax.sharding import Mesh
from jax.sharding import PartitionSpec as P


HDIM = 128
SEG = 64
PREV = 4
REACH = PREV * SEG
TILE = 128
BAND = REACH + TILE
SP = ("sp_0", "sp_1")
NZ, NX = 8, 4
ROWS = 64
EXTRA = 16
VMEM_LIMIT = 24 << 20
CHUNKS = 4
WIDTH = 2048 // CHUNKS
SCALE = HDIM ** (-0.5)
F32 = jnp.float32
BF16 = jnp.bfloat16


def odd_pair(i):
    return i ^ 1


def even_pair(n):
    return lambda i: (i + 1) % n if i % 2 else (i - 1) % n


XO, XE = ("sp_1", odd_pair), ("sp_1", even_pair(NX))
ZO, ZE = ("sp_0", odd_pair), ("sp_0", even_pair(NZ))
ZF = ("sp_0", lambda i: (i + NZ // 2) % NZ)
OWN = ((XO, XE, ZO, ZE, ZF), (ZO, ZE, XO, XE, ZF))
OTHER = ((XE, XO, ZO, ZE, ZF), (ZE, ZO, XO, XE, ZF))


def held_order(steps, device):
    if not steps:
        return [device]
    return held_order(steps[1:], steps[0](device)) + held_order(steps[1:], device)


def axis_codes(levels, axis):
    n = NZ if axis == "sp_0" else NX
    mine = [f for a, f in levels if a == axis]
    spots = [len(levels) - 1 - i for i, (a, _) in enumerate(levels) if a == axis]
    wanted = [0] * n
    for device in range(n):
        order = held_order(mine, device)
        assert sorted(order) == list(range(n))
        for at, unit in enumerate(order):
            wanted[unit] |= at << (4 * device)
    me = lax.axis_index(axis)
    codes = []
    for packed in wanted:
        at = jnp.int32(0)
        for device in range(n):
            at = jnp.where(me == device, jnp.int32((packed >> (4 * device)) & 15), at)
        code = jnp.int32(0)
        for i, spot in enumerate(spots):
            code = code | (((at >> (len(spots) - 1 - i)) & 1) << spot)
        codes.append(code)
    return codes


def unit_places(sequences):
    core = lax.axis_index("core")
    places = []
    for levels in sequences:
        along_z, along_x = axis_codes(levels, "sp_0"), axis_codes(levels, "sp_1")
        places.append([along_z[unit // NX] + along_x[unit % NX] for unit in range(NZ * NX)])
    return [jnp.where(core == 0, a, b) for a, b in zip(*places)]


def level_route(sequences, level):
    route = []
    for core, levels in enumerate(sequences):
        axis, f = levels[level]
        for z in range(NZ):
            for x in range(NX):
                to = f(z) * NX + x if axis == "sp_0" else z * NX + f(x)
                route.append(((z * NX + x) * 2 + core, to * 2 + core))
    return route


def exchange(block, sequences, level):
    return lax.ppermute(block, SP + ("core",), level_route(sequences, level))


def core_swap(block):
    return lax.ppermute(block, "core", [(0, 1), (1, 0)])


def dot(a, b, contract=((1,), (0,))):
    return lax.dot_general(a, b, (contract, ((), ())), preferred_element_type=F32)


def tile_grads(query, grad, key, value, key_t, value_t, bias):
    scores = dot(key, query, ((1,), (1,))) * SCALE + bias
    top = jnp.max(scores, axis=0, keepdims=True)
    raised = jnp.exp(scores - top)
    probs = raised * (1.0 / jnp.sum(raised, axis=0, keepdims=True))
    probs_low = probs.astype(BF16)
    attn_out = dot(value_t, probs_low).astype(BF16).astype(F32)
    out_dot = jnp.sum(attn_out * grad.T.astype(F32), axis=0, keepdims=True)
    value_part = dot(probs_low, grad)
    score_grad = probs * (dot(value, grad, ((1,), (1,))) - out_dot)
    score_low = score_grad.astype(BF16)
    query_part = (dot(key_t, score_low) * SCALE).T
    key_part = dot(score_low, query) * SCALE
    return score_grad, query_part, key_part, value_part


def tail_kernel(x_ref, wk_ref, wv_ref, out_ref):
    x = x_ref[...]
    out_ref[:, :256] = dot(x, wk_ref[...]).astype(BF16)
    out_ref[:, 256:] = dot(x, wv_ref[...]).astype(BF16)


def proj_kernel(x_ref, wq_ref, wk_ref, wv_ref, q_ref, k_ref, v_ref):
    x = x_ref[...]
    q_ref[...] = dot(x, wq_ref[...]).astype(BF16)
    k_ref[...] = dot(x, wk_ref[...]).astype(BF16)
    v_ref[...] = dot(x, wv_ref[...]).astype(BF16)


def first_kernel(
    q_ref, k_ref, v_ref, halo_ref, og_ref, far_ref,
    dq_ref, edge_ref, back_ref, bias_ref, pat_ref,
    k_s, v_s, kt_s, vt_s, ka_s, va_s,
):
    k_s[:REACH] = halo_ref[:, :256]
    v_s[:REACH] = halo_ref[:, 256:]
    k_s[REACH:] = k_ref[...]
    v_s[REACH:] = v_ref[...]
    kt_s[...] = k_s[...].T
    vt_s[...] = v_s[...].T
    ka_s[...] = jnp.zeros_like(ka_s)
    va_s[...] = jnp.zeros_like(va_s)
    outside = (lax.axis_index("sp_0") == 0) & (lax.axis_index("sp_1") == 0)
    u = lax.broadcasted_iota(jnp.int32, (BAND, TILE), 0)
    col = lax.broadcasted_iota(jnp.int32, (BAND, TILE), 1)
    low = jnp.where(col < SEG, 0, SEG)
    inside = (u >= low) & (u < low + REACH + SEG)
    for h in range(2):
        far = jnp.broadcast_to(far_ref[h : h + 1, :], (BAND, 512))
        skew = pltpu.roll(far, 0, 1, stride=1, stride_axis=0)[:, BAND:]
        bias_ref[h] = jnp.where(inside, skew, -jnp.inf)
    for t in range(2):
        rows = slice(t * TILE, (t + 1) * TILE)
        band = slice(t * TILE, t * TILE + BAND)
        for h in range(2):
            cols = slice(h * HDIM, (h + 1) * HDIM)
            bias = jnp.where(outside & (u < REACH - t * TILE), -jnp.inf, bias_ref[h])
            score_grad, query_part, key_part, value_part = tile_grads(
                q_ref[rows, cols], og_ref[rows, cols], k_s[band, cols], v_s[band, cols],
                kt_s[cols, band], vt_s[cols, band], bias,
            )
            if t == 0:
                pat_ref[h] = score_grad
            else:
                pat_ref[h] += score_grad
            dq_ref[rows, cols] = query_part.astype(BF16)
            ka_s[band, cols] += key_part
            va_s[band, cols] += value_part
    edge_ref[:, :256] = ka_s[REACH:]
    edge_ref[:, 256:] = va_s[REACH:]
    back_ref[:, :256] = ka_s[:REACH].astype(BF16)
    back_ref[:, 256:] = va_s[:REACH].astype(BF16)


def attn_kernel(
    q_ref, k_ref, v_ref, og_ref, bias_ref, pat_in, edge_in, dq_in,
    dq_ref, kg_ref, vg_ref, edge_ref, pat_ref,
    kt_s, vt_s, ka_s, va_s,
):
    i = pl.program_id(0)

    @pl.when(i == 0)
    def _():
        kt_s[...] = k_ref[...].T
        vt_s[...] = v_ref[...].T
        ka_s[:REACH] = edge_in[:, :256]
        va_s[:REACH] = edge_in[:, 256:]
        ka_s[REACH:] = jnp.zeros((768, 256), F32)
        va_s[REACH:] = jnp.zeros((768, 256), F32)
        pat_ref[...] = pat_in[...]
        dq_ref[:REACH] = dq_in[...]

    for t in range(2):
        rows = pl.ds(pl.multiple_of((i + 1) * REACH + t * TILE, TILE), TILE)
        band = pl.ds(pl.multiple_of(i * REACH + t * TILE, TILE), BAND)
        for h in range(2):
            cols = slice(h * HDIM, (h + 1) * HDIM)
            score_grad, query_part, key_part, value_part = tile_grads(
                q_ref[rows, cols], og_ref[rows, cols], k_ref[band, cols], v_ref[band, cols],
                kt_s[cols, band], vt_s[cols, band], bias_ref[h],
            )
            pat_ref[h] += score_grad
            dq_ref[rows, cols] = query_part.astype(BF16)
            ka_s[band, cols] += key_part
            va_s[band, cols] += value_part

    @pl.when(i == 2)
    def _():
        kg_ref[...] = ka_s[:768].astype(BF16)
        vg_ref[...] = va_s[:768].astype(BF16)
        edge_ref[:, :256] = ka_s[768:]
        edge_ref[:, 256:] = va_s[768:]


def finish_kernel(kg_in, vg_in, edge_ref, back_ref, dq_ref, kg_ref, vg_ref, own_ref, swap_ref):
    kg_ref[:768] = kg_in[...]
    vg_ref[:768] = vg_in[...]
    kg_ref[768:] = (edge_ref[:, :256] + back_ref[:, :256].astype(F32)).astype(BF16)
    vg_ref[768:] = (edge_ref[:, 256:] + back_ref[:, 256:].astype(F32)).astype(BF16)
    core = lax.axis_index("core")

    @pl.when(core == 0)
    def _():
        own_ref[:, :256] = kg_ref[...]
        own_ref[:, 256:] = dq_ref[:, :128]
        swap_ref[:, :256] = vg_ref[...]
        swap_ref[:, 256:] = dq_ref[:, 128:]

    @pl.when(core == 1)
    def _():
        own_ref[:, :256] = vg_ref[...]
        own_ref[:, 256:] = dq_ref[:, 128:]
        swap_ref[:, :256] = kg_ref[...]
        swap_ref[:, 256:] = dq_ref[:, :128]


def store_units(value, chunk, places, out_s):
    units = WIDTH // ROWS
    for i in range(units):
        at = pl.multiple_of(places[chunk * units + i] * ROWS, ROWS)
        out_s[pl.ds(at, ROWS), :] = value[i * ROWS : (i + 1) * ROWS].astype(BF16)


def placed_product(x_ref, grad_ref, sequences, out_s):
    places = unit_places(sequences)
    for c in range(CHUNKS):
        cols = slice(c * WIDTH, (c + 1) * WIDTH)
        store_units(dot(x_ref[:, cols], grad_ref[...], ((0,), (0,))), c, places, out_s)


def three_parts(table):
    high = table.astype(BF16).astype(F32)
    mid = (table - high).astype(BF16).astype(F32)
    low = table - high - mid
    rest = jnp.zeros((EXTRA - 6, table.shape[1]), F32)
    return jnp.concatenate([high, mid, low, rest], axis=0).astype(BF16)


def table_of(parts):
    parts = parts.astype(F32)
    return parts[0:2] + parts[2:4] + parts[4:6]


def copy_out(pairs, sem):
    copies = [pltpu.make_async_copy(src, dst, sem.at[i]) for i, (src, dst) in enumerate(pairs)]
    for copy in copies:
        copy.start()
    for copy in copies:
        copy.wait()


def own_kernel(x_ref, grad_ref, pat_ref, send_hbm, keep_hbm, table_ref, out_s, parts_s, diag_s, sem):
    placed_product(x_ref, grad_ref, OWN, out_s)
    for h in range(2):
        diag_s[...] = jnp.zeros_like(diag_s)
        for a in range(BAND // 8):
            off = BAND - 8 * a
            diag_s[:, off : off + TILE] += pat_ref[h, 8 * a : 8 * a + 8, :]
        total = jnp.zeros((1, 512), F32)
        for s in range(8):
            total += diag_s[s : s + 1, s : s + 512]
        far = jnp.sum(total[:, 256:], axis=1, keepdims=True)
        table_ref[h : h + 1, :256] = total[:, :256]
        table_ref[h : h + 1, 256:] = jnp.broadcast_to(far, (1, 128))
    parts_s[...] = three_parts(table_ref[...])
    copy_out(
        [(out_s.at[:1024], send_hbm.at[:1024]), (parts_s, send_hbm.at[1024:]), (out_s.at[1024:], keep_hbm)],
        sem,
    )


def other_kernel(x_ref, grad_ref, send_hbm, keep_hbm, out_s, sem):
    placed_product(x_ref, grad_ref, OTHER, out_s)
    copy_out([(out_s.at[:1024], send_hbm), (out_s.at[1024:], keep_hbm)], sem)


def added(keep, got):
    return keep.astype(F32) + got.astype(F32)


def level_kernel(keep_ref, got_ref, table_in, send_ref, next_ref, table_ref):
    half = next_ref.shape[0]
    n = 2 * half
    total = table_in[...] + table_of(got_ref[n:, :384])
    table_ref[...] = total
    send_ref[:half] = added(keep_ref[:half], got_ref[:half]).astype(BF16)
    next_ref[...] = added(keep_ref[half:], got_ref[half:n]).astype(BF16)
    send_ref[half:, :384] = three_parts(total)
    if send_ref.shape[1] > 384:
        send_ref[half:, 384:] = jnp.zeros((EXTRA, send_ref.shape[1] - 384), BF16)


def merge_kernel(keep_ref, got_ref, keep2_ref, got2_ref, table_in, send_ref, next_ref, table_ref):
    half = next_ref.shape[0]
    n = 2 * half
    total = table_in[...] + table_of(got_ref[n:])
    table_ref[...] = total
    send_ref[:half, :384] = added(keep_ref[:half], got_ref[:half]).astype(BF16)
    send_ref[:half, 384:] = added(keep2_ref[:half], got2_ref[:half]).astype(BF16)
    next_ref[:, :384] = added(keep_ref[half:], got_ref[half:n]).astype(BF16)
    next_ref[:, 384:] = added(keep2_ref[half:], got2_ref[half:]).astype(BF16)
    send_ref[half:, :384] = three_parts(total)
    send_ref[half:, 384:] = jnp.zeros((EXTRA, 384), BF16)


def last_kernel(keep_ref, got_ref, table_in, own_ref, swap_ref, table_ref):
    n = keep_ref.shape[0]
    table_ref[...] = table_in[...] + table_of(got_ref[n:, :384])
    own_ref[...] = added(keep_ref[:, :384], got_ref[:n, :384])
    swap_ref[...] = added(keep_ref[:, 384:], got_ref[:n, 384:])


def output_kernel(own_ref, got_ref, q_ref, k_ref, v_ref):
    core = lax.axis_index("core")

    @pl.when(core == 0)
    def _():
        k_ref[...] = own_ref[:, :256]
        v_ref[...] = got_ref[:, :256]
        q_ref[:, :128] = own_ref[:, 256:]
        q_ref[:, 128:] = got_ref[:, 256:]

    @pl.when(core == 1)
    def _():
        v_ref[...] = own_ref[:, :256]
        k_ref[...] = got_ref[:, :256]
        q_ref[:, 128:] = own_ref[:, 256:]
        q_ref[:, :128] = got_ref[:, 256:]


def sds(shape, dtype):
    return jax.ShapeDtypeStruct(shape, dtype)


def whole(shape):
    return pl.BlockSpec(shape, lambda *_: (0,) * len(shape))


def cost(flops, byte_count):
    return pl.CostEstimate(flops=flops, bytes_accessed=byte_count, transcendentals=0)


def params():
    return pltpu.CompilerParams(dimension_semantics=("arbitrary",), vmem_limit_bytes=VMEM_LIMIT)


def call(kernel, operands, outs, scratch=(), grid=(1,), flops=1 << 20, blocks=None, any_outs=()):
    specs = [whole(x.shape) for x in operands]
    for at, shape in (blocks or {}).items():
        specs[at] = whole(shape)
    out_specs = [pl.BlockSpec(memory_space=pl.ANY) if i in any_outs else whole(x.shape) for i, x in enumerate(outs)]
    moved = sum(x.size * x.dtype.itemsize for x in (*operands, *outs))
    return pl.pallas_call(
        kernel,
        grid=grid,
        in_specs=specs,
        out_specs=out_specs,
        out_shape=list(outs),
        scratch_shapes=list(scratch),
        compiler_params=params(),
        cost_estimate=cost(flops, moved),
    )(*operands)


def neighbour(block, distance):
    count = NZ * NX
    route = [(i, i + distance) for i in range(count) if 0 <= i + distance < count]
    return lax.ppermute(block, SP, route)


def staged(inputs, w_query, w_key, w_value, rel_table, out_grad):
    f32, b16 = (lambda *s: sds(s, F32)), (lambda *s: sds(s, BF16))
    v32, v16 = (lambda *s: pltpu.VMEM(s, F32)), (lambda *s: pltpu.VMEM(s, BF16))
    tile_flops = 6 * 2 * TILE * BAND * HDIM
    (tail,) = call(
        tail_kernel, (inputs[1024 - REACH :], w_key, w_value), (b16(REACH, 512),), flops=2 * 256 * 2048 * 512
    )
    halo = neighbour(tail, 1)
    far = jnp.pad(rel_table, ((0, 0), (0, 512 - rel_table.shape[1])), mode="edge")
    query, key, value = call(
        proj_kernel, (inputs, w_query, w_key, w_value), (b16(1024, 256),) * 3,
        flops=2 * 1024 * 2048 * 768,
    )
    block = (REACH, 256)
    dq0, edge, back, bias, pat = call(
        first_kernel, (query, key, value, halo, out_grad, far),
        (b16(REACH, 256), f32(REACH, 512), b16(REACH, 512), f32(2, BAND, TILE), f32(2, BAND, TILE)),
        (v16(512, 256), v16(512, 256), v16(256, 512), v16(256, 512), v32(512, 256), v32(512, 256)),
        flops=4 * tile_flops, blocks={0: block, 1: block, 2: block, 4: block},
    )
    back = neighbour(back, -1)
    dq, kg, vg, edge, pat = call(
        attn_kernel, (query, key, value, out_grad, bias, pat, edge, dq0),
        (b16(1024, 256), b16(768, 256), b16(768, 256), f32(REACH, 512), f32(2, BAND, TILE)),
        (v16(256, 1024), v16(256, 1024), v32(1024, 256), v32(1024, 256)),
        grid=(3,), flops=12 * tile_flops,
    )
    kg, vg, own, swap = call(finish_kernel, (kg, vg, edge, back, dq), (b16(1024, 256),) * 2 + (b16(1024, 384),) * 2)
    got = core_swap(swap)
    sem = pltpu.SemaphoreType.DMA((3,))
    product = 2 * 1024 * 2048 * 384
    send, keep, table = call(
        own_kernel, (inputs, own, pat), (b16(1024 + EXTRA, 384), b16(1024, 384), f32(2, 384)),
        (v16(2048, 384), v16(EXTRA, 384), v32(8, 640), sem), flops=product, any_outs=(0, 1),
    )
    send2, keep2 = call(
        other_kernel, (inputs, got), (b16(1024, 384),) * 2, (v16(2048, 384), sem),
        flops=product, any_outs=(0, 1),
    )
    got = exchange(send, OWN, 0)
    got2 = exchange(send2, OTHER, 0)
    send, keep, table = call(level_kernel, (keep, got, table), (b16(512 + EXTRA, 384), b16(512, 384), f32(2, 384)))
    got = exchange(send, OWN, 1)
    send2, keep2 = added(keep2[:512], got2[:512]).astype(BF16), added(keep2[512:], got2[512:]).astype(BF16)
    got2 = exchange(send2, OTHER, 1)
    send, keep, table = call(
        merge_kernel, (keep, got, keep2, got2, table), (b16(256 + EXTRA, 768), b16(256, 768), f32(2, 384))
    )
    for level, rows in ((2, 128), (3, 64)):
        got = exchange(send, OWN, level)
        send, keep, table = call(
            level_kernel, (keep, got, table),
            (b16(rows + EXTRA, 768), b16(rows, 768), f32(2, 384)),
        )
    got = exchange(send, OWN, 4)
    own, swap, table = call(last_kernel, (keep, got, table), (f32(64, 384), f32(64, 384), f32(2, 384)))
    got = core_swap(swap)
    dwq, dwk, dwv = call(output_kernel, (own, got), (f32(64, 256),) * 3)
    return dq, kg, vg, dwq, dwk, dwv, table[:, : rel_table.shape[1]]


def solution(mesh):
    torus = Mesh(mesh.devices.reshape(NZ, NX, -1, 2), SP + ("row", "core"))
    tp = ("row", "core")
    in_specs = (P(SP, None), P(None, tp), P(None, tp), P(None, tp), P(tp, None), P(SP, tp))
    out_specs = (P(SP, tp),) * 6 + (P(tp, None),)
    return jax.shard_map(staged, mesh=torus, in_specs=in_specs, out_specs=out_specs, check_vma=False)
```

```python
import jax
import jax.numpy as jnp
from jax import lax
from jax.experimental import pallas as pl
from jax.experimental.pallas import tpu as pltpu
from jax.sharding import Mesh
from jax.sharding import PartitionSpec as P


HDIM = 128
SEG = 64
PREV = 4
REACH = PREV * SEG
TILE = 128
BAND = REACH + TILE
SP = ("sp_0", "sp_1")
NZ, NX = 8, 4
ROWS = 64
EXTRA = 16
VMEM_LIMIT = 24 << 20
LOAD_LIMIT = 24 << 20
CHUNKS = 4
WIDTH = 2048 // CHUNKS
SCALE = HDIM ** (-0.5)
F32 = jnp.float32
BF16 = jnp.bfloat16


def odd_pair(i):
    return i ^ 1


def even_pair(n):
    return lambda i: (i + 1) % n if i % 2 else (i - 1) % n


XO, XE = ("sp_1", odd_pair), ("sp_1", even_pair(NX))
ZO, ZE = ("sp_0", odd_pair), ("sp_0", even_pair(NZ))
ZF = ("sp_0", lambda i: (i + NZ // 2) % NZ)
Z3 = ("sp_0", lambda i: (3, 6, 5, 0, 7, 2, 1, 4)[i])
OWN = ((XO, XE, ZO, ZE, Z3), (ZO, ZE, XO, XE, ZF))
OTHER = ((XE, XO, ZO, ZE, Z3), (ZE, ZO, XO, XE, ZF))


def held_order(steps, device):
    if not steps:
        return [device]
    return held_order(steps[1:], steps[0](device)) + held_order(steps[1:], device)


def axis_codes(levels, axis):
    n = NZ if axis == "sp_0" else NX
    mine = [f for a, f in levels if a == axis]
    spots = [len(levels) - 1 - i for i, (a, _) in enumerate(levels) if a == axis]
    wanted = [0] * n
    for device in range(n):
        order = held_order(mine, device)
        assert sorted(order) == list(range(n))
        for at, unit in enumerate(order):
            wanted[unit] |= at << (4 * device)
    me = lax.axis_index(axis)
    codes = []
    for packed in wanted:
        at = jnp.int32(0)
        for device in range(n):
            at = jnp.where(me == device, jnp.int32((packed >> (4 * device)) & 15), at)
        code = jnp.int32(0)
        for i, spot in enumerate(spots):
            code = code | (((at >> (len(spots) - 1 - i)) & 1) << spot)
        codes.append(code)
    return codes


def unit_places(sequences):
    core = lax.axis_index("core")
    places = []
    for levels in sequences:
        along_z, along_x = axis_codes(levels, "sp_0"), axis_codes(levels, "sp_1")
        places.append([along_z[unit // NX] + along_x[unit % NX] for unit in range(NZ * NX)])
    return [jnp.where(core == 0, a, b) for a, b in zip(*places)]


def level_route(sequences, level, across=0):
    route = []
    for core, levels in enumerate(sequences):
        axis, f = levels[level]
        for z in range(NZ):
            for x in range(NX):
                to = f(z) * NX + x if axis == "sp_0" else z * NX + f(x)
                route.append(((z * NX + x) * 2 + core, to * 2 + (core ^ across)))
    return route


def exchange(block, sequences, level, across=0):
    return lax.ppermute(block, SP + ("core",), level_route(sequences, level, across))


def core_swap(block):
    return lax.ppermute(block, "core", [(0, 1), (1, 0)])


def dot(a, b, contract=((1,), (0,))):
    return lax.dot_general(a, b, (contract, ((), ())), preferred_element_type=F32)


def tile_grads(query, grad, key, value, key_t, value_t, bias):
    scores = dot(key, query, ((1,), (1,))) * SCALE + bias
    top = jnp.max(scores, axis=0, keepdims=True)
    raised = jnp.exp(scores - top)
    probs = raised * (1.0 / jnp.sum(raised, axis=0, keepdims=True))
    probs_low = probs.astype(BF16)
    attn_out = dot(value_t, probs_low).astype(BF16).astype(F32)
    out_dot = jnp.sum(attn_out * grad.T.astype(F32), axis=0, keepdims=True)
    value_part = dot(probs_low, grad)
    score_grad = probs * (dot(value, grad, ((1,), (1,))) - out_dot)
    score_low = score_grad.astype(BF16)
    query_part = (dot(key_t, score_low) * SCALE).T
    key_part = dot(score_low, query) * SCALE
    return score_grad, query_part, key_part, value_part


def load_kernel(x_hbm, wq_hbm, wk_hbm, wv_hbm, tail_ref, x_ref, wq_ref, wk_ref, wv_ref, sem):
    top = 1024 - REACH
    pairs = (
        (wk_hbm, wk_ref), (wv_hbm, wv_ref), (x_hbm.at[top:], x_ref.at[top:]),
        (wq_hbm, wq_ref), (x_hbm.at[:top], x_ref.at[:top]),
    )
    copies = [pltpu.make_async_copy(src, dst, sem.at[i]) for i, (src, dst) in enumerate(pairs)]
    for copy in copies:
        copy.start()
    for copy in copies[:3]:
        copy.wait()
    x = x_ref[top:]
    tail_ref[:, :256] = dot(x, wk_ref[...]).astype(BF16)
    tail_ref[:, 256:] = dot(x, wv_ref[...]).astype(BF16)
    for copy in copies[3:]:
        copy.wait()


def proj_kernel(x_ref, wq_ref, wk_ref, wv_ref, q_ref, k_ref, v_ref):
    x = x_ref[...]
    q_ref[...] = dot(x, wq_ref[...]).astype(BF16)
    k_ref[...] = dot(x, wk_ref[...]).astype(BF16)
    v_ref[...] = dot(x, wv_ref[...]).astype(BF16)


def first_kernel(
    q_ref, k_ref, v_ref, halo_ref, og_ref, rel_ref,
    dq_ref, edge_ref, back_ref, bias_ref, pat_ref,
    k_s, v_s, kt_s, vt_s, ka_s, va_s,
):
    k_s[:REACH] = halo_ref[:, :256]
    v_s[:REACH] = halo_ref[:, 256:]
    k_s[REACH:] = k_ref[...]
    v_s[REACH:] = v_ref[...]
    kt_s[...] = k_s[...].T
    vt_s[...] = v_s[...].T
    ka_s[...] = jnp.zeros_like(ka_s)
    va_s[...] = jnp.zeros_like(va_s)
    outside = (lax.axis_index("sp_0") == 0) & (lax.axis_index("sp_1") == 0)
    u = lax.broadcasted_iota(jnp.int32, (BAND, TILE), 0)
    col = lax.broadcasted_iota(jnp.int32, (BAND, TILE), 1)
    low = jnp.where(col < SEG, 0, SEG)
    inside = (u >= low) & (u < low + REACH + SEG)
    for h in range(2):
        table = rel_ref[h : h + 1, :]
        far = jnp.concatenate([table[:, :256], jnp.broadcast_to(table[:, 256:257], (1, 256))], axis=1)
        far = jnp.broadcast_to(far, (BAND, 512))
        skew = pltpu.roll(far, 0, 1, stride=1, stride_axis=0)[:, BAND:]
        bias_ref[h] = jnp.where(inside, skew, -jnp.inf)
    for t in range(2):
        rows = slice(t * TILE, (t + 1) * TILE)
        band = slice(t * TILE, t * TILE + BAND)
        for h in range(2):
            cols = slice(h * HDIM, (h + 1) * HDIM)
            bias = jnp.where(outside & (u < REACH - t * TILE), -jnp.inf, bias_ref[h])
            score_grad, query_part, key_part, value_part = tile_grads(
                q_ref[rows, cols], og_ref[rows, cols], k_s[band, cols], v_s[band, cols],
                kt_s[cols, band], vt_s[cols, band], bias,
            )
            if t == 0:
                pat_ref[h] = score_grad
            else:
                pat_ref[h] += score_grad
            dq_ref[rows, cols] = query_part.astype(BF16)
            ka_s[band, cols] += key_part
            va_s[band, cols] += value_part
    edge_ref[:, :256] = ka_s[REACH:]
    edge_ref[:, 256:] = va_s[REACH:]
    back_ref[:, :256] = ka_s[:REACH].astype(BF16)
    back_ref[:, 256:] = va_s[:REACH].astype(BF16)


def attn_kernel(
    q_ref, k_ref, v_ref, og_ref, bias_ref, pat_in, edge_in, dq_in,
    dq_ref, near_ref, kg_ref, vg_ref, edge_ref, pat_ref,
    kt_s, vt_s, ka_s, va_s,
):
    kt_s[...] = k_ref[...].T
    vt_s[...] = v_ref[...].T
    ka_s[:REACH] = edge_in[:, :256]
    va_s[:REACH] = edge_in[:, 256:]
    ka_s[REACH:] = jnp.zeros((768, 256), F32)
    va_s[REACH:] = jnp.zeros((768, 256), F32)
    pat_ref[...] = pat_in[...]
    near_ref[:REACH] = dq_in[...]
    for tile in range(6):
        rows = slice(REACH + tile * TILE, REACH + (tile + 1) * TILE)
        band = slice(tile * TILE, tile * TILE + BAND)
        for h in range(2):
            cols = slice(h * HDIM, (h + 1) * HDIM)
            score_grad, query_part, key_part, value_part = tile_grads(
                q_ref[rows, cols], og_ref[rows, cols], k_ref[band, cols], v_ref[band, cols],
                kt_s[cols, band], vt_s[cols, band], bias_ref[h],
            )
            pat_ref[h] += score_grad
            near_ref[rows, cols] = query_part.astype(BF16)
            ka_s[band, cols] += key_part
            va_s[band, cols] += value_part
    dq_ref[...] = near_ref[...]
    kg_ref[...] = ka_s[:768].astype(BF16)
    vg_ref[...] = va_s[:768].astype(BF16)
    edge_ref[:, :256] = ka_s[768:]
    edge_ref[:, 256:] = va_s[768:]


def finish_kernel(kg_in, vg_in, edge_ref, back_ref, dq_ref, kg_ref, vg_ref, own_ref, swap_ref):
    kg_ref[:768] = kg_in[...]
    vg_ref[:768] = vg_in[...]
    kg_ref[768:] = (edge_ref[:, :256] + back_ref[:, :256].astype(F32)).astype(BF16)
    vg_ref[768:] = (edge_ref[:, 256:] + back_ref[:, 256:].astype(F32)).astype(BF16)
    core = lax.axis_index("core")

    @pl.when(core == 0)
    def _():
        own_ref[:, :256] = kg_ref[...]
        own_ref[:, 256:] = dq_ref[:, :128]
        swap_ref[:, :256] = vg_ref[...]
        swap_ref[:, 256:] = dq_ref[:, 128:]

    @pl.when(core == 1)
    def _():
        own_ref[:, :256] = vg_ref[...]
        own_ref[:, 256:] = dq_ref[:, 128:]
        swap_ref[:, :256] = kg_ref[...]
        swap_ref[:, 256:] = dq_ref[:, :128]


def store_units(value, chunk, places, out_s):
    units = WIDTH // ROWS
    for i in range(units):
        at = pl.multiple_of(places[chunk * units + i] * ROWS, ROWS)
        out_s[pl.ds(at, ROWS), :] = value[i * ROWS : (i + 1) * ROWS].astype(BF16)


def placed_product(x_ref, grad_ref, sequences, out_s):
    places = unit_places(sequences)
    for c in range(CHUNKS):
        cols = slice(c * WIDTH, (c + 1) * WIDTH)
        store_units(dot(x_ref[:, cols], grad_ref[...], ((0,), (0,))), c, places, out_s)


def three_parts(table):
    high = table.astype(BF16).astype(F32)
    mid = (table - high).astype(BF16).astype(F32)
    low = table - high - mid
    rest = jnp.zeros((EXTRA - 6, table.shape[1]), F32)
    return jnp.concatenate([high, mid, low, rest], axis=0).astype(BF16)


def table_of(parts):
    parts = parts.astype(F32)
    return parts[0:2] + parts[2:4] + parts[4:6]


def copy_out(pairs, sem):
    copies = [pltpu.make_async_copy(src, dst, sem.at[i]) for i, (src, dst) in enumerate(pairs)]
    for copy in copies:
        copy.start()
    for copy in copies:
        copy.wait()


def own_kernel(x_ref, grad_ref, pat_ref, send_hbm, keep_hbm, table_ref, out_s, parts_s, diag_s, sem):
    placed_product(x_ref, grad_ref, OWN, out_s)
    for h in range(2):
        diag_s[...] = jnp.zeros_like(diag_s)
        for a in range(BAND // 8):
            off = BAND - 8 * a
            diag_s[:, off : off + TILE] += pat_ref[h, 8 * a : 8 * a + 8, :]
        total = jnp.zeros((1, 512), F32)
        for s in range(8):
            total += diag_s[s : s + 1, s : s + 512]
        far = jnp.sum(total[:, 256:], axis=1, keepdims=True)
        table_ref[h : h + 1, :256] = total[:, :256]
        table_ref[h : h + 1, 256:] = jnp.broadcast_to(far, (1, 128))
    parts_s[...] = three_parts(table_ref[...])
    copy_out(
        [(out_s.at[:1024], send_hbm.at[:1024]), (parts_s, send_hbm.at[1024:]), (out_s.at[1024:], keep_hbm)],
        sem,
    )


def other_kernel(x_ref, grad_ref, send_hbm, keep_hbm, out_s, sem):
    placed_product(x_ref, grad_ref, OTHER, out_s)
    copy_out([(out_s.at[:1024], send_hbm), (out_s.at[1024:], keep_hbm)], sem)


def added(keep, got):
    return keep.astype(F32) + got.astype(F32)


def level_kernel(keep_ref, got_ref, table_in, send_ref, next_ref, table_ref):
    half = next_ref.shape[0]
    n = 2 * half
    total = table_in[...] + table_of(got_ref[n:, :384])
    table_ref[...] = total
    send_ref[:half] = added(keep_ref[:half], got_ref[:half]).astype(BF16)
    next_ref[...] = added(keep_ref[half:], got_ref[half:n]).astype(BF16)
    send_ref[half:, :384] = three_parts(total)
    if send_ref.shape[1] > 384:
        send_ref[half:, 384:] = jnp.zeros((EXTRA, send_ref.shape[1] - 384), BF16)


def merge_kernel(keep_ref, got_ref, keep2_ref, got2_ref, table_in, send_ref, next_ref, table_ref):
    half = next_ref.shape[0]
    n = 2 * half
    total = table_in[...] + table_of(got_ref[n:])
    table_ref[...] = total
    send_ref[:half, :384] = added(keep_ref[:half], got_ref[:half]).astype(BF16)
    send_ref[:half, 384:] = added(keep2_ref[:half], got2_ref[:half]).astype(BF16)
    next_ref[:, :384] = added(keep_ref[half:], got_ref[half:n]).astype(BF16)
    next_ref[:, 384:] = added(keep2_ref[half:], got2_ref[half:]).astype(BF16)
    send_ref[half:, :384] = three_parts(total)
    send_ref[half:, 384:] = jnp.zeros((EXTRA, 384), BF16)


def split_kernel(keep_ref, got_ref, table_in, one_ref, two_ref, three_ref, own_ref, table_ref):
    n = own_ref.shape[0]
    total = table_in[...] + table_of(got_ref[2 * n :, :384])
    table_ref[...] = total
    far = added(keep_ref[:n], got_ref[:n])
    one_ref[:n] = far[:, :384].astype(BF16)
    one_ref[n:] = three_parts(total)
    two_ref[...] = far[:, 384:].astype(BF16)
    near = added(keep_ref[n:], got_ref[n : 2 * n])
    own_ref[...] = near[:, :384]
    three_ref[...] = near[:, 384:]


def output_kernel(own_ref, one_ref, two_ref, three_ref, table_in, q_ref, k_ref, v_ref, table_ref):
    core = lax.axis_index("core")
    n = own_ref.shape[0]
    table = table_in[...] + table_of(one_ref[n:])
    table_ref[...] = table[:, : table_ref.shape[1]]
    own = own_ref[...] + one_ref[:n].astype(F32)
    got = three_ref[...] + two_ref[...].astype(F32)

    @pl.when(core == 0)
    def _():
        k_ref[...] = own[:, :256]
        v_ref[...] = got[:, :256]
        q_ref[:, :128] = own[:, 256:]
        q_ref[:, 128:] = got[:, 256:]

    @pl.when(core == 1)
    def _():
        v_ref[...] = own[:, :256]
        k_ref[...] = got[:, :256]
        q_ref[:, 128:] = own[:, 256:]
        q_ref[:, :128] = got[:, 256:]


def sds(shape, dtype):
    return jax.ShapeDtypeStruct(shape, dtype)


def whole(shape):
    return pl.BlockSpec(shape, lambda *_: (0,) * len(shape))


def cost(flops, byte_count):
    return pl.CostEstimate(flops=flops, bytes_accessed=byte_count, transcendentals=0)


def params(limit=None):
    return pltpu.CompilerParams(dimension_semantics=("arbitrary",), vmem_limit_bytes=limit or VMEM_LIMIT)


def call(kernel, operands, outs, scratch=(), grid=(1,), flops=1 << 20, blocks=None, any_outs=(), any_ins=(), limit=None):
    specs = [pl.BlockSpec(memory_space=pltpu.HBM) if i in any_ins else whole(x.shape) for i, x in enumerate(operands)]
    for at, shape in (blocks or {}).items():
        specs[at] = whole(shape)
    out_specs = [pl.BlockSpec(memory_space=pl.ANY) if i in any_outs else whole(x.shape) for i, x in enumerate(outs)]
    moved = sum(x.size * x.dtype.itemsize for x in (*operands, *outs))
    return pl.pallas_call(
        kernel,
        grid=grid,
        in_specs=specs,
        out_specs=out_specs,
        out_shape=list(outs),
        scratch_shapes=list(scratch),
        compiler_params=params(limit),
        cost_estimate=cost(flops, moved),
    )(*operands)


def neighbour(block, distance):
    count = NZ * NX
    route = [(i, i + distance) for i in range(count) if 0 <= i + distance < count]
    return lax.ppermute(block, SP, route)


def staged(inputs, w_query, w_key, w_value, rel_table, out_grad):
    f32, b16 = (lambda *s: sds(s, F32)), (lambda *s: sds(s, BF16))
    v32, v16 = (lambda *s: pltpu.VMEM(s, F32)), (lambda *s: pltpu.VMEM(s, BF16))
    tile_flops = 6 * 2 * TILE * BAND * HDIM
    tail, x, wq, wk, wv = call(
        load_kernel, (inputs, w_query, w_key, w_value),
        (b16(REACH, 512), b16(1024, 2048), b16(2048, 256), b16(2048, 256), b16(2048, 256)),
        (pltpu.SemaphoreType.DMA((5,)),), flops=2 * 256 * 2048 * 512, any_ins=(0, 1, 2, 3), limit=LOAD_LIMIT,
    )
    halo = neighbour(tail, 1)
    query, key, value = call(
        proj_kernel, (x, wq, wk, wv), (b16(1024, 256),) * 3,
        flops=2 * 1024 * 2048 * 768,
    )
    block = (REACH, 256)
    dq0, edge, back, bias, pat = call(
        first_kernel, (query, key, value, halo, out_grad, rel_table),
        (b16(REACH, 256), f32(REACH, 512), b16(REACH, 512), f32(2, BAND, TILE), f32(2, BAND, TILE)),
        (v16(512, 256), v16(512, 256), v16(256, 512), v16(256, 512), v32(512, 256), v32(512, 256)),
        flops=4 * tile_flops, blocks={0: block, 1: block, 2: block, 4: block},
    )
    back = neighbour(back, -1)
    dq, near, kg, vg, edge, pat = call(
        attn_kernel, (query, key, value, out_grad, bias, pat, edge, dq0),
        (b16(1024, 256), b16(1024, 256), b16(768, 256), b16(768, 256), f32(REACH, 512), f32(2, BAND, TILE)),
        (v16(256, 1024), v16(256, 1024), v32(1024, 256), v32(1024, 256)),
        flops=12 * tile_flops,
    )
    kg, vg, own, swap = call(finish_kernel, (kg, vg, edge, back, near), (b16(1024, 256),) * 2 + (b16(1024, 384),) * 2)
    got = core_swap(swap)
    sem = pltpu.SemaphoreType.DMA((3,))
    product = 2 * 1024 * 2048 * 384
    send, keep, table = call(
        own_kernel, (x, own, pat), (b16(1024 + EXTRA, 384), b16(1024, 384), f32(2, 384)),
        (v16(2048, 384), v16(EXTRA, 384), v32(8, 640), sem), flops=product, any_outs=(0, 1),
    )
    send2, keep2 = call(
        other_kernel, (x, got), (b16(1024, 384),) * 2, (v16(2048, 384), sem),
        flops=product, any_outs=(0, 1),
    )
    got = exchange(send, OWN, 0)
    got2 = exchange(send2, OTHER, 0)
    send, keep, table = call(level_kernel, (keep, got, table), (b16(512 + EXTRA, 384), b16(512, 384), f32(2, 384)))
    got = exchange(send, OWN, 1)
    send2, keep2 = added(keep2[:512], got2[:512]).astype(BF16), added(keep2[512:], got2[512:]).astype(BF16)
    got2 = exchange(send2, OTHER, 1)
    send, keep, table = call(
        merge_kernel, (keep, got, keep2, got2, table), (b16(256 + EXTRA, 768), b16(256, 768), f32(2, 384))
    )
    got = exchange(send, OWN, 2)
    send, keep, table = call(level_kernel, (keep, got, table), (b16(128 + EXTRA, 768), b16(128, 768), f32(2, 384)))
    got = exchange(send, OWN, 3)
    one, two, three, own, table = call(
        split_kernel, (keep, got, table),
        (b16(64 + EXTRA, 384), b16(64, 384), f32(64, 384), f32(64, 384), f32(2, 384)),
    )
    one = exchange(one, OWN, 4)
    two = exchange(two, OWN, 4, across=1)
    three = core_swap(three)
    dwq, dwk, dwv, table = call(
        output_kernel, (own, one, two, three, table), (f32(64, 256),) * 3 + (f32(*rel_table.shape),)
    )
    return dq, kg, vg, dwq, dwk, dwv, table


def solution(mesh):
    torus = Mesh(mesh.devices.reshape(NZ, NX, -1, 2), SP + ("row", "core"))
    tp = ("row", "core")
    in_specs = (P(SP, None), P(None, tp), P(None, tp), P(None, tp), P(tp, None), P(SP, tp))
    out_specs = (P(SP, tp),) * 6 + (P(tp, None),)
    return jax.shard_map(staged, mesh=torus, in_specs=in_specs, out_specs=out_specs, check_vma=False)
```

```python
import jax
import jax.numpy as jnp
from jax import lax
from jax.experimental import pallas as pl
from jax.experimental.pallas import tpu as pltpu
from jax.sharding import Mesh
from jax.sharding import PartitionSpec as P


HDIM = 128
SEG = 64
PREV = 4
REACH = PREV * SEG
TILE = 128
BAND = REACH + TILE
SP = ("sp_0", "sp_1")
NZ, NX = 8, 4
ROWS = 64
EXTRA = 16
VMEM_LIMIT = 24 << 20
LOAD_LIMIT = 24 << 20
CHUNKS = 4
WIDTH = 2048 // CHUNKS
SCALE = HDIM ** (-0.5)
F32 = jnp.float32
BF16 = jnp.bfloat16


def odd_pair(i):
    return i ^ 1


def even_pair(n):
    return lambda i: (i + 1) % n if i % 2 else (i - 1) % n


XO, XE = ("sp_1", odd_pair), ("sp_1", even_pair(NX))
ZO, ZE = ("sp_0", odd_pair), ("sp_0", even_pair(NZ))
ZF = ("sp_0", lambda i: (i + NZ // 2) % NZ)
Z3 = ("sp_0", lambda i: (3, 6, 5, 0, 7, 2, 1, 4)[i])
OWN = ((XO, XE, ZO, ZE, Z3), (ZO, ZE, XO, XE, ZF))
OTHER = ((XE, XO, ZO, ZE, Z3), (ZE, ZO, XO, XE, ZF))


def held_order(steps, device):
    if not steps:
        return [device]
    return held_order(steps[1:], steps[0](device)) + held_order(steps[1:], device)


def axis_codes(levels, axis):
    n = NZ if axis == "sp_0" else NX
    mine = [f for a, f in levels if a == axis]
    spots = [len(levels) - 1 - i for i, (a, _) in enumerate(levels) if a == axis]
    wanted = [0] * n
    for device in range(n):
        order = held_order(mine, device)
        assert sorted(order) == list(range(n))
        for at, unit in enumerate(order):
            wanted[unit] |= at << (4 * device)
    me = lax.axis_index(axis)
    codes = []
    for packed in wanted:
        at = jnp.int32(0)
        for device in range(n):
            at = jnp.where(me == device, jnp.int32((packed >> (4 * device)) & 15), at)
        code = jnp.int32(0)
        for i, spot in enumerate(spots):
            code = code | (((at >> (len(spots) - 1 - i)) & 1) << spot)
        codes.append(code)
    return codes


def unit_places(sequences):
    core = lax.axis_index("core")
    places = []
    for levels in sequences:
        along_z, along_x = axis_codes(levels, "sp_0"), axis_codes(levels, "sp_1")
        places.append([along_z[unit // NX] + along_x[unit % NX] for unit in range(NZ * NX)])
    return [jnp.where(core == 0, a, b) for a, b in zip(*places)]


def level_route(sequences, steps, across=0):
    route = []
    for core, levels in enumerate(sequences):
        for z in range(NZ):
            for x in range(NX):
                at = {"sp_0": z, "sp_1": x}
                for step in steps:
                    axis, f = levels[step]
                    at[axis] = f(at[axis])
                to = at["sp_0"] * NX + at["sp_1"]
                route.append(((z * NX + x) * 2 + core, to * 2 + (core ^ across)))
    return route


def exchange(block, sequences, steps, across=0):
    return lax.ppermute(block, SP + ("core",), level_route(sequences, steps, across))


def exchange_quarters(blocks, sequences, level):
    paths = ((level, level + 1), (level,), (level + 1,))
    return [exchange(x, sequences, path) for x, path in zip(blocks, paths)]


def core_swap(block):
    return lax.ppermute(block, "core", [(0, 1), (1, 0)])


def dot(a, b, contract=((1,), (0,))):
    return lax.dot_general(a, b, (contract, ((), ())), preferred_element_type=F32)


def tile_grads(query, grad, key, value, key_t, value_t, bias):
    scores = dot(key, query, ((1,), (1,))) * SCALE + bias
    top = jnp.max(scores, axis=0, keepdims=True)
    raised = jnp.exp(scores - top)
    probs = raised * (1.0 / jnp.sum(raised, axis=0, keepdims=True))
    probs_low = probs.astype(BF16)
    attn_out = dot(value_t, probs_low).astype(BF16).astype(F32)
    out_dot = jnp.sum(attn_out * grad.T.astype(F32), axis=0, keepdims=True)
    value_part = dot(probs_low, grad)
    score_grad = probs * (dot(value, grad, ((1,), (1,))) - out_dot)
    score_low = score_grad.astype(BF16)
    query_part = (dot(key_t, score_low) * SCALE).T
    key_part = dot(score_low, query) * SCALE
    return score_grad, query_part, key_part, value_part


def load_kernel(x_hbm, wq_hbm, wk_hbm, wv_hbm, tail_ref, x_ref, wq_ref, wk_ref, wv_ref, sem):
    top = 1024 - REACH
    pairs = (
        (wk_hbm, wk_ref), (wv_hbm, wv_ref), (x_hbm.at[top:], x_ref.at[top:]),
        (wq_hbm, wq_ref), (x_hbm.at[:top], x_ref.at[:top]),
    )
    copies = [pltpu.make_async_copy(src, dst, sem.at[i]) for i, (src, dst) in enumerate(pairs)]
    for copy in copies:
        copy.start()
    for copy in copies[:3]:
        copy.wait()
    x = x_ref[top:]
    tail_ref[:, :256] = dot(x, wk_ref[...]).astype(BF16)
    tail_ref[:, 256:] = dot(x, wv_ref[...]).astype(BF16)
    for copy in copies[3:]:
        copy.wait()


def proj_kernel(x_ref, wq_ref, wk_ref, wv_ref, q_ref, k_ref, v_ref):
    x = x_ref[...]
    q_ref[...] = dot(x, wq_ref[...]).astype(BF16)
    k_ref[...] = dot(x, wk_ref[...]).astype(BF16)
    v_ref[...] = dot(x, wv_ref[...]).astype(BF16)


def first_kernel(
    q_ref, k_ref, v_ref, halo_ref, og_ref, rel_ref,
    dq_ref, edge_ref, back_ref, bias_ref, pat_ref,
    k_s, v_s, kt_s, vt_s, ka_s, va_s,
):
    k_s[:REACH] = halo_ref[:, :256]
    v_s[:REACH] = halo_ref[:, 256:]
    k_s[REACH:] = k_ref[...]
    v_s[REACH:] = v_ref[...]
    kt_s[...] = k_s[...].T
    vt_s[...] = v_s[...].T
    ka_s[...] = jnp.zeros_like(ka_s)
    va_s[...] = jnp.zeros_like(va_s)
    outside = (lax.axis_index("sp_0") == 0) & (lax.axis_index("sp_1") == 0)
    u = lax.broadcasted_iota(jnp.int32, (BAND, TILE), 0)
    col = lax.broadcasted_iota(jnp.int32, (BAND, TILE), 1)
    low = jnp.where(col < SEG, 0, SEG)
    inside = (u >= low) & (u < low + REACH + SEG)
    for h in range(2):
        table = rel_ref[h : h + 1, :]
        far = jnp.concatenate([table[:, :256], jnp.broadcast_to(table[:, 256:257], (1, 256))], axis=1)
        far = jnp.broadcast_to(far, (BAND, 512))
        skew = pltpu.roll(far, 0, 1, stride=1, stride_axis=0)[:, BAND:]
        bias_ref[h] = jnp.where(inside, skew, -jnp.inf)
    for t in range(2):
        rows = slice(t * TILE, (t + 1) * TILE)
        band = slice(t * TILE, t * TILE + BAND)
        for h in range(2):
            cols = slice(h * HDIM, (h + 1) * HDIM)
            bias = jnp.where(outside & (u < REACH - t * TILE), -jnp.inf, bias_ref[h])
            score_grad, query_part, key_part, value_part = tile_grads(
                q_ref[rows, cols], og_ref[rows, cols], k_s[band, cols], v_s[band, cols],
                kt_s[cols, band], vt_s[cols, band], bias,
            )
            if t == 0:
                pat_ref[h] = score_grad
            else:
                pat_ref[h] += score_grad
            dq_ref[rows, cols] = query_part.astype(BF16)
            ka_s[band, cols] += key_part
            va_s[band, cols] += value_part
    edge_ref[:, :256] = ka_s[REACH:]
    edge_ref[:, 256:] = va_s[REACH:]
    back_ref[:, :256] = ka_s[:REACH].astype(BF16)
    back_ref[:, 256:] = va_s[:REACH].astype(BF16)


def attn_kernel(
    q_ref, k_ref, v_ref, og_ref, bias_ref, pat_in, edge_in, dq_in,
    dq_ref, near_ref, kg_ref, vg_ref, edge_ref, pat_ref,
    kt_s, vt_s, ka_s, va_s,
):
    kt_s[...] = k_ref[...].T
    vt_s[...] = v_ref[...].T
    ka_s[:REACH] = edge_in[:, :256]
    va_s[:REACH] = edge_in[:, 256:]
    ka_s[REACH:] = jnp.zeros((768, 256), F32)
    va_s[REACH:] = jnp.zeros((768, 256), F32)
    pat_ref[...] = pat_in[...]
    near_ref[:REACH] = dq_in[...]
    for tile in range(6):
        rows = slice(REACH + tile * TILE, REACH + (tile + 1) * TILE)
        band = slice(tile * TILE, tile * TILE + BAND)
        for h in range(2):
            cols = slice(h * HDIM, (h + 1) * HDIM)
            score_grad, query_part, key_part, value_part = tile_grads(
                q_ref[rows, cols], og_ref[rows, cols], k_ref[band, cols], v_ref[band, cols],
                kt_s[cols, band], vt_s[cols, band], bias_ref[h],
            )
            pat_ref[h] += score_grad
            near_ref[rows, cols] = query_part.astype(BF16)
            ka_s[band, cols] += key_part
            va_s[band, cols] += value_part
    dq_ref[...] = near_ref[...]
    kg_ref[...] = ka_s[:768].astype(BF16)
    vg_ref[...] = va_s[:768].astype(BF16)
    edge_ref[:, :256] = ka_s[768:]
    edge_ref[:, 256:] = va_s[768:]


def finish_kernel(kg_in, vg_in, edge_ref, back_ref, dq_ref, kg_ref, vg_ref, own_ref, swap_ref):
    kg_ref[:768] = kg_in[...]
    vg_ref[:768] = vg_in[...]
    kg_ref[768:] = (edge_ref[:, :256] + back_ref[:, :256].astype(F32)).astype(BF16)
    vg_ref[768:] = (edge_ref[:, 256:] + back_ref[:, 256:].astype(F32)).astype(BF16)
    core = lax.axis_index("core")

    @pl.when(core == 0)
    def _():
        own_ref[:, :256] = kg_ref[...]
        own_ref[:, 256:] = dq_ref[:, :128]
        swap_ref[:, :256] = vg_ref[...]
        swap_ref[:, 256:] = dq_ref[:, 128:]

    @pl.when(core == 1)
    def _():
        own_ref[:, :256] = vg_ref[...]
        own_ref[:, 256:] = dq_ref[:, 128:]
        swap_ref[:, :256] = kg_ref[...]
        swap_ref[:, 256:] = dq_ref[:, :128]


def store_units(value, chunk, places, out_s):
    units = WIDTH // ROWS
    for i in range(units):
        at = pl.multiple_of(places[chunk * units + i] * ROWS, ROWS)
        out_s[pl.ds(at, ROWS), :] = value[i * ROWS : (i + 1) * ROWS].astype(BF16)


def placed_product(x_ref, grad_ref, sequences, out_s):
    places = unit_places(sequences)
    for c in range(CHUNKS):
        cols = slice(c * WIDTH, (c + 1) * WIDTH)
        store_units(dot(x_ref[:, cols], grad_ref[...], ((0,), (0,))), c, places, out_s)


def three_parts(table):
    high = table.astype(BF16).astype(F32)
    mid = (table - high).astype(BF16).astype(F32)
    low = table - high - mid
    rest = jnp.zeros((EXTRA - 6, table.shape[1]), F32)
    return jnp.concatenate([high, mid, low, rest], axis=0).astype(BF16)


def table_of(parts):
    parts = parts.astype(F32)
    return parts[0:2] + parts[2:4] + parts[4:6]


def copy_out(pairs, sem):
    copies = [pltpu.make_async_copy(src, dst, sem.at[i]) for i, (src, dst) in enumerate(pairs)]
    for copy in copies:
        copy.start()
    for copy in copies:
        copy.wait()


def own_kernel(x_ref, grad_ref, m0_hbm, m1_hbm, m2_hbm, keep_hbm, out_s, sem):
    placed_product(x_ref, grad_ref, OWN, out_s)
    copy_out([(out_s.at[512 * i : 512 * (i + 1)], m) for i, m in enumerate((m0_hbm, m1_hbm, m2_hbm, keep_hbm))], sem)


def other_kernel(
    x_ref, grad_ref, pat_ref, m0_hbm, m1_hbm, m2_hbm, keep_hbm, table_ref, out_s, parts_s, diag_s, sem
):
    placed_product(x_ref, grad_ref, OTHER, out_s)
    for h in range(2):
        diag_s[...] = jnp.zeros_like(diag_s)
        for a in range(BAND // 8):
            off = BAND - 8 * a
            diag_s[:, off : off + TILE] += pat_ref[h, 8 * a : 8 * a + 8, :]
        total = jnp.zeros((1, 512), F32)
        for s in range(8):
            total += diag_s[s : s + 1, s : s + 512]
        far = jnp.sum(total[:, 256:], axis=1, keepdims=True)
        table_ref[h : h + 1, :256] = total[:, :256]
        table_ref[h : h + 1, 256:] = jnp.broadcast_to(far, (1, 128))
    parts_s[...] = three_parts(table_ref[...])
    pairs = [(out_s.at[1536:], keep_hbm)]
    for i, m in enumerate((m0_hbm, m1_hbm, m2_hbm)):
        pairs += [(out_s.at[512 * i : 512 * (i + 1)], m.at[:512]), (parts_s, m.at[512:])]
    copy_out(pairs, sem)


def summed(keep_ref, got_refs, rows):
    total = keep_ref[rows].astype(F32)
    for got in got_refs:
        total += got[rows].astype(F32)
    return total


def summed_table(table_in, got_refs, n):
    total = table_in[...]
    for got in got_refs:
        total += table_of(got[n:, :384])
    return total


def merge_kernel(
    keep_ref, a0, a1, a2, keep2_ref, b0, b1, b2, table_in, m0_ref, m1_ref, m2_ref, next_ref, table_ref
):
    total = summed_table(table_in, (b0, b1, b2), 512)
    table_ref[...] = total
    parts = three_parts(total)
    for i, out in enumerate((m0_ref, m1_ref, m2_ref, next_ref)):
        rows = slice(128 * i, 128 * (i + 1))
        out[:128, :384] = summed(keep_ref, (a0, a1, a2), rows).astype(BF16)
        out[:128, 384:] = summed(keep2_ref, (b0, b1, b2), rows).astype(BF16)
        if i < 3:
            out[128:, :384] = parts
            out[128:, 384:] = jnp.zeros((EXTRA, 384), BF16)


def split_kernel(keep_ref, g0, g1, g2, table_in, one_ref, two_ref, three_ref, own_ref, table_ref):
    n = own_ref.shape[0]
    total = summed_table(table_in, (g0, g1, g2), 2 * n)
    table_ref[...] = total
    far = summed(keep_ref, (g0, g1, g2), slice(0, n))
    one_ref[:n] = far[:, :384].astype(BF16)
    one_ref[n:] = three_parts(total)
    two_ref[...] = far[:, 384:].astype(BF16)
    near = summed(keep_ref, (g0, g1, g2), slice(n, 2 * n))
    own_ref[...] = near[:, :384]
    three_ref[...] = near[:, 384:]


def output_kernel(own_ref, one_ref, two_ref, three_ref, table_in, q_ref, k_ref, v_ref, table_ref):
    core = lax.axis_index("core")
    n = own_ref.shape[0]
    table = table_in[...] + table_of(one_ref[n:])
    table_ref[...] = table[:, : table_ref.shape[1]]
    own = own_ref[...] + one_ref[:n].astype(F32)
    got = three_ref[...] + two_ref[...].astype(F32)

    @pl.when(core == 0)
    def _():
        k_ref[...] = own[:, :256]
        v_ref[...] = got[:, :256]
        q_ref[:, :128] = own[:, 256:]
        q_ref[:, 128:] = got[:, 256:]

    @pl.when(core == 1)
    def _():
        v_ref[...] = own[:, :256]
        k_ref[...] = got[:, :256]
        q_ref[:, 128:] = own[:, 256:]
        q_ref[:, :128] = got[:, 256:]


def sds(shape, dtype):
    return jax.ShapeDtypeStruct(shape, dtype)


def whole(shape):
    return pl.BlockSpec(shape, lambda *_: (0,) * len(shape))


def cost(flops, byte_count):
    return pl.CostEstimate(flops=flops, bytes_accessed=byte_count, transcendentals=0)


def params(limit=None):
    return pltpu.CompilerParams(dimension_semantics=("arbitrary",), vmem_limit_bytes=limit or VMEM_LIMIT)


def call(kernel, operands, outs, scratch=(), grid=(1,), flops=1 << 20, blocks=None, any_outs=(), any_ins=(), limit=None):
    specs = [pl.BlockSpec(memory_space=pltpu.HBM) if i in any_ins else whole(x.shape) for i, x in enumerate(operands)]
    for at, shape in (blocks or {}).items():
        specs[at] = whole(shape)
    out_specs = [pl.BlockSpec(memory_space=pl.ANY) if i in any_outs else whole(x.shape) for i, x in enumerate(outs)]
    moved = sum(x.size * x.dtype.itemsize for x in (*operands, *outs))
    return pl.pallas_call(
        kernel,
        grid=grid,
        in_specs=specs,
        out_specs=out_specs,
        out_shape=list(outs),
        scratch_shapes=list(scratch),
        compiler_params=params(limit),
        cost_estimate=cost(flops, moved),
    )(*operands)


def neighbour(block, distance):
    count = NZ * NX
    route = [(i, i + distance) for i in range(count) if 0 <= i + distance < count]
    return lax.ppermute(block, SP, route)


def staged(inputs, w_query, w_key, w_value, rel_table, out_grad):
    f32, b16 = (lambda *s: sds(s, F32)), (lambda *s: sds(s, BF16))
    v32, v16 = (lambda *s: pltpu.VMEM(s, F32)), (lambda *s: pltpu.VMEM(s, BF16))
    tile_flops = 6 * 2 * TILE * BAND * HDIM
    in_hbm = tuple(pltpu.with_memory_space_constraint(v, pltpu.HBM) for v in (inputs, w_query, w_key, w_value))
    tail, x, wq, wk, wv = call(
        load_kernel, in_hbm,
        (b16(REACH, 512), b16(1024, 2048), b16(2048, 256), b16(2048, 256), b16(2048, 256)),
        (pltpu.SemaphoreType.DMA((5,)),), flops=2 * 256 * 2048 * 512, any_ins=(0, 1, 2, 3), limit=LOAD_LIMIT,
    )
    halo = neighbour(tail, 1)
    query, key, value = call(
        proj_kernel, (x, wq, wk, wv), (b16(1024, 256),) * 3,
        flops=2 * 1024 * 2048 * 768,
    )
    block = (REACH, 256)
    dq0, edge, back, bias, pat = call(
        first_kernel, (query, key, value, halo, out_grad, rel_table),
        (b16(REACH, 256), f32(REACH, 512), b16(REACH, 512), f32(2, BAND, TILE), f32(2, BAND, TILE)),
        (v16(512, 256), v16(512, 256), v16(256, 512), v16(256, 512), v32(512, 256), v32(512, 256)),
        flops=4 * tile_flops, blocks={0: block, 1: block, 2: block, 4: block},
    )
    back = neighbour(back, -1)
    dq, near, kg, vg, edge, pat = call(
        attn_kernel, (query, key, value, out_grad, bias, pat, edge, dq0),
        (b16(1024, 256), b16(1024, 256), b16(768, 256), b16(768, 256), f32(REACH, 512), f32(2, BAND, TILE)),
        (v16(256, 1024), v16(256, 1024), v32(1024, 256), v32(1024, 256)),
        flops=12 * tile_flops,
    )
    kg, vg, own, swap = call(finish_kernel, (kg, vg, edge, back, near), (b16(1024, 256),) * 2 + (b16(1024, 384),) * 2)
    got = core_swap(swap)
    product = 2 * 1024 * 2048 * 384
    *send, keep = call(
        own_kernel, (x, own), (b16(512, 384),) * 4,
        (v16(2048, 384), pltpu.SemaphoreType.DMA((4,))), flops=product, any_outs=(0, 1, 2, 3),
    )
    *send2, keep2, table = call(
        other_kernel, (x, got, pat), (b16(512 + EXTRA, 384),) * 3 + (b16(512, 384), f32(2, 384)),
        (v16(2048, 384), v16(EXTRA, 384), v32(8, 640), pltpu.SemaphoreType.DMA((7,))),
        flops=product, any_outs=(0, 1, 2, 3),
    )
    a = exchange_quarters(send, OWN, 0)
    b = exchange_quarters(send2, OTHER, 0)
    *send, keep, table = call(
        merge_kernel, (keep, *a, keep2, *b, table),
        (b16(128 + EXTRA, 768),) * 3 + (b16(128, 768), f32(2, 384)),
    )
    c = exchange_quarters(send, OWN, 2)
    one, two, three, own, table = call(
        split_kernel, (keep, *c, table),
        (b16(64 + EXTRA, 384), b16(64, 384), f32(64, 384), f32(64, 384), f32(2, 384)),
    )
    one = exchange(one, OWN, (4,))
    two = exchange(two, OWN, (4,), across=1)
    three = core_swap(three)
    dwq, dwk, dwv, table = call(
        output_kernel, (own, one, two, three, table), (f32(64, 256),) * 3 + (f32(*rel_table.shape),)
    )
    return dq, kg, vg, dwq, dwk, dwv, table


def solution(mesh):
    torus = Mesh(mesh.devices.reshape(NZ, NX, -1, 2), SP + ("row", "core"))
    tp = ("row", "core")
    in_specs = (P(SP, None), P(None, tp), P(None, tp), P(None, tp), P(tp, None), P(SP, tp))
    out_specs = (P(SP, tp),) * 6 + (P(tp, None),)
    return jax.shard_map(staged, mesh=torus, in_specs=in_specs, out_specs=out_specs, check_vma=False)
```

```python
import jax
import jax.numpy as jnp
from jax import lax
from jax.experimental import pallas as pl
from jax.experimental.pallas import tpu as pltpu
from jax.sharding import Mesh
from jax.sharding import PartitionSpec as P


HDIM = 128
SEG = 64
PREV = 4
REACH = PREV * SEG
TILE = 128
BAND = REACH + TILE
SP = ("sp_0", "sp_1")
NZ, NX = 8, 4
ROWS = 64
EXTRA = 16
LATE = 384
VMEM_LIMIT = 24 << 20
LOAD_LIMIT = 24 << 20
CHUNKS = 4
WIDTH = 2048 // CHUNKS
SCALE = HDIM ** (-0.5)
F32 = jnp.float32
BF16 = jnp.bfloat16


def odd_pair(i):
    return i ^ 1


def even_pair(n):
    return lambda i: (i + 1) % n if i % 2 else (i - 1) % n


XO, XE = ("sp_1", odd_pair), ("sp_1", even_pair(NX))
ZO, ZE = ("sp_0", odd_pair), ("sp_0", even_pair(NZ))
Z3 = ("sp_0", lambda i: (3, 6, 5, 0, 7, 2, 1, 4)[i])
LEVELS = ((XO, XE, ZO, ZE, Z3), (ZO, ZE, XO, XE, Z3))


def held_order(steps, device):
    if not steps:
        return [device]
    return held_order(steps[1:], steps[0](device)) + held_order(steps[1:], device)


def axis_codes(levels, axis):
    n = NZ if axis == "sp_0" else NX
    mine = [f for a, f in levels if a == axis]
    spots = [len(levels) - 1 - i for i, (a, _) in enumerate(levels) if a == axis]
    wanted = [0] * n
    for device in range(n):
        order = held_order(mine, device)
        assert sorted(order) == list(range(n))
        for at, unit in enumerate(order):
            wanted[unit] |= at << (4 * device)
    me = lax.axis_index(axis)
    codes = []
    for packed in wanted:
        at = jnp.int32(0)
        for device in range(n):
            at = jnp.where(me == device, jnp.int32((packed >> (4 * device)) & 15), at)
        code = jnp.int32(0)
        for i, spot in enumerate(spots):
            code = code | (((at >> (len(spots) - 1 - i)) & 1) << spot)
        codes.append(code)
    return codes


def unit_places():
    core = lax.axis_index("core")
    places = []
    for levels in LEVELS:
        along_z, along_x = axis_codes(levels, "sp_0"), axis_codes(levels, "sp_1")
        places.append([along_z[unit // NX] + along_x[unit % NX] for unit in range(NZ * NX)])
    return [jnp.where(core == 0, a, b) for a, b in zip(*places)]


def level_route(steps, across=0):
    route = []
    for core, levels in enumerate(LEVELS):
        for z in range(NZ):
            for x in range(NX):
                at = {"sp_0": z, "sp_1": x}
                for step in steps:
                    axis, f = levels[step]
                    at[axis] = f(at[axis])
                to = at["sp_0"] * NX + at["sp_1"]
                route.append(((z * NX + x) * 2 + core, to * 2 + (core ^ across)))
    return route


def exchange(block, steps, across=0):
    return lax.ppermute(block, SP + ("core",), level_route(steps, across))


def exchange_quarters(blocks, level):
    paths = ((level, level + 1), (level,), (level + 1,))
    return [exchange(x, path) for x, path in zip(blocks, paths)]


def core_swap(block):
    return lax.ppermute(block, "core", [(0, 1), (1, 0)])


def dot(a, b, contract=((1,), (0,))):
    return lax.dot_general(a, b, (contract, ((), ())), preferred_element_type=F32)


def tile_grads(query, grad, key, value, key_t, value_t, bias):
    scores = dot(key, query, ((1,), (1,))) * SCALE + bias
    top = jnp.max(scores, axis=0, keepdims=True)
    raised = jnp.exp(scores - top)
    probs = raised * (1.0 / jnp.sum(raised, axis=0, keepdims=True))
    probs_low = probs.astype(BF16)
    attn_out = dot(value_t, probs_low).astype(BF16).astype(F32)
    out_dot = jnp.sum(attn_out * grad.T.astype(F32), axis=0, keepdims=True)
    value_part = dot(probs_low, grad)
    score_grad = probs * (dot(value, grad, ((1,), (1,))) - out_dot)
    score_low = score_grad.astype(BF16)
    query_part = (dot(key_t, score_low) * SCALE).T
    key_part = dot(score_low, query) * SCALE
    return score_grad, query_part, key_part, value_part


def load_kernel(x_hbm, wq_hbm, wk_hbm, wv_hbm, tail_ref, x_ref, wq_ref, wk_ref, wv_ref, sem):
    top = 1024 - REACH
    pairs = (
        (wk_hbm, wk_ref), (wv_hbm, wv_ref), (x_hbm.at[top:], x_ref.at[top:]),
        (wq_hbm, wq_ref), (x_hbm.at[:top], x_ref.at[:top]),
    )
    copies = [pltpu.make_async_copy(src, dst, sem.at[i]) for i, (src, dst) in enumerate(pairs)]
    for copy in copies:
        copy.start()
    for copy in copies[:3]:
        copy.wait()
    x = x_ref[top:]
    tail_ref[:, :256] = dot(x, wk_ref[...]).astype(BF16)
    tail_ref[:, 256:] = dot(x, wv_ref[...]).astype(BF16)
    for copy in copies[3:]:
        copy.wait()


def proj_kernel(x_ref, wq_ref, wk_ref, wv_ref, q_ref, k_ref, v_ref):
    x = x_ref[...]
    q_ref[...] = dot(x, wq_ref[...]).astype(BF16)
    k_ref[...] = dot(x, wk_ref[...]).astype(BF16)
    v_ref[...] = dot(x, wv_ref[...]).astype(BF16)


def tiles(which, q_ref, k_ref, v_ref, og_ref, bias_ref, kt_s, vt_s, pat_ref, dq_ref, dq_at, ka_s, va_s, acc_at):
    for tile in which:
        rows = slice(REACH + tile * TILE, REACH + (tile + 1) * TILE)
        band = slice(tile * TILE, tile * TILE + BAND)
        to = slice(band.start - acc_at, band.stop - acc_at)
        for h in range(2):
            cols = slice(h * HDIM, (h + 1) * HDIM)
            score_grad, query_part, key_part, value_part = tile_grads(
                q_ref[rows, cols], og_ref[rows, cols], k_ref[band, cols], v_ref[band, cols],
                kt_s[cols, to], vt_s[cols, to], bias_ref[h],
            )
            pat_ref[h] += score_grad
            dq_ref[rows.start - dq_at : rows.stop - dq_at, cols] = query_part.astype(BF16)
            ka_s[to, cols] += key_part
            va_s[to, cols] += value_part


def late_kernel(
    q_ref, k_ref, v_ref, og_ref, rel_ref,
    dq_ref, acc_ref, bias_ref, pat_ref,
    kt_s, vt_s, ka_s, va_s,
):
    u = lax.broadcasted_iota(jnp.int32, (BAND, TILE), 0)
    col = lax.broadcasted_iota(jnp.int32, (BAND, TILE), 1)
    low = jnp.where(col < SEG, 0, SEG)
    inside = (u >= low) & (u < low + REACH + SEG)
    for h in range(2):
        table = rel_ref[h : h + 1, :]
        far = jnp.concatenate([table[:, :256], jnp.broadcast_to(table[:, 256:257], (1, 256))], axis=1)
        far = jnp.broadcast_to(far, (BAND, 512))
        skew = pltpu.roll(far, 0, 1, stride=1, stride_axis=0)[:, BAND:]
        bias_ref[h] = jnp.where(inside, skew, -jnp.inf)
    pat_ref[...] = jnp.zeros_like(pat_ref)
    kt_s[...] = k_ref[LATE:].T
    vt_s[...] = v_ref[LATE:].T
    ka_s[...] = jnp.zeros_like(ka_s)
    va_s[...] = jnp.zeros_like(va_s)
    tiles(
        range(3, 6), q_ref, k_ref, v_ref, og_ref, bias_ref, kt_s, vt_s, pat_ref, dq_ref, LATE + REACH,
        ka_s, va_s, LATE,
    )
    acc_ref[:, :256] = ka_s[...]
    acc_ref[:, 256:] = va_s[...]


def first_kernel(
    q_ref, k_ref, v_ref, halo_ref, og_ref, bias_ref, pat_in,
    dq_ref, edge_ref, back_ref, pat_ref,
    k_s, v_s, kt_s, vt_s, ka_s, va_s,
):
    k_s[:REACH] = halo_ref[:, :256]
    v_s[:REACH] = halo_ref[:, 256:]
    k_s[REACH:] = k_ref[...]
    v_s[REACH:] = v_ref[...]
    kt_s[...] = k_s[...].T
    vt_s[...] = v_s[...].T
    ka_s[...] = jnp.zeros_like(ka_s)
    va_s[...] = jnp.zeros_like(va_s)
    pat_ref[...] = pat_in[...]
    outside = (lax.axis_index("sp_0") == 0) & (lax.axis_index("sp_1") == 0)
    u = lax.broadcasted_iota(jnp.int32, (BAND, TILE), 0)
    for t in range(2):
        rows = slice(t * TILE, (t + 1) * TILE)
        band = slice(t * TILE, t * TILE + BAND)
        for h in range(2):
            cols = slice(h * HDIM, (h + 1) * HDIM)
            bias = jnp.where(outside & (u < REACH - t * TILE), -jnp.inf, bias_ref[h])
            score_grad, query_part, key_part, value_part = tile_grads(
                q_ref[rows, cols], og_ref[rows, cols], k_s[band, cols], v_s[band, cols],
                kt_s[cols, band], vt_s[cols, band], bias,
            )
            pat_ref[h] += score_grad
            dq_ref[rows, cols] = query_part.astype(BF16)
            ka_s[band, cols] += key_part
            va_s[band, cols] += value_part
    edge_ref[:, :256] = ka_s[REACH:]
    edge_ref[:, 256:] = va_s[REACH:]
    back_ref[:, :256] = ka_s[:REACH].astype(BF16)
    back_ref[:, 256:] = va_s[:REACH].astype(BF16)


def attn_kernel(
    q_ref, k_ref, v_ref, og_ref, bias_ref, pat_in, edge_in, acc_in, dq_in, dq_late,
    dq_ref, near_ref, kg_ref, vg_ref, edge_ref, pat_ref,
    kt_s, vt_s, ka_s, va_s,
):
    kt_s[...] = k_ref[: LATE + REACH].T
    vt_s[...] = v_ref[: LATE + REACH].T
    ka_s[:REACH] = edge_in[:, :256]
    va_s[:REACH] = edge_in[:, 256:]
    ka_s[REACH:LATE] = jnp.zeros((LATE - REACH, 256), F32)
    va_s[REACH:LATE] = jnp.zeros((LATE - REACH, 256), F32)
    ka_s[LATE:] = acc_in[: LATE + REACH - LATE, :256]
    va_s[LATE:] = acc_in[: LATE + REACH - LATE, 256:]
    pat_ref[...] = pat_in[...]
    near_ref[:REACH] = dq_in[...]
    near_ref[LATE + REACH :] = dq_late[...]
    tiles(range(3), q_ref, k_ref, v_ref, og_ref, bias_ref, kt_s, vt_s, pat_ref, near_ref, 0, ka_s, va_s, 0)
    dq_ref[...] = near_ref[...]
    last = LATE + REACH
    kg_ref[:last] = ka_s[...].astype(BF16)
    vg_ref[:last] = va_s[...].astype(BF16)
    kg_ref[last:] = acc_in[last - LATE : 768 - LATE, :256].astype(BF16)
    vg_ref[last:] = acc_in[last - LATE : 768 - LATE, 256:].astype(BF16)
    edge_ref[...] = acc_in[768 - LATE :]


def finish_kernel(kg_in, vg_in, edge_ref, back_ref, kg_ref, vg_ref, own_ref, swap_ref):
    kg_ref[:768] = kg_in[...]
    vg_ref[:768] = vg_in[...]
    kg_ref[768:] = (edge_ref[:, :256] + back_ref[:, :256].astype(F32)).astype(BF16)
    vg_ref[768:] = (edge_ref[:, 256:] + back_ref[:, 256:].astype(F32)).astype(BF16)
    core = lax.axis_index("core")

    @pl.when(core == 0)
    def _():
        own_ref[...] = kg_ref[...]
        swap_ref[...] = vg_ref[...]

    @pl.when(core == 1)
    def _():
        own_ref[...] = vg_ref[...]
        swap_ref[...] = kg_ref[...]


def store_units(value, chunk, places, out_s):
    units = WIDTH // ROWS
    for i in range(units):
        at = pl.multiple_of(places[chunk * units + i] * ROWS, ROWS)
        out_s[pl.ds(at, ROWS), :] = value[i * ROWS : (i + 1) * ROWS].astype(BF16)


def placed_product(x_ref, grad_ref, out_s):
    places = unit_places()
    for c in range(CHUNKS):
        cols = slice(c * WIDTH, (c + 1) * WIDTH)
        store_units(dot(x_ref[:, cols], grad_ref[...], ((0,), (0,))), c, places, out_s)


def three_parts(table):
    high = table.astype(BF16).astype(F32)
    mid = (table - high).astype(BF16).astype(F32)
    low = table - high - mid
    rest = jnp.zeros((EXTRA - 12, table.shape[1]), F32)
    return jnp.concatenate([high, mid, low, rest], axis=0).astype(BF16)


def table_of(parts):
    parts = parts.astype(F32)
    return parts[0:4] + parts[4:8] + parts[8:12]


def copy_out(pairs, sem):
    copies = [pltpu.make_async_copy(src, dst, sem.at[i]) for i, (src, dst) in enumerate(pairs)]
    for copy in copies:
        copy.start()
    for copy in copies:
        copy.wait()


def query_kernel(
    x_ref, grad_ref, pat_ref, m0_hbm, m1_hbm, m2_hbm, keep_hbm, table_ref, out_s, parts_s, diag_s, sem
):
    placed_product(x_ref, grad_ref, out_s)
    for h in range(2):
        diag_s[...] = jnp.zeros_like(diag_s)
        for a in range(BAND // 8):
            off = BAND - 8 * a
            diag_s[:, off : off + TILE] += pat_ref[h, 8 * a : 8 * a + 8, :]
        total = jnp.zeros((1, 512), F32)
        for s in range(8):
            total += diag_s[s : s + 1, s : s + 512]
        far = jnp.sum(total[:, 256:], axis=1, keepdims=True)
        table_ref[h : h + 1, :] = total[:, :256]
        table_ref[2 + h : 3 + h, :] = jnp.broadcast_to(far, (1, 256))
    parts_s[...] = three_parts(table_ref[...])
    pairs = [(out_s.at[1536:], keep_hbm)]
    for i, m in enumerate((m0_hbm, m1_hbm, m2_hbm)):
        pairs += [(out_s.at[512 * i : 512 * (i + 1)], m.at[:512]), (parts_s, m.at[512:])]
    copy_out(pairs, sem)


def own_kernel(x_ref, grad_ref, out_ref):
    placed_product(x_ref, grad_ref, out_ref)


def other_kernel(x_ref, grad_ref, own_hbm, m0_hbm, m1_hbm, m2_hbm, keep_hbm, out_s, sem, sem2):
    pairs = []
    for i, m in enumerate((m0_hbm, m1_hbm, m2_hbm, keep_hbm)):
        rows = slice(512 * i, 512 * (i + 1))
        pairs.append(pltpu.make_async_copy(own_hbm.at[rows], m.at[:, :256], sem2.at[i]))
        pairs[-1].start()
    placed_product(x_ref, grad_ref, out_s)
    copy_out(
        [
            (out_s.at[512 * i : 512 * (i + 1)], m.at[:, 256:])
            for i, m in enumerate((m0_hbm, m1_hbm, m2_hbm, keep_hbm))
        ],
        sem,
    )
    for copy in pairs:
        copy.wait()


def summed(keep_ref, got_refs, rows):
    total = keep_ref[rows].astype(F32)
    for got in got_refs:
        total += got[rows].astype(F32)
    return total


def summed_table(table_in, got_refs, n):
    total = table_in[...]
    for got in got_refs:
        total += table_of(got[n:, :256])
    return total


def merge_kernel(
    keep_ref, a0, a1, a2, keep2_ref, b0, b1, b2, table_in, m0_ref, m1_ref, m2_ref, next_ref, table_ref
):
    total = summed_table(table_in, (a0, a1, a2), 512)
    table_ref[...] = total
    parts = three_parts(total)
    for i, out in enumerate((m0_ref, m1_ref, m2_ref, next_ref)):
        rows = slice(128 * i, 128 * (i + 1))
        out[:128, :256] = summed(keep_ref, (a0, a1, a2), rows).astype(BF16)
        out[:128, 256:] = summed(keep2_ref, (b0, b1, b2), rows).astype(BF16)
        if i < 3:
            out[128:, :256] = parts
            out[128:, 256:] = jnp.zeros((EXTRA, 512), BF16)


def split_kernel(keep_ref, g0, g1, g2, table_in, one_ref, two_ref, three_ref, own_ref, table_ref):
    n = own_ref.shape[0]
    total = summed_table(table_in, (g0, g1, g2), 2 * n)
    table_ref[...] = total
    far = summed(keep_ref, (g0, g1, g2), slice(0, n))
    one_ref[:n] = far[:, :512].astype(BF16)
    one_ref[n:, :256] = three_parts(total)
    one_ref[n:, 256:] = jnp.zeros((EXTRA, 256), BF16)
    two_ref[...] = far[:, 512:].astype(BF16)
    near = summed(keep_ref, (g0, g1, g2), slice(n, 2 * n))
    own_ref[...] = near[:, :512]
    three_ref[...] = near[:, 512:]


def output_kernel(own_ref, one_ref, two_ref, three_ref, table_in, q_ref, k_ref, v_ref, table_ref):
    core = lax.axis_index("core")
    n = own_ref.shape[0]
    table = table_in[...] + table_of(one_ref[n:, :256])
    table_ref[:, :256] = table[:2]
    table_ref[:, 256:] = table[2:, :1]
    own = own_ref[...] + one_ref[:n].astype(F32)
    got = three_ref[...] + two_ref[...].astype(F32)
    q_ref[...] = own[:, :256]

    @pl.when(core == 0)
    def _():
        k_ref[...] = own[:, 256:]
        v_ref[...] = got

    @pl.when(core == 1)
    def _():
        v_ref[...] = own[:, 256:]
        k_ref[...] = got


def sds(shape, dtype):
    return jax.ShapeDtypeStruct(shape, dtype)


def whole(shape):
    return pl.BlockSpec(shape, lambda *_: (0,) * len(shape))


def cost(flops, byte_count):
    return pl.CostEstimate(flops=flops, bytes_accessed=byte_count, transcendentals=0)


def params(limit=None):
    return pltpu.CompilerParams(dimension_semantics=("arbitrary",), vmem_limit_bytes=limit or VMEM_LIMIT)


def call(kernel, operands, outs, scratch=(), grid=(1,), flops=1 << 20, blocks=None, any_outs=(), any_ins=(), limit=None):
    specs = [pl.BlockSpec(memory_space=pltpu.HBM) if i in any_ins else whole(x.shape) for i, x in enumerate(operands)]
    for at, shape in (blocks or {}).items():
        specs[at] = whole(shape)
    out_specs = [pl.BlockSpec(memory_space=pl.ANY) if i in any_outs else whole(x.shape) for i, x in enumerate(outs)]
    moved = sum(x.size * x.dtype.itemsize for x in (*operands, *outs))
    return pl.pallas_call(
        kernel,
        grid=grid,
        in_specs=specs,
        out_specs=out_specs,
        out_shape=list(outs),
        scratch_shapes=list(scratch),
        compiler_params=params(limit),
        cost_estimate=cost(flops, moved),
    )(*operands)


def neighbour(block, distance):
    count = NZ * NX
    route = [(i, i + distance) for i in range(count) if 0 <= i + distance < count]
    return lax.ppermute(block, SP, route)


def staged(inputs, w_query, w_key, w_value, rel_table, out_grad):
    f32, b16 = (lambda *s: sds(s, F32)), (lambda *s: sds(s, BF16))
    v32, v16 = (lambda *s: pltpu.VMEM(s, F32)), (lambda *s: pltpu.VMEM(s, BF16))
    tile_flops = 6 * 2 * TILE * BAND * HDIM
    in_hbm = tuple(pltpu.with_memory_space_constraint(v, pltpu.HBM) for v in (inputs, w_query, w_key, w_value))
    tail, x, wq, wk, wv = call(
        load_kernel, in_hbm,
        (b16(REACH, 512), b16(1024, 2048), b16(2048, 256), b16(2048, 256), b16(2048, 256)),
        (pltpu.SemaphoreType.DMA((5,)),), flops=2 * 256 * 2048 * 512, any_ins=(0, 1, 2, 3), limit=LOAD_LIMIT,
    )
    halo = neighbour(tail, 1)
    query, key, value = call(
        proj_kernel, (x, wq, wk, wv), (b16(1024, 256),) * 3,
        flops=2 * 1024 * 2048 * 768,
    )
    block = (REACH, 256)
    span = 1024 - LATE
    pattern = f32(2, BAND, TILE)
    dq_late, acc, bias, pat = call(
        late_kernel, (query, key, value, out_grad, rel_table),
        (b16(384, 256), f32(span, 512), pattern, pattern),
        (v16(256, span), v16(256, span), v32(span, 256), v32(span, 256)), flops=6 * tile_flops,
    )
    dq0, edge, back, pat = call(
        first_kernel, (query, key, value, halo, out_grad, bias, pat),
        (b16(REACH, 256), f32(REACH, 512), b16(REACH, 512), pattern),
        (v16(512, 256), v16(512, 256), v16(256, 512), v16(256, 512), v32(512, 256), v32(512, 256)),
        flops=4 * tile_flops, blocks={0: block, 1: block, 2: block, 4: block},
    )
    back = neighbour(back, -1)
    dq, near, kg, vg, edge, pat = call(
        attn_kernel, (query, key, value, out_grad, bias, pat, edge, acc, dq0, dq_late),
        (b16(1024, 256), b16(1024, 256), b16(768, 256), b16(768, 256), f32(REACH, 512), pattern),
        (v16(256, 640), v16(256, 640), v32(640, 256), v32(640, 256)), flops=6 * tile_flops,
    )
    product = 2 * 1024 * 2048 * 256
    dma = pltpu.SemaphoreType.DMA
    *send, keep, table = call(
        query_kernel, (x, near, pat), (b16(512 + EXTRA, 256),) * 3 + (b16(512, 256), f32(4, 256)),
        (v16(2048, 256), v16(EXTRA, 256), v32(8, 640), dma((7,))), flops=product, any_outs=(0, 1, 2, 3),
    )
    a = exchange_quarters(send, 0)
    kg, vg, own, swap = call(finish_kernel, (kg, vg, edge, back), (b16(1024, 256),) * 4)
    got = core_swap(swap)
    (placed,) = call(own_kernel, (x, own), (b16(2048, 256),), flops=product)
    *send2, keep2 = call(
        other_kernel, (x, got, placed), (b16(512, 512),) * 4,
        (v16(2048, 256), dma((4,)), dma((4,))), flops=product, any_outs=(0, 1, 2, 3), any_ins=(2,),
    )
    b = exchange_quarters(send2, 0)
    *send, keep, table = call(
        merge_kernel, (keep, *a, keep2, *b, table),
        (b16(128 + EXTRA, 768),) * 3 + (b16(128, 768), f32(4, 256)),
    )
    c = exchange_quarters(send, 2)
    one, two, three, own, table = call(
        split_kernel, (keep, *c, table),
        (b16(64 + EXTRA, 512), b16(64, 256), f32(64, 256), f32(64, 512), f32(4, 256)),
    )
    one = exchange(one, (4,))
    two = exchange(two, (4,), across=1)
    three = core_swap(three)
    dwq, dwk, dwv, table = call(
        output_kernel, (own, one, two, three, table), (f32(64, 256),) * 3 + (f32(*rel_table.shape),)
    )
    return dq, kg, vg, dwq, dwk, dwv, table


def solution(mesh):
    torus = Mesh(mesh.devices.reshape(NZ, NX, -1, 2), SP + ("row", "core"))
    tp = ("row", "core")
    in_specs = (P(SP, None), P(None, tp), P(None, tp), P(None, tp), P(tp, None), P(SP, tp))
    out_specs = (P(SP, tp),) * 6 + (P(tp, None),)
    return jax.shard_map(staged, mesh=torus, in_specs=in_specs, out_specs=out_specs, check_vma=False)
```

```python
import jax
import jax.numpy as jnp
from jax import lax
from jax.experimental import pallas as pl
from jax.experimental.pallas import tpu as pltpu
from jax.sharding import Mesh
from jax.sharding import PartitionSpec as P


HDIM = 128
SEG = 64
PREV = 4
REACH = PREV * SEG
TILE = 128
BAND = REACH + TILE
SP = ("sp_0", "sp_1")
NZ, NX = 8, 4
ROWS = 64
EXTRA = 16
LATE = 384
VMEM_LIMIT = 24 << 20
LOAD_LIMIT = 24 << 20
CHUNKS = 4
WIDTH = 2048 // CHUNKS
SCALE = HDIM ** (-0.5)
F32 = jnp.float32
BF16 = jnp.bfloat16


def odd_pair(i):
    return i ^ 1


def even_pair(n):
    return lambda i: (i + 1) % n if i % 2 else (i - 1) % n


XO, XE = ("sp_1", odd_pair), ("sp_1", even_pair(NX))
ZO, ZE = ("sp_0", odd_pair), ("sp_0", even_pair(NZ))
Z3 = ("sp_0", lambda i: (3, 6, 5, 0, 7, 2, 1, 4)[i])
LEVELS = ((ZO, ZE, XO, XE, Z3), (XO, XE, ZO, ZE, Z3))


def held_order(steps, device):
    if not steps:
        return [device]
    return held_order(steps[1:], steps[0](device)) + held_order(steps[1:], device)


def axis_codes(levels, axis):
    n = NZ if axis == "sp_0" else NX
    mine = [f for a, f in levels if a == axis]
    spots = [len(levels) - 1 - i for i, (a, _) in enumerate(levels) if a == axis]
    wanted = [0] * n
    for device in range(n):
        order = held_order(mine, device)
        assert sorted(order) == list(range(n))
        for at, unit in enumerate(order):
            wanted[unit] |= at << (4 * device)
    me = lax.axis_index(axis)
    codes = []
    for packed in wanted:
        at = jnp.int32(0)
        for device in range(n):
            at = jnp.where(me == device, jnp.int32((packed >> (4 * device)) & 15), at)
        code = jnp.int32(0)
        for i, spot in enumerate(spots):
            code = code | (((at >> (len(spots) - 1 - i)) & 1) << spot)
        codes.append(code)
    return codes


def unit_places():
    core = lax.axis_index("core")
    places = []
    for levels in LEVELS:
        along_z, along_x = axis_codes(levels, "sp_0"), axis_codes(levels, "sp_1")
        places.append([along_z[unit // NX] + along_x[unit % NX] for unit in range(NZ * NX)])
    return [jnp.where(core == 0, a, b) for a, b in zip(*places)]


def level_route(steps, across=0):
    route = []
    for core, levels in enumerate(LEVELS):
        for z in range(NZ):
            for x in range(NX):
                at = {"sp_0": z, "sp_1": x}
                for step in steps:
                    axis, f = levels[step]
                    at[axis] = f(at[axis])
                to = at["sp_0"] * NX + at["sp_1"]
                route.append(((z * NX + x) * 2 + core, to * 2 + (core ^ across)))
    return route


def exchange(block, steps, across=0):
    return lax.ppermute(block, SP + ("core",), level_route(steps, across))


def exchange_quarters(blocks, level):
    paths = ((level, level + 1), (level,), (level + 1,))
    return [exchange(x, path) for x, path in zip(blocks, paths)]


def core_swap(block):
    return lax.ppermute(block, "core", [(0, 1), (1, 0)])


def dot(a, b, contract=((1,), (0,))):
    return lax.dot_general(a, b, (contract, ((), ())), preferred_element_type=F32)


def tile_grads(query, grad, key, value, key_t, value_t, bias):
    scores = dot(key, query, ((1,), (1,))) * SCALE + bias
    top = jnp.max(scores, axis=0, keepdims=True)
    raised = jnp.exp(scores - top)
    probs = raised * (1.0 / jnp.sum(raised, axis=0, keepdims=True))
    probs_low = probs.astype(BF16)
    attn_out = dot(value_t, probs_low).astype(BF16).astype(F32)
    out_dot = jnp.sum(attn_out * grad.T.astype(F32), axis=0, keepdims=True)
    value_part = dot(probs_low, grad)
    score_grad = probs * (dot(value, grad, ((1,), (1,))) - out_dot)
    score_low = score_grad.astype(BF16)
    query_part = (dot(key_t, score_low) * SCALE).T
    key_part = dot(score_low, query) * SCALE
    return score_grad, query_part, key_part, value_part


def load_kernel(x_hbm, wq_hbm, wk_hbm, wv_hbm, tail_ref, x_ref, wq_ref, wk_ref, wv_ref, sem):
    top = 1024 - REACH
    pairs = (
        (wk_hbm, wk_ref), (wv_hbm, wv_ref), (x_hbm.at[top:], x_ref.at[top:]),
        (wq_hbm, wq_ref), (x_hbm.at[:top], x_ref.at[:top]),
    )
    copies = [pltpu.make_async_copy(src, dst, sem.at[i]) for i, (src, dst) in enumerate(pairs)]
    for copy in copies:
        copy.start()
    for copy in copies[:3]:
        copy.wait()
    x = x_ref[top:]
    tail_ref[:, :256] = dot(x, wk_ref[...]).astype(BF16)
    tail_ref[:, 256:] = dot(x, wv_ref[...]).astype(BF16)
    for copy in copies[3:]:
        copy.wait()


def proj_kernel(x_ref, wq_ref, wk_ref, wv_ref, q_ref, k_ref, v_ref):
    x = x_ref[...]
    q_ref[...] = dot(x, wq_ref[...]).astype(BF16)
    k_ref[...] = dot(x, wk_ref[...]).astype(BF16)
    v_ref[...] = dot(x, wv_ref[...]).astype(BF16)


def tiles(which, q_ref, k_ref, v_ref, og_ref, bias_ref, kt_s, vt_s, pat_ref, dq_ref, dq_at, ka_s, va_s, acc_at):
    for tile in which:
        rows = slice(REACH + tile * TILE, REACH + (tile + 1) * TILE)
        band = slice(tile * TILE, tile * TILE + BAND)
        to = slice(band.start - acc_at, band.stop - acc_at)
        for h in range(2):
            cols = slice(h * HDIM, (h + 1) * HDIM)
            score_grad, query_part, key_part, value_part = tile_grads(
                q_ref[rows, cols], og_ref[rows, cols], k_ref[band, cols], v_ref[band, cols],
                kt_s[cols, to], vt_s[cols, to], bias_ref[h],
            )
            pat_ref[h] += score_grad
            dq_ref[rows.start - dq_at : rows.stop - dq_at, cols] = query_part.astype(BF16)
            ka_s[to, cols] += key_part
            va_s[to, cols] += value_part


def late_kernel(
    q_ref, k_ref, v_ref, og_ref, rel_ref,
    dq_ref, acc_ref, bias_ref, pat_ref,
    kt_s, vt_s, ka_s, va_s,
):
    u = lax.broadcasted_iota(jnp.int32, (BAND, TILE), 0)
    col = lax.broadcasted_iota(jnp.int32, (BAND, TILE), 1)
    low = jnp.where(col < SEG, 0, SEG)
    inside = (u >= low) & (u < low + REACH + SEG)
    for h in range(2):
        table = rel_ref[h : h + 1, :]
        far = jnp.concatenate([table[:, :256], jnp.broadcast_to(table[:, 256:257], (1, 256))], axis=1)
        far = jnp.broadcast_to(far, (BAND, 512))
        skew = pltpu.roll(far, 0, 1, stride=1, stride_axis=0)[:, BAND:]
        bias_ref[h] = jnp.where(inside, skew, -jnp.inf)
    pat_ref[...] = jnp.zeros_like(pat_ref)
    kt_s[...] = k_ref[LATE:].T
    vt_s[...] = v_ref[LATE:].T
    ka_s[...] = jnp.zeros_like(ka_s)
    va_s[...] = jnp.zeros_like(va_s)
    tiles(
        range(3, 6), q_ref, k_ref, v_ref, og_ref, bias_ref, kt_s, vt_s, pat_ref, dq_ref, LATE + REACH,
        ka_s, va_s, LATE,
    )
    acc_ref[:, :256] = ka_s[...]
    acc_ref[:, 256:] = va_s[...]


def first_kernel(
    q_ref, k_ref, v_ref, halo_ref, og_ref, bias_ref, pat_in,
    dq_ref, edge_ref, back_ref, pat_ref,
    k_s, v_s, kt_s, vt_s, ka_s, va_s,
):
    k_s[:REACH] = halo_ref[:, :256]
    v_s[:REACH] = halo_ref[:, 256:]
    k_s[REACH:] = k_ref[...]
    v_s[REACH:] = v_ref[...]
    kt_s[...] = k_s[...].T
    vt_s[...] = v_s[...].T
    ka_s[...] = jnp.zeros_like(ka_s)
    va_s[...] = jnp.zeros_like(va_s)
    pat_ref[...] = pat_in[...]
    outside = (lax.axis_index("sp_0") == 0) & (lax.axis_index("sp_1") == 0)
    u = lax.broadcasted_iota(jnp.int32, (BAND, TILE), 0)
    for t in range(2):
        rows = slice(t * TILE, (t + 1) * TILE)
        band = slice(t * TILE, t * TILE + BAND)
        for h in range(2):
            cols = slice(h * HDIM, (h + 1) * HDIM)
            bias = jnp.where(outside & (u < REACH - t * TILE), -jnp.inf, bias_ref[h])
            score_grad, query_part, key_part, value_part = tile_grads(
                q_ref[rows, cols], og_ref[rows, cols], k_s[band, cols], v_s[band, cols],
                kt_s[cols, band], vt_s[cols, band], bias,
            )
            pat_ref[h] += score_grad
            dq_ref[rows, cols] = query_part.astype(BF16)
            ka_s[band, cols] += key_part
            va_s[band, cols] += value_part
    edge_ref[:, :256] = ka_s[REACH:]
    edge_ref[:, 256:] = va_s[REACH:]
    back_ref[:, :256] = ka_s[:REACH].astype(BF16)
    back_ref[:, 256:] = va_s[:REACH].astype(BF16)


def attn_kernel(
    q_ref, k_ref, v_ref, og_ref, bias_ref, pat_in, edge_in, acc_in, dq_in, dq_late,
    near_ref, kg_ref, vg_ref, edge_ref, pat_ref,
    kt_s, vt_s, ka_s, va_s,
):
    kt_s[...] = k_ref[: LATE + REACH].T
    vt_s[...] = v_ref[: LATE + REACH].T
    ka_s[:REACH] = edge_in[:, :256]
    va_s[:REACH] = edge_in[:, 256:]
    ka_s[REACH:LATE] = jnp.zeros((LATE - REACH, 256), F32)
    va_s[REACH:LATE] = jnp.zeros((LATE - REACH, 256), F32)
    ka_s[LATE:] = acc_in[: LATE + REACH - LATE, :256]
    va_s[LATE:] = acc_in[: LATE + REACH - LATE, 256:]
    pat_ref[...] = pat_in[...]
    near_ref[:REACH] = dq_in[...]
    near_ref[LATE + REACH :] = dq_late[...]
    tiles(range(3), q_ref, k_ref, v_ref, og_ref, bias_ref, kt_s, vt_s, pat_ref, near_ref, 0, ka_s, va_s, 0)
    last = LATE + REACH
    kg_ref[:last] = ka_s[...].astype(BF16)
    vg_ref[:last] = va_s[...].astype(BF16)
    kg_ref[last:] = acc_in[last - LATE : 768 - LATE, :256].astype(BF16)
    vg_ref[last:] = acc_in[last - LATE : 768 - LATE, 256:].astype(BF16)
    edge_ref[...] = acc_in[768 - LATE :]


def finish_kernel(kg_in, vg_in, edge_ref, back_ref, own_ref, swap_ref):
    core = lax.axis_index("core")
    key = (edge_ref[:, :256] + back_ref[:, :256].astype(F32)).astype(BF16)
    value = (edge_ref[:, 256:] + back_ref[:, 256:].astype(F32)).astype(BF16)

    def put(to_key, to_value):
        to_key[:768] = kg_in[...]
        to_value[:768] = vg_in[...]
        to_key[768:] = key
        to_value[768:] = value

    @pl.when(core == 0)
    def _():
        put(own_ref, swap_ref)

    @pl.when(core == 1)
    def _():
        put(swap_ref, own_ref)


def emit_kernel(dq_in, own_in, swap_in, dq_ref, kg_ref, vg_ref, sem):
    core = lax.axis_index("core")
    query = pltpu.make_async_copy(dq_in, dq_ref, sem.at[0])
    query.start()

    @pl.when(core == 0)
    def _():
        copy_out([(own_in, kg_ref), (swap_in, vg_ref)], sem.at[1:])

    @pl.when(core == 1)
    def _():
        copy_out([(swap_in, kg_ref), (own_in, vg_ref)], sem.at[1:])

    query.wait()


def store_units(value, chunk, places, out_s):
    units = WIDTH // ROWS
    for i in range(units):
        at = pl.multiple_of(places[chunk * units + i] * ROWS, ROWS)
        out_s[pl.ds(at, ROWS), :] = value[i * ROWS : (i + 1) * ROWS].astype(BF16)


def placed_product(x_ref, grad_ref, out_s):
    places = unit_places()
    for c in range(CHUNKS):
        cols = slice(c * WIDTH, (c + 1) * WIDTH)
        store_units(dot(x_ref[:, cols], grad_ref[...], ((0,), (0,))), c, places, out_s)


def three_parts(table):
    high = table.astype(BF16).astype(F32)
    mid = (table - high).astype(BF16).astype(F32)
    low = table - high - mid
    rest = jnp.zeros((EXTRA - 12, table.shape[1]), F32)
    return jnp.concatenate([high, mid, low, rest], axis=0).astype(BF16)


def table_of(parts):
    parts = parts.astype(F32)
    return parts[0:4] + parts[4:8] + parts[8:12]


def copy_out(pairs, sem):
    copies = [pltpu.make_async_copy(src, dst, sem.at[i]) for i, (src, dst) in enumerate(pairs)]
    for copy in copies:
        copy.start()
    for copy in copies:
        copy.wait()


def query_kernel(
    x_ref, grad_ref, pat_ref, m0_hbm, m1_hbm, m2_hbm, keep_hbm, table_ref, out_s, parts_s, diag_s, sem
):
    placed_product(x_ref, grad_ref, out_s)
    for h in range(2):
        diag_s[...] = jnp.zeros_like(diag_s)
        for a in range(BAND // 8):
            off = BAND - 8 * a
            diag_s[:, off : off + TILE] += pat_ref[h, 8 * a : 8 * a + 8, :]
        total = jnp.zeros((1, 512), F32)
        for s in range(8):
            total += diag_s[s : s + 1, s : s + 512]
        far = jnp.sum(total[:, 256:], axis=1, keepdims=True)
        table_ref[h : h + 1, :] = total[:, :256]
        table_ref[2 + h : 3 + h, :] = jnp.broadcast_to(far, (1, 256))
    parts_s[...] = three_parts(table_ref[...])
    pairs = [(out_s.at[1536:], keep_hbm)]
    for i, m in enumerate((m0_hbm, m1_hbm, m2_hbm)):
        pairs += [(out_s.at[512 * i : 512 * (i + 1)], m.at[:512]), (parts_s, m.at[512:])]
    copy_out(pairs, sem)


def own_kernel(x_ref, grad_ref, out_ref):
    placed_product(x_ref, grad_ref, out_ref)


def other_kernel(x_ref, grad_ref, own_hbm, m0_hbm, m1_hbm, m2_hbm, keep_hbm, out_s, sem, sem2):
    pairs = []
    for i, m in enumerate((m0_hbm, m1_hbm, m2_hbm, keep_hbm)):
        rows = slice(512 * i, 512 * (i + 1))
        pairs.append(pltpu.make_async_copy(own_hbm.at[rows], m.at[:, :256], sem2.at[i]))
        pairs[-1].start()
    placed_product(x_ref, grad_ref, out_s)
    copy_out(
        [
            (out_s.at[512 * i : 512 * (i + 1)], m.at[:, 256:])
            for i, m in enumerate((m0_hbm, m1_hbm, m2_hbm, keep_hbm))
        ],
        sem,
    )
    for copy in pairs:
        copy.wait()


def summed(keep_ref, got_refs, rows):
    total = keep_ref[rows].astype(F32)
    for got in got_refs:
        total += got[rows].astype(F32)
    return total


def summed_table(table_in, got_refs, n):
    total = table_in[...]
    for got in got_refs:
        total += table_of(got[n:, :256])
    return total


def merge_kernel(
    keep_ref, a0, a1, a2, keep2_ref, b0, b1, b2, table_in, m0_ref, m1_ref, m2_ref, next_ref, table_ref
):
    total = summed_table(table_in, (a0, a1, a2), 512)
    table_ref[...] = total
    parts = three_parts(total)
    for i, out in enumerate((m0_ref, m1_ref, m2_ref, next_ref)):
        rows = slice(128 * i, 128 * (i + 1))
        out[:128, :256] = summed(keep_ref, (a0, a1, a2), rows).astype(BF16)
        out[:128, 256:] = summed(keep2_ref, (b0, b1, b2), rows).astype(BF16)
        if i < 3:
            out[128:, :256] = parts
            out[128:, 256:] = jnp.zeros((EXTRA, 512), BF16)


def split_kernel(keep_ref, g0, g1, g2, table_in, one_ref, two_ref, three_ref, own_ref, table_ref):
    n = own_ref.shape[0]
    total = summed_table(table_in, (g0, g1, g2), 2 * n)
    table_ref[...] = total
    far = summed(keep_ref, (g0, g1, g2), slice(0, n))
    one_ref[:n] = far[:, :512].astype(BF16)
    one_ref[n:, :256] = three_parts(total)
    one_ref[n:, 256:] = jnp.zeros((EXTRA, 256), BF16)
    two_ref[...] = far[:, 512:].astype(BF16)
    near = summed(keep_ref, (g0, g1, g2), slice(n, 2 * n))
    own_ref[...] = near[:, :512]
    three_ref[...] = near[:, 512:]


def output_kernel(own_ref, one_ref, two_ref, three_ref, table_in, q_ref, k_ref, v_ref, table_ref):
    core = lax.axis_index("core")
    n = own_ref.shape[0]
    table = table_in[...] + table_of(one_ref[n:, :256])
    table_ref[:, :256] = table[:2]
    table_ref[:, 256:] = table[2:, :1]
    own = own_ref[...] + one_ref[:n].astype(F32)
    got = three_ref[...] + two_ref[...].astype(F32)
    q_ref[...] = own[:, :256]

    @pl.when(core == 0)
    def _():
        k_ref[...] = own[:, 256:]
        v_ref[...] = got

    @pl.when(core == 1)
    def _():
        v_ref[...] = own[:, 256:]
        k_ref[...] = got


def sds(shape, dtype):
    return jax.ShapeDtypeStruct(shape, dtype)


def whole(shape):
    return pl.BlockSpec(shape, lambda *_: (0,) * len(shape))


def cost(flops, byte_count):
    return pl.CostEstimate(flops=flops, bytes_accessed=byte_count, transcendentals=0)


def params(limit=None):
    return pltpu.CompilerParams(dimension_semantics=("arbitrary",), vmem_limit_bytes=limit or VMEM_LIMIT)


def call(kernel, operands, outs, scratch=(), grid=(1,), flops=1 << 20, blocks=None, any_outs=(), any_ins=(), limit=None):
    specs = [pl.BlockSpec(memory_space=pltpu.HBM) if i in any_ins else whole(x.shape) for i, x in enumerate(operands)]
    for at, shape in (blocks or {}).items():
        specs[at] = whole(shape)
    out_specs = [pl.BlockSpec(memory_space=pl.ANY) if i in any_outs else whole(x.shape) for i, x in enumerate(outs)]
    moved = sum(x.size * x.dtype.itemsize for x in (*operands, *outs))
    return pl.pallas_call(
        kernel,
        grid=grid,
        in_specs=specs,
        out_specs=out_specs,
        out_shape=list(outs),
        scratch_shapes=list(scratch),
        compiler_params=params(limit),
        cost_estimate=cost(flops, moved),
    )(*operands)


def neighbour(block, distance):
    count = NZ * NX
    route = [(i, i + distance) for i in range(count) if 0 <= i + distance < count]
    return lax.ppermute(block, SP, route)


def staged(inputs, w_query, w_key, w_value, rel_table, out_grad):
    f32, b16 = (lambda *s: sds(s, F32)), (lambda *s: sds(s, BF16))
    v32, v16 = (lambda *s: pltpu.VMEM(s, F32)), (lambda *s: pltpu.VMEM(s, BF16))
    tile_flops = 6 * 2 * TILE * BAND * HDIM
    in_hbm = tuple(pltpu.with_memory_space_constraint(v, pltpu.HBM) for v in (inputs, w_query, w_key, w_value))
    tail, x, wq, wk, wv = call(
        load_kernel, in_hbm,
        (b16(REACH, 512), b16(1024, 2048), b16(2048, 256), b16(2048, 256), b16(2048, 256)),
        (pltpu.SemaphoreType.DMA((5,)),), flops=2 * 256 * 2048 * 512, any_ins=(0, 1, 2, 3), limit=LOAD_LIMIT,
    )
    halo = neighbour(tail, 1)
    query, key, value = call(
        proj_kernel, (x, wq, wk, wv), (b16(1024, 256),) * 3,
        flops=2 * 1024 * 2048 * 768,
    )
    block = (REACH, 256)
    span = 1024 - LATE
    pattern = f32(2, BAND, TILE)
    dq_late, acc, bias, pat = call(
        late_kernel, (query, key, value, out_grad, rel_table),
        (b16(384, 256), f32(span, 512), pattern, pattern),
        (v16(256, span), v16(256, span), v32(span, 256), v32(span, 256)), flops=6 * tile_flops,
    )
    dq0, edge, back, pat = call(
        first_kernel, (query, key, value, halo, out_grad, bias, pat),
        (b16(REACH, 256), f32(REACH, 512), b16(REACH, 512), pattern),
        (v16(512, 256), v16(512, 256), v16(256, 512), v16(256, 512), v32(512, 256), v32(512, 256)),
        flops=4 * tile_flops, blocks={0: block, 1: block, 2: block, 4: block},
    )
    back = neighbour(back, -1)
    dq, kg, vg, edge, pat = call(
        attn_kernel, (query, key, value, out_grad, bias, pat, edge, acc, dq0, dq_late),
        (b16(1024, 256), b16(768, 256), b16(768, 256), f32(REACH, 512), pattern),
        (v16(256, 640), v16(256, 640), v32(640, 256), v32(640, 256)), flops=6 * tile_flops,
    )
    product = 2 * 1024 * 2048 * 256
    dma = pltpu.SemaphoreType.DMA
    *send, keep, table = call(
        query_kernel, (x, dq, pat), (b16(512 + EXTRA, 256),) * 3 + (b16(512, 256), f32(4, 256)),
        (v16(2048, 256), v16(EXTRA, 256), v32(8, 640), dma((7,))), flops=product, any_outs=(0, 1, 2, 3),
    )
    a = exchange_quarters(send, 0)
    own, swap = call(finish_kernel, (kg, vg, edge, back), (b16(1024, 256),) * 2)
    got = core_swap(swap)
    (placed,) = call(own_kernel, (x, own), (b16(2048, 256),), flops=product)
    *send2, keep2 = call(
        other_kernel, (x, got, placed), (b16(512, 512),) * 4,
        (v16(2048, 256), dma((4,)), dma((4,))), flops=product, any_outs=(0, 1, 2, 3), any_ins=(2,),
    )
    b = exchange_quarters(send2, 0)
    dq, kg, vg = call(
        emit_kernel, (dq, own, swap), (b16(1024, 256),) * 3, (dma((3,)),),
        any_ins=(0, 1, 2), any_outs=(0, 1, 2),
    )
    *send, keep, table = call(
        merge_kernel, (keep, *a, keep2, *b, table),
        (b16(128 + EXTRA, 768),) * 3 + (b16(128, 768), f32(4, 256)),
    )
    c = exchange_quarters(send, 2)
    one, two, three, own, table = call(
        split_kernel, (keep, *c, table),
        (b16(64 + EXTRA, 512), b16(64, 256), f32(64, 256), f32(64, 512), f32(4, 256)),
    )
    one = exchange(one, (4,))
    two = exchange(two, (4,), across=1)
    three = core_swap(three)
    dwq, dwk, dwv, table = call(
        output_kernel, (own, one, two, three, table), (f32(64, 256),) * 3 + (f32(*rel_table.shape),)
    )
    return dq, kg, vg, dwq, dwk, dwv, table


def solution(mesh):
    torus = Mesh(mesh.devices.reshape(NZ, NX, -1, 2), SP + ("row", "core"))
    tp = ("row", "core")
    in_specs = (P(SP, None), P(None, tp), P(None, tp), P(None, tp), P(tp, None), P(SP, tp))
    out_specs = (P(SP, tp),) * 6 + (P(tp, None),)
    return jax.shard_map(staged, mesh=torus, in_specs=in_specs, out_specs=out_specs, check_vma=False)
```

```python
import jax
import jax.numpy as jnp
from jax import lax
from jax.experimental import pallas as pl
from jax.experimental.pallas import tpu as pltpu
from jax.sharding import Mesh
from jax.sharding import PartitionSpec as P


HDIM = 128
SEG = 64
PREV = 4
REACH = PREV * SEG
TILE = 128
BAND = REACH + TILE
SP = ("sp_0", "sp_1")
NZ, NX = 8, 4
ROWS = 64
EXTRA = 16
LATE = 256
VMEM_LIMIT = 24 << 20
LOAD_LIMIT = 24 << 20
CHUNKS = 4
WIDTH = 2048 // CHUNKS
SCALE = HDIM ** (-0.5)
F32 = jnp.float32
BF16 = jnp.bfloat16


def odd_pair(i):
    return i ^ 1


def even_pair(n):
    return lambda i: (i + 1) % n if i % 2 else (i - 1) % n


XO, XE = ("sp_1", odd_pair), ("sp_1", even_pair(NX))
ZO, ZE = ("sp_0", odd_pair), ("sp_0", even_pair(NZ))
Z3 = ("sp_0", lambda i: (3, 6, 5, 0, 7, 2, 1, 4)[i])
LEVELS = ((XO, XE, ZO, ZE, Z3), (ZO, ZE, XO, XE, Z3))


def held_order(steps, device):
    if not steps:
        return [device]
    return held_order(steps[1:], steps[0](device)) + held_order(steps[1:], device)


def axis_codes(levels, axis):
    n = NZ if axis == "sp_0" else NX
    mine = [f for a, f in levels if a == axis]
    spots = [len(levels) - 1 - i for i, (a, _) in enumerate(levels) if a == axis]
    wanted = [0] * n
    for device in range(n):
        order = held_order(mine, device)
        assert sorted(order) == list(range(n))
        for at, unit in enumerate(order):
            wanted[unit] |= at << (4 * device)
    me = lax.axis_index(axis)
    codes = []
    for packed in wanted:
        at = jnp.int32(0)
        for device in range(n):
            at = jnp.where(me == device, jnp.int32((packed >> (4 * device)) & 15), at)
        code = jnp.int32(0)
        for i, spot in enumerate(spots):
            code = code | (((at >> (len(spots) - 1 - i)) & 1) << spot)
        codes.append(code)
    return codes


def unit_places():
    core = lax.axis_index("core")
    places = []
    for levels in LEVELS:
        along_z, along_x = axis_codes(levels, "sp_0"), axis_codes(levels, "sp_1")
        places.append([along_z[unit // NX] + along_x[unit % NX] for unit in range(NZ * NX)])
    return [jnp.where(core == 0, a, b) for a, b in zip(*places)]


def level_route(steps, across=0):
    route = []
    for core, levels in enumerate(LEVELS):
        for z in range(NZ):
            for x in range(NX):
                at = {"sp_0": z, "sp_1": x}
                for step in steps:
                    axis, f = levels[step]
                    at[axis] = f(at[axis])
                to = at["sp_0"] * NX + at["sp_1"]
                route.append(((z * NX + x) * 2 + core, to * 2 + (core ^ across)))
    return route


def exchange(block, steps, across=0):
    return lax.ppermute(block, SP + ("core",), level_route(steps, across))


def exchange_quarters(blocks, level):
    paths = ((level, level + 1), (level,), (level + 1,))
    return [exchange(x, path) for x, path in zip(blocks, paths)]


def core_swap(block):
    return lax.ppermute(block, "core", [(0, 1), (1, 0)])


def dot(a, b, contract=((1,), (0,))):
    return lax.dot_general(a, b, (contract, ((), ())), preferred_element_type=F32)


def tile_grads(query, grad, key, value, key_t, value_t, bias):
    scores = dot(key, query, ((1,), (1,))) * SCALE + bias
    top = jnp.max(scores, axis=0, keepdims=True)
    raised = jnp.exp(scores - top)
    probs = raised * (1.0 / jnp.sum(raised, axis=0, keepdims=True))
    probs_low = probs.astype(BF16)
    attn_out = dot(value_t, probs_low).astype(BF16).astype(F32)
    out_dot = jnp.sum(attn_out * grad.T.astype(F32), axis=0, keepdims=True)
    value_part = dot(probs_low, grad)
    score_grad = probs * (dot(value, grad, ((1,), (1,))) - out_dot)
    score_low = score_grad.astype(BF16)
    query_part = (dot(key_t, score_low) * SCALE).T
    key_part = dot(score_low, query) * SCALE
    return score_grad, query_part, key_part, value_part


def load_kernel(x_hbm, wq_hbm, wk_hbm, wv_hbm, tail_ref, x_ref, wq_ref, wk_ref, wv_ref, sem):
    top = 1024 - REACH
    pairs = (
        (wk_hbm, wk_ref), (wv_hbm, wv_ref), (x_hbm.at[top:], x_ref.at[top:]),
        (wq_hbm, wq_ref), (x_hbm.at[:top], x_ref.at[:top]),
    )
    copies = [pltpu.make_async_copy(src, dst, sem.at[i]) for i, (src, dst) in enumerate(pairs)]
    for copy in copies:
        copy.start()
    for copy in copies[:3]:
        copy.wait()
    x = x_ref[top:]
    tail_ref[:, :256] = dot(x, wk_ref[...]).astype(BF16)
    tail_ref[:, 256:] = dot(x, wv_ref[...]).astype(BF16)
    for copy in copies[3:]:
        copy.wait()


def proj_kernel(x_ref, wq_ref, wk_ref, wv_ref, q_ref, k_ref, v_ref):
    x = x_ref[...]
    q_ref[...] = dot(x, wq_ref[...]).astype(BF16)
    k_ref[...] = dot(x, wk_ref[...]).astype(BF16)
    v_ref[...] = dot(x, wv_ref[...]).astype(BF16)


def tiles(which, q_ref, k_ref, v_ref, og_ref, bias_ref, kt_s, vt_s, pat_ref, dq_ref, dq_at, ka_s, va_s, acc_at):
    for tile in which:
        rows = slice(REACH + tile * TILE, REACH + (tile + 1) * TILE)
        band = slice(tile * TILE, tile * TILE + BAND)
        to = slice(band.start - acc_at, band.stop - acc_at)
        for h in range(2):
            cols = slice(h * HDIM, (h + 1) * HDIM)
            score_grad, query_part, key_part, value_part = tile_grads(
                q_ref[rows, cols], og_ref[rows, cols], k_ref[band, cols], v_ref[band, cols],
                kt_s[cols, to], vt_s[cols, to], bias_ref[h],
            )
            pat_ref[h] += score_grad
            dq_ref[rows.start - dq_at : rows.stop - dq_at, cols] = query_part.astype(BF16)
            ka_s[to, cols] += key_part
            va_s[to, cols] += value_part


def late_kernel(
    q_ref, k_ref, v_ref, og_ref, rel_ref,
    dq_ref, acc_ref, bias_ref, pat_ref,
    kt_s, vt_s, ka_s, va_s,
):
    u = lax.broadcasted_iota(jnp.int32, (BAND, TILE), 0)
    col = lax.broadcasted_iota(jnp.int32, (BAND, TILE), 1)
    low = jnp.where(col < SEG, 0, SEG)
    inside = (u >= low) & (u < low + REACH + SEG)
    for h in range(2):
        table = rel_ref[h : h + 1, :]
        far = jnp.concatenate([table[:, :256], jnp.broadcast_to(table[:, 256:257], (1, 256))], axis=1)
        far = jnp.broadcast_to(far, (BAND, 512))
        skew = pltpu.roll(far, 0, 1, stride=1, stride_axis=0)[:, BAND:]
        bias_ref[h] = jnp.where(inside, skew, -jnp.inf)
    pat_ref[...] = jnp.zeros_like(pat_ref)
    kt_s[...] = k_ref[LATE:].T
    vt_s[...] = v_ref[LATE:].T
    ka_s[...] = jnp.zeros_like(ka_s)
    va_s[...] = jnp.zeros_like(va_s)
    tiles(
        range(LATE // TILE, 6), q_ref, k_ref, v_ref, og_ref, bias_ref, kt_s, vt_s, pat_ref, dq_ref, LATE + REACH,
        ka_s, va_s, LATE,
    )
    acc_ref[:, :256] = ka_s[...]
    acc_ref[:, 256:] = va_s[...]


def first_kernel(
    q_ref, k_ref, v_ref, halo_ref, og_ref, bias_ref, pat_in,
    dq_ref, edge_ref, back_ref, pat_ref,
    k_s, v_s, kt_s, vt_s, ka_s, va_s,
):
    k_s[:REACH] = halo_ref[:, :256]
    v_s[:REACH] = halo_ref[:, 256:]
    k_s[REACH:] = k_ref[...]
    v_s[REACH:] = v_ref[...]
    kt_s[...] = k_s[...].T
    vt_s[...] = v_s[...].T
    ka_s[...] = jnp.zeros_like(ka_s)
    va_s[...] = jnp.zeros_like(va_s)
    pat_ref[...] = pat_in[...]
    outside = (lax.axis_index("sp_0") == 0) & (lax.axis_index("sp_1") == 0)
    u = lax.broadcasted_iota(jnp.int32, (BAND, TILE), 0)
    for t in range(2):
        rows = slice(t * TILE, (t + 1) * TILE)
        band = slice(t * TILE, t * TILE + BAND)
        for h in range(2):
            cols = slice(h * HDIM, (h + 1) * HDIM)
            bias = jnp.where(outside & (u < REACH - t * TILE), -jnp.inf, bias_ref[h])
            score_grad, query_part, key_part, value_part = tile_grads(
                q_ref[rows, cols], og_ref[rows, cols], k_s[band, cols], v_s[band, cols],
                kt_s[cols, band], vt_s[cols, band], bias,
            )
            pat_ref[h] += score_grad
            dq_ref[rows, cols] = query_part.astype(BF16)
            ka_s[band, cols] += key_part
            va_s[band, cols] += value_part
    edge_ref[:, :256] = ka_s[REACH:]
    edge_ref[:, 256:] = va_s[REACH:]
    back_ref[:, :256] = ka_s[:REACH].astype(BF16)
    back_ref[:, 256:] = va_s[:REACH].astype(BF16)


def attn_kernel(
    q_ref, k_ref, v_ref, og_ref, bias_ref, pat_in, edge_in, acc_in, dq_in, dq_late,
    near_ref, kg_ref, vg_ref, edge_ref, pat_ref,
    kt_s, vt_s, ka_s, va_s,
):
    kt_s[...] = k_ref[: LATE + REACH].T
    vt_s[...] = v_ref[: LATE + REACH].T
    ka_s[:REACH] = edge_in[:, :256]
    va_s[:REACH] = edge_in[:, 256:]
    ka_s[LATE:] = acc_in[: LATE + REACH - LATE, :256]
    va_s[LATE:] = acc_in[: LATE + REACH - LATE, 256:]
    pat_ref[...] = pat_in[...]
    near_ref[:REACH] = dq_in[...]
    near_ref[LATE + REACH :] = dq_late[...]
    tiles(range(LATE // TILE), q_ref, k_ref, v_ref, og_ref, bias_ref, kt_s, vt_s, pat_ref, near_ref, 0, ka_s, va_s, 0)
    last = LATE + REACH
    kg_ref[:last] = ka_s[...].astype(BF16)
    vg_ref[:last] = va_s[...].astype(BF16)
    kg_ref[last:] = acc_in[last - LATE : 768 - LATE, :256].astype(BF16)
    vg_ref[last:] = acc_in[last - LATE : 768 - LATE, 256:].astype(BF16)
    edge_ref[...] = acc_in[768 - LATE :]


def finish_kernel(kg_in, vg_in, edge_ref, back_ref, own_ref, swap_ref):
    core = lax.axis_index("core")
    key = (edge_ref[:, :256] + back_ref[:, :256].astype(F32)).astype(BF16)
    value = (edge_ref[:, 256:] + back_ref[:, 256:].astype(F32)).astype(BF16)

    def put(to_key, to_value):
        to_key[:768] = kg_in[...]
        to_value[:768] = vg_in[...]
        to_key[768:] = key
        to_value[768:] = value

    @pl.when(core == 0)
    def _():
        put(own_ref, swap_ref)

    @pl.when(core == 1)
    def _():
        put(swap_ref, own_ref)


def emit_kernel(dq_in, own_in, swap_in, dq_ref, kg_ref, vg_ref, sem):
    core = lax.axis_index("core")
    query = pltpu.make_async_copy(dq_in, dq_ref, sem.at[0])
    query.start()

    @pl.when(core == 0)
    def _():
        copy_out([(own_in, kg_ref), (swap_in, vg_ref)], sem.at[1:])

    @pl.when(core == 1)
    def _():
        copy_out([(swap_in, kg_ref), (own_in, vg_ref)], sem.at[1:])

    query.wait()


def store_units(value, chunk, places, out_s):
    units = WIDTH // ROWS
    for i in range(units):
        at = pl.multiple_of(places[chunk * units + i] * ROWS, ROWS)
        out_s[pl.ds(at, ROWS), :] = value[i * ROWS : (i + 1) * ROWS].astype(BF16)


def placed_product(x_ref, grad_ref, out_s):
    places = unit_places()
    for c in range(CHUNKS):
        cols = slice(c * WIDTH, (c + 1) * WIDTH)
        store_units(dot(x_ref[:, cols], grad_ref[...], ((0,), (0,))), c, places, out_s)


def three_parts(table):
    high = table.astype(BF16).astype(F32)
    mid = (table - high).astype(BF16).astype(F32)
    low = table - high - mid
    rest = jnp.zeros((EXTRA - 12, table.shape[1]), F32)
    return jnp.concatenate([high, mid, low, rest], axis=0).astype(BF16)


def table_of(parts):
    parts = parts.astype(F32)
    return parts[0:4] + parts[4:8] + parts[8:12]


def copy_out(pairs, sem):
    copies = [pltpu.make_async_copy(src, dst, sem.at[i]) for i, (src, dst) in enumerate(pairs)]
    for copy in copies:
        copy.start()
    for copy in copies:
        copy.wait()


def query_kernel(
    x_ref, grad_ref, pat_ref, m0_hbm, m1_hbm, m2_hbm, keep_hbm, table_ref, out_s, parts_s, diag_s, sem
):
    placed_product(x_ref, grad_ref, out_s)
    for h in range(2):
        diag_s[...] = jnp.zeros_like(diag_s)
        for a in range(BAND // 8):
            off = BAND - 8 * a
            diag_s[:, off : off + TILE] += pat_ref[h, 8 * a : 8 * a + 8, :]
        total = jnp.zeros((1, 512), F32)
        for s in range(8):
            total += diag_s[s : s + 1, s : s + 512]
        far = jnp.sum(total[:, 256:], axis=1, keepdims=True)
        table_ref[h : h + 1, :] = total[:, :256]
        table_ref[2 + h : 3 + h, :] = jnp.broadcast_to(far, (1, 256))
    parts_s[...] = three_parts(table_ref[...])
    pairs = [(out_s.at[1536:], keep_hbm)]
    for i, m in enumerate((m0_hbm, m1_hbm, m2_hbm)):
        pairs += [(out_s.at[512 * i : 512 * (i + 1)], m.at[:512]), (parts_s, m.at[512:])]
    copy_out(pairs, sem)


def own_kernel(x_ref, grad_ref, out_ref):
    placed_product(x_ref, grad_ref, out_ref)


def other_kernel(x_ref, grad_ref, own_hbm, m0_hbm, m1_hbm, m2_hbm, keep_hbm, out_s, sem, sem2):
    pairs = []
    for i, m in enumerate((m0_hbm, m1_hbm, m2_hbm, keep_hbm)):
        rows = slice(512 * i, 512 * (i + 1))
        pairs.append(pltpu.make_async_copy(own_hbm.at[rows], m.at[:, :256], sem2.at[i]))
        pairs[-1].start()
    placed_product(x_ref, grad_ref, out_s)
    copy_out(
        [
            (out_s.at[512 * i : 512 * (i + 1)], m.at[:, 256:])
            for i, m in enumerate((m0_hbm, m1_hbm, m2_hbm, keep_hbm))
        ],
        sem,
    )
    for copy in pairs:
        copy.wait()


def summed(keep_ref, got_refs, rows):
    total = keep_ref[rows].astype(F32)
    for got in got_refs:
        total += got[rows].astype(F32)
    return total


def summed_table(table_in, got_refs, n):
    total = table_in[...]
    for got in got_refs:
        total += table_of(got[n:, :256])
    return total


def merge_kernel(
    keep_ref, a0, a1, a2, keep2_ref, b0, b1, b2, table_in, m0_ref, m1_ref, m2_ref, next_ref, table_ref
):
    total = summed_table(table_in, (a0, a1, a2), 512)
    table_ref[...] = total
    parts = three_parts(total)
    for i, out in enumerate((m0_ref, m1_ref, m2_ref, next_ref)):
        rows = slice(128 * i, 128 * (i + 1))
        out[:128, :256] = summed(keep_ref, (a0, a1, a2), rows).astype(BF16)
        out[:128, 256:] = summed(keep2_ref, (b0, b1, b2), rows).astype(BF16)
        if i < 3:
            out[128:, :256] = parts
            out[128:, 256:] = jnp.zeros((EXTRA, 512), BF16)


def split_kernel(keep_ref, g0, g1, g2, table_in, one_ref, two_ref, three_ref, own_ref, table_ref):
    n = own_ref.shape[0]
    total = summed_table(table_in, (g0, g1, g2), 2 * n)
    table_ref[...] = total
    far = summed(keep_ref, (g0, g1, g2), slice(0, n))
    one_ref[:n] = far[:, :512].astype(BF16)
    one_ref[n:, :256] = three_parts(total)
    one_ref[n:, 256:] = jnp.zeros((EXTRA, 256), BF16)
    two_ref[...] = far[:, 512:].astype(BF16)
    near = summed(keep_ref, (g0, g1, g2), slice(n, 2 * n))
    own_ref[...] = near[:, :512]
    three_ref[...] = near[:, 512:]


def output_kernel(own_ref, one_ref, two_ref, three_ref, table_in, q_ref, k_ref, v_ref, table_ref):
    core = lax.axis_index("core")
    n = own_ref.shape[0]
    table = table_in[...] + table_of(one_ref[n:, :256])
    table_ref[:, :256] = table[:2]
    table_ref[:, 256:] = table[2:, :1]
    own = own_ref[...] + one_ref[:n].astype(F32)
    got = three_ref[...] + two_ref[...].astype(F32)
    q_ref[...] = own[:, :256]

    @pl.when(core == 0)
    def _():
        k_ref[...] = own[:, 256:]
        v_ref[...] = got

    @pl.when(core == 1)
    def _():
        v_ref[...] = own[:, 256:]
        k_ref[...] = got


def sds(shape, dtype):
    return jax.ShapeDtypeStruct(shape, dtype)


def whole(shape):
    return pl.BlockSpec(shape, lambda *_: (0,) * len(shape))


def cost(flops, byte_count):
    return pl.CostEstimate(flops=flops, bytes_accessed=byte_count, transcendentals=0)


def params(limit=None):
    return pltpu.CompilerParams(dimension_semantics=("arbitrary",), vmem_limit_bytes=limit or VMEM_LIMIT)


def call(kernel, operands, outs, scratch=(), grid=(1,), flops=1 << 20, blocks=None, any_outs=(), any_ins=(), limit=None):
    specs = [pl.BlockSpec(memory_space=pltpu.HBM) if i in any_ins else whole(x.shape) for i, x in enumerate(operands)]
    for at, shape in (blocks or {}).items():
        specs[at] = whole(shape)
    out_specs = [pl.BlockSpec(memory_space=pl.ANY) if i in any_outs else whole(x.shape) for i, x in enumerate(outs)]
    moved = sum(x.size * x.dtype.itemsize for x in (*operands, *outs))
    return pl.pallas_call(
        kernel,
        grid=grid,
        in_specs=specs,
        out_specs=out_specs,
        out_shape=list(outs),
        scratch_shapes=list(scratch),
        compiler_params=params(limit),
        cost_estimate=cost(flops, moved),
    )(*operands)


def neighbour(block, distance):
    count = NZ * NX
    route = [(i, i + distance) for i in range(count) if 0 <= i + distance < count]
    return lax.ppermute(block, SP, route)


def staged(inputs, w_query, w_key, w_value, rel_table, out_grad):
    f32, b16 = (lambda *s: sds(s, F32)), (lambda *s: sds(s, BF16))
    v32, v16 = (lambda *s: pltpu.VMEM(s, F32)), (lambda *s: pltpu.VMEM(s, BF16))
    tile_flops = 6 * 2 * TILE * BAND * HDIM
    in_hbm = tuple(pltpu.with_memory_space_constraint(v, pltpu.HBM) for v in (inputs, w_query, w_key, w_value))
    tail, x, wq, wk, wv = call(
        load_kernel, in_hbm,
        (b16(REACH, 512), b16(1024, 2048), b16(2048, 256), b16(2048, 256), b16(2048, 256)),
        (pltpu.SemaphoreType.DMA((5,)),), flops=2 * 256 * 2048 * 512, any_ins=(0, 1, 2, 3), limit=LOAD_LIMIT,
    )
    halo = neighbour(tail, 1)
    query, key, value = call(
        proj_kernel, (x, wq, wk, wv), (b16(1024, 256),) * 3,
        flops=2 * 1024 * 2048 * 768,
    )
    block = (REACH, 256)
    span = 1024 - LATE
    pattern = f32(2, BAND, TILE)
    dq_late, acc, bias, pat = call(
        late_kernel, (query, key, value, out_grad, rel_table),
        (b16(span - REACH, 256), f32(span, 512), pattern, pattern),
        (v16(256, span), v16(256, span), v32(span, 256), v32(span, 256)), flops=6 * tile_flops,
    )
    dq0, edge, back, pat = call(
        first_kernel, (query, key, value, halo, out_grad, bias, pat),
        (b16(REACH, 256), f32(REACH, 512), b16(REACH, 512), pattern),
        (v16(512, 256), v16(512, 256), v16(256, 512), v16(256, 512), v32(512, 256), v32(512, 256)),
        flops=4 * tile_flops, blocks={0: block, 1: block, 2: block, 4: block},
    )
    back = neighbour(back, -1)
    dq, kg, vg, edge, pat = call(
        attn_kernel, (query, key, value, out_grad, bias, pat, edge, acc, dq0, dq_late),
        (b16(1024, 256), b16(768, 256), b16(768, 256), f32(REACH, 512), pattern),
        (v16(256, LATE + REACH), v16(256, LATE + REACH), v32(LATE + REACH, 256), v32(LATE + REACH, 256)), flops=6 * tile_flops,
    )
    product = 2 * 1024 * 2048 * 256
    dma = pltpu.SemaphoreType.DMA
    *send, keep, table = call(
        query_kernel, (x, dq, pat), (b16(512 + EXTRA, 256),) * 3 + (b16(512, 256), f32(4, 256)),
        (v16(2048, 256), v16(EXTRA, 256), v32(8, 640), dma((7,))), flops=product, any_outs=(0, 1, 2, 3),
    )
    a = exchange_quarters(send, 0)
    own, swap = call(finish_kernel, (kg, vg, edge, back), (b16(1024, 256),) * 2)
    got = core_swap(swap)
    (placed,) = call(own_kernel, (x, own), (b16(2048, 256),), flops=product)
    *send2, keep2 = call(
        other_kernel, (x, got, placed), (b16(512, 512),) * 4,
        (v16(2048, 256), dma((4,)), dma((4,))), flops=product, any_outs=(0, 1, 2, 3), any_ins=(2,),
    )
    b = exchange_quarters(send2, 0)
    dq, kg, vg = call(
        emit_kernel, (dq, own, swap), (b16(1024, 256),) * 3, (dma((3,)),),
        any_ins=(0, 1, 2), any_outs=(0, 1, 2),
    )
    *send, keep, table = call(
        merge_kernel, (keep, *a, keep2, *b, table),
        (b16(128 + EXTRA, 768),) * 3 + (b16(128, 768), f32(4, 256)),
    )
    c = exchange_quarters(send, 2)
    one, two, three, own, table = call(
        split_kernel, (keep, *c, table),
        (b16(64 + EXTRA, 512), b16(64, 256), f32(64, 256), f32(64, 512), f32(4, 256)),
    )
    one = exchange(one, (4,))
    two = exchange(two, (4,), across=1)
    three = core_swap(three)
    dwq, dwk, dwv, table = call(
        output_kernel, (own, one, two, three, table), (f32(64, 256),) * 3 + (f32(*rel_table.shape),)
    )
    return dq, kg, vg, dwq, dwk, dwv, table


def solution(mesh):
    torus = Mesh(mesh.devices.reshape(NZ, NX, -1, 2), SP + ("row", "core"))
    tp = ("row", "core")
    in_specs = (P(SP, None), P(None, tp), P(None, tp), P(None, tp), P(tp, None), P(SP, tp))
    out_specs = (P(SP, tp),) * 6 + (P(tp, None),)
    return jax.shard_map(staged, mesh=torus, in_specs=in_specs, out_specs=out_specs, check_vma=False)
```

```python
import jax
import jax.numpy as jnp
from jax import lax
from jax.experimental import pallas as pl
from jax.experimental.pallas import tpu as pltpu
from jax.sharding import Mesh
from jax.sharding import PartitionSpec as P


HDIM = 128
SEG = 64
PREV = 4
REACH = PREV * SEG
TILE = 128
BAND = REACH + TILE
SP = ("sp_0", "sp_1")
NZ, NX = 8, 4
ROWS = 64
EXTRA = 16
LATE = 256
VMEM_LIMIT = 24 << 20
LOAD_LIMIT = 24 << 20
CHUNKS = 4
WIDTH = 2048 // CHUNKS
SCALE = HDIM ** (-0.5)
F32 = jnp.float32
BF16 = jnp.bfloat16


def odd_pair(i):
    return i ^ 1


def even_pair(n):
    return lambda i: (i + 1) % n if i % 2 else (i - 1) % n


XO, XE = ("sp_1", odd_pair), ("sp_1", even_pair(NX))
ZO, ZE = ("sp_0", odd_pair), ("sp_0", even_pair(NZ))
Z3 = ("sp_0", lambda i: (3, 6, 5, 0, 7, 2, 1, 4)[i])
LEVELS = ((XO, XE, ZO, ZE, Z3), (ZO, ZE, XO, XE, Z3))


def held_order(steps, device):
    if not steps:
        return [device]
    return held_order(steps[1:], steps[0](device)) + held_order(steps[1:], device)


def axis_codes(levels, axis):
    n = NZ if axis == "sp_0" else NX
    mine = [f for a, f in levels if a == axis]
    spots = [len(levels) - 1 - i for i, (a, _) in enumerate(levels) if a == axis]
    wanted = [0] * n
    for device in range(n):
        order = held_order(mine, device)
        assert sorted(order) == list(range(n))
        for at, unit in enumerate(order):
            wanted[unit] |= at << (4 * device)
    me = lax.axis_index(axis)
    codes = []
    for packed in wanted:
        at = jnp.int32(0)
        for device in range(n):
            at = jnp.where(me == device, jnp.int32((packed >> (4 * device)) & 15), at)
        code = jnp.int32(0)
        for i, spot in enumerate(spots):
            code = code | (((at >> (len(spots) - 1 - i)) & 1) << spot)
        codes.append(code)
    return codes


def unit_places():
    core = lax.axis_index("core")
    places = []
    for levels in LEVELS:
        along_z, along_x = axis_codes(levels, "sp_0"), axis_codes(levels, "sp_1")
        places.append([along_z[unit // NX] + along_x[unit % NX] for unit in range(NZ * NX)])
    return [jnp.where(core == 0, a, b) for a, b in zip(*places)]


def level_route(steps, across=0):
    route = []
    for core, levels in enumerate(LEVELS):
        for z in range(NZ):
            for x in range(NX):
                at = {"sp_0": z, "sp_1": x}
                for step in steps:
                    axis, f = levels[step]
                    at[axis] = f(at[axis])
                to = at["sp_0"] * NX + at["sp_1"]
                route.append(((z * NX + x) * 2 + core, to * 2 + (core ^ across)))
    return route


def exchange(block, steps, across=0):
    return lax.ppermute(block, SP + ("core",), level_route(steps, across))


def exchange_quarters(blocks, level):
    paths = ((level, level + 1), (level,), (level + 1,))
    return [exchange(x, path) for x, path in zip(blocks, paths)]


def core_swap(block):
    return lax.ppermute(block, "core", [(0, 1), (1, 0)])


def dot(a, b, contract=((1,), (0,))):
    return lax.dot_general(a, b, (contract, ((), ())), preferred_element_type=F32)


def tile_grads(query, grad, key, value, key_t, value_t, bias):
    scores = dot(key, query, ((1,), (1,))) * SCALE + bias
    top = jnp.max(scores, axis=0, keepdims=True)
    raised = jnp.exp(scores - top)
    probs = raised * (1.0 / jnp.sum(raised, axis=0, keepdims=True))
    probs_low = probs.astype(BF16)
    attn_out = dot(value_t, probs_low).astype(BF16).astype(F32)
    out_dot = jnp.sum(attn_out * grad.T.astype(F32), axis=0, keepdims=True)
    value_part = dot(probs_low, grad)
    score_grad = probs * (dot(value, grad, ((1,), (1,))) - out_dot)
    score_low = score_grad.astype(BF16)
    query_part = (dot(key_t, score_low) * SCALE).T
    key_part = dot(score_low, query) * SCALE
    return score_grad, query_part, key_part, value_part


def load_kernel(x_hbm, wk_hbm, wv_hbm, tail_ref, wk_ref, wv_ref, x_s, sem):
    pairs = ((wk_hbm, wk_ref), (x_hbm.at[1024 - REACH :], x_s), (wv_hbm, wv_ref))
    copies = [pltpu.make_async_copy(src, dst, sem.at[i]) for i, (src, dst) in enumerate(pairs)]
    for copy in copies:
        copy.start()
    for copy in copies[:2]:
        copy.wait()
    tail_ref[:, :256] = dot(x_s[...], wk_ref[...]).astype(BF16)
    copies[2].wait()
    tail_ref[:, 256:] = dot(x_s[...], wv_ref[...]).astype(BF16)


def proj_kernel(x_ref, wq_ref, wk_ref, wv_ref, q_ref, k_ref, v_ref):
    x = x_ref[...]
    q_ref[...] = dot(x, wq_ref[...]).astype(BF16)
    k_ref[...] = dot(x, wk_ref[...]).astype(BF16)
    v_ref[...] = dot(x, wv_ref[...]).astype(BF16)


def tiles(which, q_ref, k_ref, v_ref, og_ref, bias_ref, kt_s, vt_s, pat_ref, dq_ref, dq_at, ka_s, va_s, acc_at):
    for tile in which:
        rows = slice(REACH + tile * TILE, REACH + (tile + 1) * TILE)
        band = slice(tile * TILE, tile * TILE + BAND)
        to = slice(band.start - acc_at, band.stop - acc_at)
        for h in range(2):
            cols = slice(h * HDIM, (h + 1) * HDIM)
            score_grad, query_part, key_part, value_part = tile_grads(
                q_ref[rows, cols], og_ref[rows, cols], k_ref[band, cols], v_ref[band, cols],
                kt_s[cols, to], vt_s[cols, to], bias_ref[h],
            )
            pat_ref[h] += score_grad
            dq_ref[rows.start - dq_at : rows.stop - dq_at, cols] = query_part.astype(BF16)
            ka_s[to, cols] += key_part
            va_s[to, cols] += value_part


def late_kernel(
    q_ref, k_ref, v_ref, og_ref, rel_ref,
    dq_ref, acc_ref, bias_ref, pat_ref,
    kt_s, vt_s, ka_s, va_s,
):
    u = lax.broadcasted_iota(jnp.int32, (BAND, TILE), 0)
    col = lax.broadcasted_iota(jnp.int32, (BAND, TILE), 1)
    low = jnp.where(col < SEG, 0, SEG)
    inside = (u >= low) & (u < low + REACH + SEG)
    for h in range(2):
        table = rel_ref[h : h + 1, :]
        far = jnp.concatenate([table[:, :256], jnp.broadcast_to(table[:, 256:257], (1, 256))], axis=1)
        far = jnp.broadcast_to(far, (BAND, 512))
        skew = pltpu.roll(far, 0, 1, stride=1, stride_axis=0)[:, BAND:]
        bias_ref[h] = jnp.where(inside, skew, -jnp.inf)
    pat_ref[...] = jnp.zeros_like(pat_ref)
    kt_s[...] = k_ref[LATE:].T
    vt_s[...] = v_ref[LATE:].T
    ka_s[...] = jnp.zeros_like(ka_s)
    va_s[...] = jnp.zeros_like(va_s)
    tiles(
        range(LATE // TILE, 6), q_ref, k_ref, v_ref, og_ref, bias_ref, kt_s, vt_s, pat_ref, dq_ref, LATE + REACH,
        ka_s, va_s, LATE,
    )
    acc_ref[:, :256] = ka_s[...]
    acc_ref[:, 256:] = va_s[...]


def first_kernel(
    q_ref, k_ref, v_ref, halo_ref, og_ref, bias_ref, pat_in,
    dq_ref, edge_ref, back_ref, pat_ref,
    k_s, v_s, kt_s, vt_s, ka_s, va_s,
):
    k_s[:REACH] = halo_ref[:, :256]
    v_s[:REACH] = halo_ref[:, 256:]
    k_s[REACH:] = k_ref[...]
    v_s[REACH:] = v_ref[...]
    kt_s[...] = k_s[...].T
    vt_s[...] = v_s[...].T
    ka_s[...] = jnp.zeros_like(ka_s)
    va_s[...] = jnp.zeros_like(va_s)
    pat_ref[...] = pat_in[...]
    outside = (lax.axis_index("sp_0") == 0) & (lax.axis_index("sp_1") == 0)
    u = lax.broadcasted_iota(jnp.int32, (BAND, TILE), 0)
    for t in range(2):
        rows = slice(t * TILE, (t + 1) * TILE)
        band = slice(t * TILE, t * TILE + BAND)
        for h in range(2):
            cols = slice(h * HDIM, (h + 1) * HDIM)
            bias = jnp.where(outside & (u < REACH - t * TILE), -jnp.inf, bias_ref[h])
            score_grad, query_part, key_part, value_part = tile_grads(
                q_ref[rows, cols], og_ref[rows, cols], k_s[band, cols], v_s[band, cols],
                kt_s[cols, band], vt_s[cols, band], bias,
            )
            pat_ref[h] += score_grad
            dq_ref[rows, cols] = query_part.astype(BF16)
            ka_s[band, cols] += key_part
            va_s[band, cols] += value_part
    edge_ref[:, :256] = ka_s[REACH:]
    edge_ref[:, 256:] = va_s[REACH:]
    back_ref[:, :256] = ka_s[:REACH].astype(BF16)
    back_ref[:, 256:] = va_s[:REACH].astype(BF16)


def attn_kernel(
    q_ref, k_ref, v_ref, og_ref, bias_ref, pat_in, edge_in, acc_in, dq_in, dq_late,
    near_ref, kg_ref, vg_ref, edge_ref, pat_ref,
    kt_s, vt_s, ka_s, va_s,
):
    kt_s[...] = k_ref[: LATE + REACH].T
    vt_s[...] = v_ref[: LATE + REACH].T
    ka_s[:REACH] = edge_in[:, :256]
    va_s[:REACH] = edge_in[:, 256:]
    ka_s[LATE:] = acc_in[: LATE + REACH - LATE, :256]
    va_s[LATE:] = acc_in[: LATE + REACH - LATE, 256:]
    pat_ref[...] = pat_in[...]
    near_ref[:REACH] = dq_in[...]
    near_ref[LATE + REACH :] = dq_late[...]
    tiles(range(LATE // TILE), q_ref, k_ref, v_ref, og_ref, bias_ref, kt_s, vt_s, pat_ref, near_ref, 0, ka_s, va_s, 0)
    last = LATE + REACH
    kg_ref[:last] = ka_s[...].astype(BF16)
    vg_ref[:last] = va_s[...].astype(BF16)
    kg_ref[last:] = acc_in[last - LATE : 768 - LATE, :256].astype(BF16)
    vg_ref[last:] = acc_in[last - LATE : 768 - LATE, 256:].astype(BF16)
    edge_ref[...] = acc_in[768 - LATE :]


def finish_kernel(kg_in, vg_in, edge_ref, back_ref, own_ref, swap_ref):
    core = lax.axis_index("core")
    key = (edge_ref[:, :256] + back_ref[:, :256].astype(F32)).astype(BF16)
    value = (edge_ref[:, 256:] + back_ref[:, 256:].astype(F32)).astype(BF16)

    def put(to_key, to_value):
        to_key[:768] = kg_in[...]
        to_value[:768] = vg_in[...]
        to_key[768:] = key
        to_value[768:] = value

    @pl.when(core == 0)
    def _():
        put(own_ref, swap_ref)

    @pl.when(core == 1)
    def _():
        put(swap_ref, own_ref)


def emit_kernel(dq_in, own_in, swap_in, dq_ref, kg_ref, vg_ref, sem):
    core = lax.axis_index("core")
    query = pltpu.make_async_copy(dq_in, dq_ref, sem.at[0])
    query.start()

    @pl.when(core == 0)
    def _():
        copy_out([(own_in, kg_ref), (swap_in, vg_ref)], sem.at[1:])

    @pl.when(core == 1)
    def _():
        copy_out([(swap_in, kg_ref), (own_in, vg_ref)], sem.at[1:])

    query.wait()


def store_units(value, chunk, places, out_s):
    units = WIDTH // ROWS
    for i in range(units):
        at = pl.multiple_of(places[chunk * units + i] * ROWS, ROWS)
        out_s[pl.ds(at, ROWS), :] = value[i * ROWS : (i + 1) * ROWS].astype(BF16)


def placed_product(x_ref, grad_ref, out_s):
    places = unit_places()
    for c in range(CHUNKS):
        cols = slice(c * WIDTH, (c + 1) * WIDTH)
        store_units(dot(x_ref[:, cols], grad_ref[...], ((0,), (0,))), c, places, out_s)


def three_parts(table):
    high = table.astype(BF16).astype(F32)
    mid = (table - high).astype(BF16).astype(F32)
    low = table - high - mid
    rest = jnp.zeros((EXTRA - 12, table.shape[1]), F32)
    return jnp.concatenate([high, mid, low, rest], axis=0).astype(BF16)


def table_of(parts):
    parts = parts.astype(F32)
    return parts[0:4] + parts[4:8] + parts[8:12]


def copy_out(pairs, sem):
    copies = [pltpu.make_async_copy(src, dst, sem.at[i]) for i, (src, dst) in enumerate(pairs)]
    for copy in copies:
        copy.start()
    for copy in copies:
        copy.wait()


def query_kernel(
    x_ref, grad_ref, pat_ref, m0_hbm, m1_hbm, m2_hbm, keep_hbm, table_ref, out_s, parts_s, diag_s, sem
):
    placed_product(x_ref, grad_ref, out_s)
    for h in range(2):
        diag_s[...] = jnp.zeros_like(diag_s)
        for a in range(BAND // 8):
            off = BAND - 8 * a
            diag_s[:, off : off + TILE] += pat_ref[h, 8 * a : 8 * a + 8, :]
        total = jnp.zeros((1, 512), F32)
        for s in range(8):
            total += diag_s[s : s + 1, s : s + 512]
        far = jnp.sum(total[:, 256:], axis=1, keepdims=True)
        table_ref[h : h + 1, :] = total[:, :256]
        table_ref[2 + h : 3 + h, :] = jnp.broadcast_to(far, (1, 256))
    parts_s[...] = three_parts(table_ref[...])
    pairs = [(out_s.at[1536:], keep_hbm)]
    for i, m in enumerate((m0_hbm, m1_hbm, m2_hbm)):
        pairs += [(out_s.at[512 * i : 512 * (i + 1)], m.at[:512]), (parts_s, m.at[512:])]
    copy_out(pairs, sem)


def own_kernel(x_ref, grad_ref, out_ref):
    placed_product(x_ref, grad_ref, out_ref)


def other_kernel(x_ref, grad_ref, own_hbm, m0_hbm, m1_hbm, m2_hbm, keep_hbm, out_s, sem, sem2):
    pairs = []
    for i, m in enumerate((m0_hbm, m1_hbm, m2_hbm, keep_hbm)):
        rows = slice(512 * i, 512 * (i + 1))
        pairs.append(pltpu.make_async_copy(own_hbm.at[rows], m.at[:, :256], sem2.at[i]))
        pairs[-1].start()
    placed_product(x_ref, grad_ref, out_s)
    copy_out(
        [
            (out_s.at[512 * i : 512 * (i + 1)], m.at[:, 256:])
            for i, m in enumerate((m0_hbm, m1_hbm, m2_hbm, keep_hbm))
        ],
        sem,
    )
    for copy in pairs:
        copy.wait()


def summed(keep_ref, got_refs, rows):
    total = keep_ref[rows].astype(F32)
    for got in got_refs:
        total += got[rows].astype(F32)
    return total


def summed_table(table_in, got_refs, n):
    total = table_in[...]
    for got in got_refs:
        total += table_of(got[n:, :256])
    return total


def merge_kernel(
    keep_ref, a0, a1, a2, keep2_ref, b0, b1, b2, table_in, m0_ref, m1_ref, m2_ref, next_ref, table_ref
):
    total = summed_table(table_in, (a0, a1, a2), 512)
    table_ref[...] = total
    parts = three_parts(total)
    for i, out in enumerate((m0_ref, m1_ref, m2_ref, next_ref)):
        rows = slice(128 * i, 128 * (i + 1))
        out[:128, :256] = summed(keep_ref, (a0, a1, a2), rows).astype(BF16)
        out[:128, 256:] = summed(keep2_ref, (b0, b1, b2), rows).astype(BF16)
        if i < 3:
            out[128:, :256] = parts
            out[128:, 256:] = jnp.zeros((EXTRA, 512), BF16)


def split_kernel(keep_ref, g0, g1, g2, table_in, one_ref, two_ref, three_ref, own_ref, table_ref):
    n = own_ref.shape[0]
    total = summed_table(table_in, (g0, g1, g2), 2 * n)
    table_ref[...] = total
    far = summed(keep_ref, (g0, g1, g2), slice(0, n))
    one_ref[:n] = far[:, :512].astype(BF16)
    one_ref[n:, :256] = three_parts(total)
    one_ref[n:, 256:] = jnp.zeros((EXTRA, 256), BF16)
    two_ref[...] = far[:, 512:].astype(BF16)
    near = summed(keep_ref, (g0, g1, g2), slice(n, 2 * n))
    own_ref[...] = near[:, :512]
    three_ref[...] = near[:, 512:]


def output_kernel(own_ref, one_ref, two_ref, three_ref, table_in, q_ref, k_ref, v_ref, table_ref):
    core = lax.axis_index("core")
    n = own_ref.shape[0]
    table = table_in[...] + table_of(one_ref[n:, :256])
    table_ref[:, :256] = table[:2]
    table_ref[:, 256:] = table[2:, :1]
    own = own_ref[...] + one_ref[:n].astype(F32)
    got = three_ref[...] + two_ref[...].astype(F32)
    q_ref[...] = own[:, :256]

    @pl.when(core == 0)
    def _():
        k_ref[...] = own[:, 256:]
        v_ref[...] = got

    @pl.when(core == 1)
    def _():
        v_ref[...] = own[:, 256:]
        k_ref[...] = got


def sds(shape, dtype):
    return jax.ShapeDtypeStruct(shape, dtype)


def whole(shape):
    return pl.BlockSpec(shape, lambda *_: (0,) * len(shape))


def cost(flops, byte_count):
    return pl.CostEstimate(flops=flops, bytes_accessed=byte_count, transcendentals=0)


def params(limit=None):
    return pltpu.CompilerParams(dimension_semantics=("arbitrary",), vmem_limit_bytes=limit or VMEM_LIMIT)


def call(kernel, operands, outs, scratch=(), grid=(1,), flops=1 << 20, blocks=None, any_outs=(), any_ins=(), limit=None):
    specs = [pl.BlockSpec(memory_space=pltpu.HBM) if i in any_ins else whole(x.shape) for i, x in enumerate(operands)]
    for at, shape in (blocks or {}).items():
        specs[at] = whole(shape)
    out_specs = [pl.BlockSpec(memory_space=pl.ANY) if i in any_outs else whole(x.shape) for i, x in enumerate(outs)]
    moved = sum(x.size * x.dtype.itemsize for x in (*operands, *outs))
    return pl.pallas_call(
        kernel,
        grid=grid,
        in_specs=specs,
        out_specs=out_specs,
        out_shape=list(outs),
        scratch_shapes=list(scratch),
        compiler_params=params(limit),
        cost_estimate=cost(flops, moved),
    )(*operands)


def neighbour(block, distance):
    count = NZ * NX
    route = [(i, i + distance) for i in range(count) if 0 <= i + distance < count]
    return lax.ppermute(block, SP, route)


def staged(inputs, w_query, w_key, w_value, rel_table, out_grad):
    f32, b16 = (lambda *s: sds(s, F32)), (lambda *s: sds(s, BF16))
    v32, v16 = (lambda *s: pltpu.VMEM(s, F32)), (lambda *s: pltpu.VMEM(s, BF16))
    tile_flops = 6 * 2 * TILE * BAND * HDIM
    in_hbm = tuple(pltpu.with_memory_space_constraint(v, pltpu.HBM) for v in (inputs, w_key, w_value))
    tail, wk, wv = call(
        load_kernel, in_hbm, (b16(REACH, 512), b16(2048, 256), b16(2048, 256)),
        (v16(REACH, 2048), pltpu.SemaphoreType.DMA((3,))), flops=2 * 256 * 2048 * 512, any_ins=(0, 1, 2),
        limit=LOAD_LIMIT,
    )
    x, wq = inputs, w_query
    halo = neighbour(tail, 1)
    query, key, value = call(
        proj_kernel, (x, wq, wk, wv), (b16(1024, 256),) * 3,
        flops=2 * 1024 * 2048 * 768,
    )
    block = (REACH, 256)
    span = 1024 - LATE
    pattern = f32(2, BAND, TILE)
    dq_late, acc, bias, pat = call(
        late_kernel, (query, key, value, out_grad, rel_table),
        (b16(span - REACH, 256), f32(span, 512), pattern, pattern),
        (v16(256, span), v16(256, span), v32(span, 256), v32(span, 256)), flops=6 * tile_flops,
    )
    dq0, edge, back, pat = call(
        first_kernel, (query, key, value, halo, out_grad, bias, pat),
        (b16(REACH, 256), f32(REACH, 512), b16(REACH, 512), pattern),
        (v16(512, 256), v16(512, 256), v16(256, 512), v16(256, 512), v32(512, 256), v32(512, 256)),
        flops=4 * tile_flops, blocks={0: block, 1: block, 2: block, 4: block},
    )
    back = neighbour(back, -1)
    dq, kg, vg, edge, pat = call(
        attn_kernel, (query, key, value, out_grad, bias, pat, edge, acc, dq0, dq_late),
        (b16(1024, 256), b16(768, 256), b16(768, 256), f32(REACH, 512), pattern),
        (v16(256, LATE + REACH), v16(256, LATE + REACH), v32(LATE + REACH, 256), v32(LATE + REACH, 256)), flops=6 * tile_flops,
    )
    product = 2 * 1024 * 2048 * 256
    dma = pltpu.SemaphoreType.DMA
    *send, keep, table = call(
        query_kernel, (x, dq, pat), (b16(512 + EXTRA, 256),) * 3 + (b16(512, 256), f32(4, 256)),
        (v16(2048, 256), v16(EXTRA, 256), v32(8, 640), dma((7,))), flops=product, any_outs=(0, 1, 2, 3),
    )
    a = exchange_quarters(send, 0)
    own, swap = call(finish_kernel, (kg, vg, edge, back), (b16(1024, 256),) * 2)
    got = core_swap(swap)
    (placed,) = call(own_kernel, (x, own), (b16(2048, 256),), flops=product)
    *send2, keep2 = call(
        other_kernel, (x, got, placed), (b16(512, 512),) * 4,
        (v16(2048, 256), dma((4,)), dma((4,))), flops=product, any_outs=(0, 1, 2, 3), any_ins=(2,),
    )
    b = exchange_quarters(send2, 0)
    dq, kg, vg = call(
        emit_kernel, (dq, own, swap), (b16(1024, 256),) * 3, (dma((3,)),),
        any_ins=(0, 1, 2), any_outs=(0, 1, 2),
    )
    *send, keep, table = call(
        merge_kernel, (keep, *a, keep2, *b, table),
        (b16(128 + EXTRA, 768),) * 3 + (b16(128, 768), f32(4, 256)),
    )
    c = exchange_quarters(send, 2)
    one, two, three, own, table = call(
        split_kernel, (keep, *c, table),
        (b16(64 + EXTRA, 512), b16(64, 256), f32(64, 256), f32(64, 512), f32(4, 256)),
    )
    one = exchange(one, (4,))
    two = exchange(two, (4,), across=1)
    three = core_swap(three)
    dwq, dwk, dwv, table = call(
        output_kernel, (own, one, two, three, table), (f32(64, 256),) * 3 + (f32(*rel_table.shape),)
    )
    return dq, kg, vg, dwq, dwk, dwv, table


def solution(mesh):
    torus = Mesh(mesh.devices.reshape(NZ, NX, -1, 2), SP + ("row", "core"))
    tp = ("row", "core")
    in_specs = (P(SP, None), P(None, tp), P(None, tp), P(None, tp), P(tp, None), P(SP, tp))
    out_specs = (P(SP, tp),) * 6 + (P(tp, None),)
    return jax.shard_map(staged, mesh=torus, in_specs=in_specs, out_specs=out_specs, check_vma=False)
```

```python
import jax
import jax.numpy as jnp
from jax import lax
from jax.experimental import pallas as pl
from jax.experimental.pallas import tpu as pltpu
from jax.sharding import Mesh
from jax.sharding import PartitionSpec as P


HDIM = 128
SEG = 64
PREV = 4
REACH = PREV * SEG
TILE = 128
BAND = REACH + TILE
SP = ("sp_0", "sp_1")
NZ, NX = 8, 4
ROWS = 64
EXTRA = 16
LATE = 384
VMEM_LIMIT = 24 << 20
CHUNKS = 4
WIDTH = 2048 // CHUNKS
SCALE = HDIM ** (-0.5)
F32 = jnp.float32
BF16 = jnp.bfloat16


def odd_pair(i):
    return i ^ 1


def even_pair(n):
    return lambda i: (i + 1) % n if i % 2 else (i - 1) % n


XO, XE = ("sp_1", odd_pair), ("sp_1", even_pair(NX))
ZO, ZE = ("sp_0", odd_pair), ("sp_0", even_pair(NZ))
Z3 = ("sp_0", lambda i: (3, 6, 5, 0, 7, 2, 1, 4)[i])
LEVELS = ((XO, XE, ZO, ZE, Z3), (ZO, ZE, XO, XE, Z3))


def held_order(steps, device):
    if not steps:
        return [device]
    return held_order(steps[1:], steps[0](device)) + held_order(steps[1:], device)


def axis_codes(levels, axis):
    n = NZ if axis == "sp_0" else NX
    mine = [f for a, f in levels if a == axis]
    spots = [len(levels) - 1 - i for i, (a, _) in enumerate(levels) if a == axis]
    wanted = [0] * n
    for device in range(n):
        order = held_order(mine, device)
        assert sorted(order) == list(range(n))
        for at, unit in enumerate(order):
            wanted[unit] |= at << (4 * device)
    me = lax.axis_index(axis)
    codes = []
    for packed in wanted:
        at = jnp.int32(0)
        for device in range(n):
            at = jnp.where(me == device, jnp.int32((packed >> (4 * device)) & 15), at)
        code = jnp.int32(0)
        for i, spot in enumerate(spots):
            code = code | (((at >> (len(spots) - 1 - i)) & 1) << spot)
        codes.append(code)
    return codes


def unit_places():
    core = lax.axis_index("core")
    places = []
    for levels in LEVELS:
        along_z, along_x = axis_codes(levels, "sp_0"), axis_codes(levels, "sp_1")
        places.append([along_z[unit // NX] + along_x[unit % NX] for unit in range(NZ * NX)])
    return [jnp.where(core == 0, a, b) for a, b in zip(*places)]


def level_route(steps, across=0):
    route = []
    for core, levels in enumerate(LEVELS):
        for z in range(NZ):
            for x in range(NX):
                at = {"sp_0": z, "sp_1": x}
                for step in steps:
                    axis, f = levels[step]
                    at[axis] = f(at[axis])
                to = at["sp_0"] * NX + at["sp_1"]
                route.append(((z * NX + x) * 2 + core, to * 2 + (core ^ across)))
    return route


def exchange(block, steps, across=0):
    return lax.ppermute(block, SP + ("core",), level_route(steps, across))


def exchange_quarters(blocks, level):
    paths = ((level, level + 1), (level,), (level + 1,))
    return [exchange(x, path) for x, path in zip(blocks, paths)]


def core_swap(block):
    return lax.ppermute(block, "core", [(0, 1), (1, 0)])


def dot(a, b, contract=((1,), (0,))):
    return lax.dot_general(a, b, (contract, ((), ())), preferred_element_type=F32)


def tile_grads(query, grad, key, value, key_t, value_t, bias):
    scores = dot(key, query, ((1,), (1,))) * SCALE + bias
    top = jnp.max(scores, axis=0, keepdims=True)
    raised = jnp.exp(scores - top)
    probs = raised * (1.0 / jnp.sum(raised, axis=0, keepdims=True))
    probs_low = probs.astype(BF16)
    attn_out = dot(value_t, probs_low).astype(BF16).astype(F32)
    out_dot = jnp.sum(attn_out * grad.T.astype(F32), axis=0, keepdims=True)
    value_part = dot(probs_low, grad)
    score_grad = probs * (dot(value, grad, ((1,), (1,))) - out_dot)
    score_low = score_grad.astype(BF16)
    query_part = (dot(key_t, score_low) * SCALE).T
    key_part = dot(score_low, query) * SCALE
    return score_grad, query_part, key_part, value_part


def load_kernel(x_hbm, wk_hbm, wv_hbm, tail_ref, wk_ref, wv_ref, x_ref, sem):
    pairs = ((wk_hbm, wk_ref), (x_hbm.at[1024 - REACH :], x_ref), (wv_hbm, wv_ref))
    copies = [pltpu.make_async_copy(src, dst, sem.at[i]) for i, (src, dst) in enumerate(pairs)]
    for copy in copies:
        copy.start()
    for copy in copies[:2]:
        copy.wait()
    tail_ref[:, :256] = dot(x_ref[...], wk_ref[...]).astype(BF16)
    copies[2].wait()
    tail_ref[:, 256:] = dot(x_ref[...], wv_ref[...]).astype(BF16)


def proj_kernel(x_hbm, wq_hbm, wk_ref, wv_ref, x_tail, tail_ref, q_ref, k_ref, v_ref, x_ref, wq_s, sem):
    top = 1024 - REACH
    pairs = [(x_hbm.at[c : c + REACH], x_ref.at[c : c + REACH]) for c in range(0, top, REACH)]
    pairs += [(wq_hbm, wq_s)]
    copies = [pltpu.make_async_copy(src, dst, sem.at[i]) for i, (src, dst) in enumerate(pairs)]
    for copy in copies:
        copy.start()
    x_ref[top:] = x_tail[...]
    k_ref[top:] = tail_ref[:, :256]
    v_ref[top:] = tail_ref[:, 256:]
    for i, c in enumerate(range(0, top, REACH)):
        copies[i].wait()
        x = x_ref[c : c + REACH]
        k_ref[c : c + REACH] = dot(x, wk_ref[...]).astype(BF16)
        v_ref[c : c + REACH] = dot(x, wv_ref[...]).astype(BF16)
    copies[-1].wait()
    q_ref[...] = dot(x_ref[...], wq_s[...]).astype(BF16)


def tiles(which, q_ref, k_ref, v_ref, og_ref, bias_ref, kt_s, vt_s, pat_ref, dq_ref, dq_at, ka_s, va_s, acc_at):
    for tile in which:
        rows = slice(REACH + tile * TILE, REACH + (tile + 1) * TILE)
        band = slice(tile * TILE, tile * TILE + BAND)
        to = slice(band.start - acc_at, band.stop - acc_at)
        for h in range(2):
            cols = slice(h * HDIM, (h + 1) * HDIM)
            score_grad, query_part, key_part, value_part = tile_grads(
                q_ref[rows, cols], og_ref[rows, cols], k_ref[band, cols], v_ref[band, cols],
                kt_s[cols, to], vt_s[cols, to], bias_ref[h],
            )
            pat_ref[h] += score_grad
            dq_ref[rows.start - dq_at : rows.stop - dq_at, cols] = query_part.astype(BF16)
            ka_s[to, cols] += key_part
            va_s[to, cols] += value_part


def late_kernel(
    q_ref, k_ref, v_ref, og_ref, rel_ref,
    dq_ref, acc_ref, bias_ref, pat_ref,
    kt_s, vt_s, ka_s, va_s,
):
    u = lax.broadcasted_iota(jnp.int32, (BAND, TILE), 0)
    col = lax.broadcasted_iota(jnp.int32, (BAND, TILE), 1)
    low = jnp.where(col < SEG, 0, SEG)
    inside = (u >= low) & (u < low + REACH + SEG)
    for h in range(2):
        table = rel_ref[h : h + 1, :]
        far = jnp.concatenate([table[:, :256], jnp.broadcast_to(table[:, 256:257], (1, 256))], axis=1)
        far = jnp.broadcast_to(far, (BAND, 512))
        skew = pltpu.roll(far, 0, 1, stride=1, stride_axis=0)[:, BAND:]
        bias_ref[h] = jnp.where(inside, skew, -jnp.inf)
    pat_ref[...] = jnp.zeros_like(pat_ref)
    kt_s[...] = k_ref[LATE:].T
    vt_s[...] = v_ref[LATE:].T
    ka_s[...] = jnp.zeros_like(ka_s)
    va_s[...] = jnp.zeros_like(va_s)
    tiles(
        range(LATE // TILE, 6), q_ref, k_ref, v_ref, og_ref, bias_ref, kt_s, vt_s, pat_ref, dq_ref, LATE + REACH,
        ka_s, va_s, LATE,
    )
    acc_ref[:, :256] = ka_s[...]
    acc_ref[:, 256:] = va_s[...]


def first_kernel(
    q_ref, k_ref, v_ref, halo_ref, og_ref, bias_ref, pat_in,
    dq_ref, edge_ref, back_ref, pat_ref,
    k_s, v_s, kt_s, vt_s, ka_s, va_s,
):
    k_s[:REACH] = halo_ref[:, :256]
    v_s[:REACH] = halo_ref[:, 256:]
    k_s[REACH:] = k_ref[...]
    v_s[REACH:] = v_ref[...]
    kt_s[...] = k_s[...].T
    vt_s[...] = v_s[...].T
    ka_s[...] = jnp.zeros_like(ka_s)
    va_s[...] = jnp.zeros_like(va_s)
    pat_ref[...] = pat_in[...]
    outside = (lax.axis_index("sp_0") == 0) & (lax.axis_index("sp_1") == 0)
    u = lax.broadcasted_iota(jnp.int32, (BAND, TILE), 0)
    for t in range(2):
        rows = slice(t * TILE, (t + 1) * TILE)
        band = slice(t * TILE, t * TILE + BAND)
        for h in range(2):
            cols = slice(h * HDIM, (h + 1) * HDIM)
            bias = jnp.where(outside & (u < REACH - t * TILE), -jnp.inf, bias_ref[h])
            score_grad, query_part, key_part, value_part = tile_grads(
                q_ref[rows, cols], og_ref[rows, cols], k_s[band, cols], v_s[band, cols],
                kt_s[cols, band], vt_s[cols, band], bias,
            )
            pat_ref[h] += score_grad
            dq_ref[rows, cols] = query_part.astype(BF16)
            ka_s[band, cols] += key_part
            va_s[band, cols] += value_part
    edge_ref[:, :256] = ka_s[REACH:]
    edge_ref[:, 256:] = va_s[REACH:]
    back_ref[:, :256] = ka_s[:REACH].astype(BF16)
    back_ref[:, 256:] = va_s[:REACH].astype(BF16)


def attn_kernel(
    q_ref, k_ref, v_ref, og_ref, bias_ref, pat_in, edge_in, acc_in, dq_in, dq_late,
    near_ref, kg_ref, vg_ref, edge_ref, pat_ref,
    kt_s, vt_s, ka_s, va_s,
):
    kt_s[...] = k_ref[: LATE + REACH].T
    vt_s[...] = v_ref[: LATE + REACH].T
    ka_s[:REACH] = edge_in[:, :256]
    va_s[:REACH] = edge_in[:, 256:]
    if LATE > REACH:
        ka_s[REACH:LATE] = jnp.zeros((LATE - REACH, 256), F32)
        va_s[REACH:LATE] = jnp.zeros((LATE - REACH, 256), F32)
    ka_s[LATE:] = acc_in[: LATE + REACH - LATE, :256]
    va_s[LATE:] = acc_in[: LATE + REACH - LATE, 256:]
    pat_ref[...] = pat_in[...]
    near_ref[:REACH] = dq_in[...]
    near_ref[LATE + REACH :] = dq_late[...]
    tiles(range(LATE // TILE), q_ref, k_ref, v_ref, og_ref, bias_ref, kt_s, vt_s, pat_ref, near_ref, 0, ka_s, va_s, 0)
    last = LATE + REACH
    kg_ref[:last] = ka_s[...].astype(BF16)
    vg_ref[:last] = va_s[...].astype(BF16)
    kg_ref[last:] = acc_in[last - LATE : 768 - LATE, :256].astype(BF16)
    vg_ref[last:] = acc_in[last - LATE : 768 - LATE, 256:].astype(BF16)
    edge_ref[...] = acc_in[768 - LATE :]


def finish_kernel(kg_in, vg_in, edge_ref, back_ref, own_ref, swap_ref):
    core = lax.axis_index("core")
    key = (edge_ref[:, :256] + back_ref[:, :256].astype(F32)).astype(BF16)
    value = (edge_ref[:, 256:] + back_ref[:, 256:].astype(F32)).astype(BF16)

    def put(to_key, to_value):
        to_key[:768] = kg_in[...]
        to_value[:768] = vg_in[...]
        to_key[768:] = key
        to_value[768:] = value

    @pl.when(core == 0)
    def _():
        put(own_ref, swap_ref)

    @pl.when(core == 1)
    def _():
        put(swap_ref, own_ref)


def emit_kernel(dq_in, own_in, swap_in, dq_ref, kg_ref, vg_ref, sem):
    core = lax.axis_index("core")
    query = pltpu.make_async_copy(dq_in, dq_ref, sem.at[0])
    query.start()

    @pl.when(core == 0)
    def _():
        copy_out([(own_in, kg_ref), (swap_in, vg_ref)], sem.at[1:])

    @pl.when(core == 1)
    def _():
        copy_out([(swap_in, kg_ref), (own_in, vg_ref)], sem.at[1:])

    query.wait()


def store_units(value, chunk, places, out_s):
    units = WIDTH // ROWS
    for i in range(units):
        at = pl.multiple_of(places[chunk * units + i] * ROWS, ROWS)
        out_s[pl.ds(at, ROWS), :] = value[i * ROWS : (i + 1) * ROWS].astype(BF16)


def placed_product(x_ref, grad_ref, out_s):
    places = unit_places()
    for c in range(CHUNKS):
        cols = slice(c * WIDTH, (c + 1) * WIDTH)
        store_units(dot(x_ref[:, cols], grad_ref[...], ((0,), (0,))), c, places, out_s)


def three_parts(table):
    high = table.astype(BF16).astype(F32)
    mid = (table - high).astype(BF16).astype(F32)
    low = table - high - mid
    rest = jnp.zeros((EXTRA - 12, table.shape[1]), F32)
    return jnp.concatenate([high, mid, low, rest], axis=0).astype(BF16)


def table_of(parts):
    parts = parts.astype(F32)
    return parts[0:4] + parts[4:8] + parts[8:12]


def copy_out(pairs, sem):
    copies = [pltpu.make_async_copy(src, dst, sem.at[i]) for i, (src, dst) in enumerate(pairs)]
    for copy in copies:
        copy.start()
    for copy in copies:
        copy.wait()


def query_kernel(
    x_ref, grad_ref, pat_ref, m0_hbm, m1_hbm, m2_hbm, keep_hbm, table_ref, out_s, parts_s, diag_s, sem
):
    placed_product(x_ref, grad_ref, out_s)
    for h in range(2):
        diag_s[...] = jnp.zeros_like(diag_s)
        for a in range(BAND // 8):
            off = BAND - 8 * a
            diag_s[:, off : off + TILE] += pat_ref[h, 8 * a : 8 * a + 8, :]
        total = jnp.zeros((1, 512), F32)
        for s in range(8):
            total += diag_s[s : s + 1, s : s + 512]
        far = jnp.sum(total[:, 256:], axis=1, keepdims=True)
        table_ref[h : h + 1, :] = total[:, :256]
        table_ref[2 + h : 3 + h, :] = jnp.broadcast_to(far, (1, 256))
    parts_s[...] = three_parts(table_ref[...])
    pairs = [(out_s.at[1536:], keep_hbm)]
    for i, m in enumerate((m0_hbm, m1_hbm, m2_hbm)):
        pairs += [(out_s.at[512 * i : 512 * (i + 1)], m.at[:512]), (parts_s, m.at[512:])]
    copy_out(pairs, sem)


def own_kernel(x_ref, grad_ref, out_ref):
    placed_product(x_ref, grad_ref, out_ref)


def other_kernel(x_ref, grad_ref, own_hbm, m0_hbm, m1_hbm, m2_hbm, keep_hbm, out_s, sem, sem2):
    pairs = []
    for i, m in enumerate((m0_hbm, m1_hbm, m2_hbm, keep_hbm)):
        rows = slice(512 * i, 512 * (i + 1))
        pairs.append(pltpu.make_async_copy(own_hbm.at[rows], m.at[:, :256], sem2.at[i]))
        pairs[-1].start()
    placed_product(x_ref, grad_ref, out_s)
    copy_out(
        [
            (out_s.at[512 * i : 512 * (i + 1)], m.at[:, 256:])
            for i, m in enumerate((m0_hbm, m1_hbm, m2_hbm, keep_hbm))
        ],
        sem,
    )
    for copy in pairs:
        copy.wait()


def summed(keep_ref, got_refs, rows):
    total = keep_ref[rows].astype(F32)
    for got in got_refs:
        total += got[rows].astype(F32)
    return total


def summed_table(table_in, got_refs, n):
    total = table_in[...]
    for got in got_refs:
        total += table_of(got[n:, :256])
    return total


def merge_kernel(
    keep_ref, a0, a1, a2, keep2_ref, b0, b1, b2, table_in, m0_ref, m1_ref, m2_ref, next_ref, table_ref
):
    total = summed_table(table_in, (a0, a1, a2), 512)
    table_ref[...] = total
    parts = three_parts(total)
    for i, out in enumerate((m0_ref, m1_ref, m2_ref, next_ref)):
        rows = slice(128 * i, 128 * (i + 1))
        out[:128, :256] = summed(keep_ref, (a0, a1, a2), rows).astype(BF16)
        out[:128, 256:] = summed(keep2_ref, (b0, b1, b2), rows).astype(BF16)
        if i < 3:
            out[128:, :256] = parts
            out[128:, 256:] = jnp.zeros((EXTRA, 512), BF16)


def split_kernel(keep_ref, g0, g1, g2, table_in, one_ref, two_ref, three_ref, own_ref, table_ref):
    n = own_ref.shape[0]
    total = summed_table(table_in, (g0, g1, g2), 2 * n)
    table_ref[...] = total
    far = summed(keep_ref, (g0, g1, g2), slice(0, n))
    one_ref[:n] = far[:, :512].astype(BF16)
    one_ref[n:, :256] = three_parts(total)
    one_ref[n:, 256:] = jnp.zeros((EXTRA, 256), BF16)
    two_ref[...] = far[:, 512:].astype(BF16)
    near = summed(keep_ref, (g0, g1, g2), slice(n, 2 * n))
    own_ref[...] = near[:, :512]
    three_ref[...] = near[:, 512:]


def output_kernel(own_ref, one_ref, two_ref, three_ref, table_in, q_ref, k_ref, v_ref, table_ref):
    core = lax.axis_index("core")
    n = own_ref.shape[0]
    table = table_in[...] + table_of(one_ref[n:, :256])
    table_ref[:, :256] = table[:2]
    table_ref[:, 256:] = table[2:, :1]
    own = own_ref[...] + one_ref[:n].astype(F32)
    got = three_ref[...] + two_ref[...].astype(F32)
    q_ref[...] = own[:, :256]

    @pl.when(core == 0)
    def _():
        k_ref[...] = own[:, 256:]
        v_ref[...] = got

    @pl.when(core == 1)
    def _():
        v_ref[...] = own[:, 256:]
        k_ref[...] = got


def sds(shape, dtype):
    return jax.ShapeDtypeStruct(shape, dtype)


def whole(shape):
    return pl.BlockSpec(shape, lambda *_: (0,) * len(shape))


def cost(flops, byte_count):
    return pl.CostEstimate(flops=flops, bytes_accessed=byte_count, transcendentals=0)


def params(limit=None):
    return pltpu.CompilerParams(dimension_semantics=("arbitrary",), vmem_limit_bytes=limit or VMEM_LIMIT)


def call(kernel, operands, outs, scratch=(), grid=(1,), flops=1 << 20, blocks=None, any_outs=(), any_ins=(), limit=None):
    specs = [pl.BlockSpec(memory_space=pltpu.HBM) if i in any_ins else whole(x.shape) for i, x in enumerate(operands)]
    for at, shape in (blocks or {}).items():
        specs[at] = whole(shape)
    out_specs = [pl.BlockSpec(memory_space=pl.ANY) if i in any_outs else whole(x.shape) for i, x in enumerate(outs)]
    moved = sum(x.size * x.dtype.itemsize for x in (*operands, *outs))
    return pl.pallas_call(
        kernel,
        grid=grid,
        in_specs=specs,
        out_specs=out_specs,
        out_shape=list(outs),
        scratch_shapes=list(scratch),
        compiler_params=params(limit),
        cost_estimate=cost(flops, moved),
    )(*operands)


def neighbour(block, distance):
    count = NZ * NX
    route = [(i, i + distance) for i in range(count) if 0 <= i + distance < count]
    return lax.ppermute(block, SP, route)


def staged(inputs, w_query, w_key, w_value, rel_table, out_grad):
    f32, b16 = (lambda *s: sds(s, F32)), (lambda *s: sds(s, BF16))
    v32, v16 = (lambda *s: pltpu.VMEM(s, F32)), (lambda *s: pltpu.VMEM(s, BF16))
    tile_flops = 6 * 2 * TILE * BAND * HDIM
    x_hbm, wq_hbm, wk_hbm, wv_hbm = (
        pltpu.with_memory_space_constraint(v, pltpu.HBM) for v in (inputs, w_query, w_key, w_value)
    )
    dma = pltpu.SemaphoreType.DMA
    tail, wk, wv, x_tail = call(
        load_kernel, (x_hbm, wk_hbm, wv_hbm),
        (b16(REACH, 512), b16(2048, 256), b16(2048, 256), b16(REACH, 2048)),
        (dma((3,)),), flops=2 * 256 * 2048 * 512, any_ins=(0, 1, 2),
    )
    halo = neighbour(tail, 1)
    query, key, value, x = call(
        proj_kernel, (x_hbm, wq_hbm, wk, wv, x_tail, tail),
        (b16(1024, 256),) * 3 + (b16(1024, 2048),), (v16(2048, 256), dma((4,))),
        flops=2 * 1024 * 2048 * 768, any_ins=(0, 1),
    )
    block = (REACH, 256)
    span = 1024 - LATE
    pattern = f32(2, BAND, TILE)
    dq_late, acc, bias, pat = call(
        late_kernel, (query, key, value, out_grad, rel_table),
        (b16(span - REACH, 256), f32(span, 512), pattern, pattern),
        (v16(256, span), v16(256, span), v32(span, 256), v32(span, 256)), flops=6 * tile_flops,
    )
    dq0, edge, back, pat = call(
        first_kernel, (query, key, value, halo, out_grad, bias, pat),
        (b16(REACH, 256), f32(REACH, 512), b16(REACH, 512), pattern),
        (v16(512, 256), v16(512, 256), v16(256, 512), v16(256, 512), v32(512, 256), v32(512, 256)),
        flops=4 * tile_flops, blocks={0: block, 1: block, 2: block, 4: block},
    )
    back = neighbour(back, -1)
    dq, kg, vg, edge, pat = call(
        attn_kernel, (query, key, value, out_grad, bias, pat, edge, acc, dq0, dq_late),
        (b16(1024, 256), b16(768, 256), b16(768, 256), f32(REACH, 512), pattern),
        (v16(256, LATE + REACH), v16(256, LATE + REACH), v32(LATE + REACH, 256), v32(LATE + REACH, 256)), flops=6 * tile_flops,
    )
    product = 2 * 1024 * 2048 * 256
    *send, keep, table = call(
        query_kernel, (x, dq, pat), (b16(512 + EXTRA, 256),) * 3 + (b16(512, 256), f32(4, 256)),
        (v16(2048, 256), v16(EXTRA, 256), v32(8, 640), dma((7,))), flops=product, any_outs=(0, 1, 2, 3),
    )
    a = exchange_quarters(send, 0)
    own, swap = call(finish_kernel, (kg, vg, edge, back), (b16(1024, 256),) * 2)
    got = core_swap(swap)
    (placed,) = call(own_kernel, (x, own), (b16(2048, 256),), flops=product)
    *send2, keep2 = call(
        other_kernel, (x, got, placed), (b16(512, 512),) * 4,
        (v16(2048, 256), dma((4,)), dma((4,))), flops=product, any_outs=(0, 1, 2, 3), any_ins=(2,),
    )
    b = exchange_quarters(send2, 0)
    dq, kg, vg = call(
        emit_kernel, (dq, own, swap), (b16(1024, 256),) * 3, (dma((3,)),),
        any_ins=(0, 1, 2), any_outs=(0, 1, 2),
    )
    *send, keep, table = call(
        merge_kernel, (keep, *a, keep2, *b, table),
        (b16(128 + EXTRA, 768),) * 3 + (b16(128, 768), f32(4, 256)),
    )
    c = exchange_quarters(send, 2)
    one, two, three, own, table = call(
        split_kernel, (keep, *c, table),
        (b16(64 + EXTRA, 512), b16(64, 256), f32(64, 256), f32(64, 512), f32(4, 256)),
    )
    one = exchange(one, (4,))
    two = exchange(two, (4,), across=1)
    three = core_swap(three)
    dwq, dwk, dwv, table = call(
        output_kernel, (own, one, two, three, table), (f32(64, 256),) * 3 + (f32(*rel_table.shape),)
    )
    return dq, kg, vg, dwq, dwk, dwv, table


def solution(mesh):
    torus = Mesh(mesh.devices.reshape(NZ, NX, -1, 2), SP + ("row", "core"))
    tp = ("row", "core")
    in_specs = (P(SP, None), P(None, tp), P(None, tp), P(None, tp), P(tp, None), P(SP, tp))
    out_specs = (P(SP, tp),) * 6 + (P(tp, None),)
    return jax.shard_map(staged, mesh=torus, in_specs=in_specs, out_specs=out_specs, check_vma=False)
```

```python
import jax
import jax.numpy as jnp
from jax import lax
from jax.experimental import pallas as pl
from jax.experimental.pallas import tpu as pltpu
from jax.sharding import Mesh
from jax.sharding import PartitionSpec as P


HDIM = 128
SEG = 64
PREV = 4
REACH = PREV * SEG
TILE = 128
BAND = REACH + TILE
SP = ("sp_0", "sp_1")
NZ, NX = 8, 4
ROWS = 64
EXTRA = 16
LATE = 384
VMEM_LIMIT = 24 << 20
CHUNKS = 4
WIDTH = 2048 // CHUNKS
SCALE = HDIM ** (-0.5)
F32 = jnp.float32
BF16 = jnp.bfloat16


def odd_pair(i):
    return i ^ 1


def even_pair(n):
    return lambda i: (i + 1) % n if i % 2 else (i - 1) % n


XO, XE = ("sp_1", odd_pair), ("sp_1", even_pair(NX))
ZO, ZE = ("sp_0", odd_pair), ("sp_0", even_pair(NZ))
Z3 = ("sp_0", lambda i: (3, 6, 5, 0, 7, 2, 1, 4)[i])
LEVELS = ((XO, XE, ZO, ZE, Z3), (ZO, ZE, XO, XE, Z3))


def held_order(steps, device):
    if not steps:
        return [device]
    return held_order(steps[1:], steps[0](device)) + held_order(steps[1:], device)


def axis_codes(levels, axis):
    n = NZ if axis == "sp_0" else NX
    mine = [f for a, f in levels if a == axis]
    spots = [len(levels) - 1 - i for i, (a, _) in enumerate(levels) if a == axis]
    wanted = [0] * n
    for device in range(n):
        order = held_order(mine, device)
        assert sorted(order) == list(range(n))
        for at, unit in enumerate(order):
            wanted[unit] |= at << (4 * device)
    me = lax.axis_index(axis)
    codes = []
    for packed in wanted:
        at = jnp.int32(0)
        for device in range(n):
            at = jnp.where(me == device, jnp.int32((packed >> (4 * device)) & 15), at)
        code = jnp.int32(0)
        for i, spot in enumerate(spots):
            code = code | (((at >> (len(spots) - 1 - i)) & 1) << spot)
        codes.append(code)
    return codes


def unit_places():
    core = lax.axis_index("core")
    places = []
    for levels in LEVELS:
        along_z, along_x = axis_codes(levels, "sp_0"), axis_codes(levels, "sp_1")
        places.append([along_z[unit // NX] + along_x[unit % NX] for unit in range(NZ * NX)])
    return [jnp.where(core == 0, a, b) for a, b in zip(*places)]


def level_route(steps, across=0):
    route = []
    for core, levels in enumerate(LEVELS):
        for z in range(NZ):
            for x in range(NX):
                at = {"sp_0": z, "sp_1": x}
                for step in steps:
                    axis, f = levels[step]
                    at[axis] = f(at[axis])
                to = at["sp_0"] * NX + at["sp_1"]
                route.append(((z * NX + x) * 2 + core, to * 2 + (core ^ across)))
    return route


def exchange(block, steps, across=0):
    return lax.ppermute(block, SP + ("core",), level_route(steps, across))


def exchange_quarters(blocks, level):
    paths = ((level, level + 1), (level,), (level + 1,))
    return [exchange(x, path) for x, path in zip(blocks, paths)]


def core_swap(block):
    return lax.ppermute(block, "core", [(0, 1), (1, 0)])


def dot(a, b, contract=((1,), (0,))):
    return lax.dot_general(a, b, (contract, ((), ())), preferred_element_type=F32)


def tile_grads(query, grad, key, value, key_t, value_t, bias):
    scores = dot(key, query, ((1,), (1,))) * SCALE + bias
    top = jnp.max(scores, axis=0, keepdims=True)
    raised = jnp.exp(scores - top)
    probs = raised * (1.0 / jnp.sum(raised, axis=0, keepdims=True))
    probs_low = probs.astype(BF16)
    attn_out = dot(value_t, probs_low).astype(BF16).astype(F32)
    out_dot = jnp.sum(attn_out * grad.T.astype(F32), axis=0, keepdims=True)
    value_part = dot(probs_low, grad)
    score_grad = probs * (dot(value, grad, ((1,), (1,))) - out_dot)
    score_low = score_grad.astype(BF16)
    query_part = (dot(key_t, score_low) * SCALE).T
    key_part = dot(score_low, query) * SCALE
    return score_grad, query_part, key_part, value_part


def load_kernel(x_hbm, wk_hbm, wv_hbm, tail_ref, wk_ref, wv_ref, x_ref, sem):
    halves = (slice(0, 1024), slice(1024, 2048))
    pairs = [(x_hbm.at[1024 - REACH :], x_ref)]
    pairs += [(w_hbm.at[rows], w_ref.at[rows]) for w_hbm, w_ref in ((wk_hbm, wk_ref), (wv_hbm, wv_ref)) for rows in halves]
    copies = [pltpu.make_async_copy(src, dst, sem.at[i]) for i, (src, dst) in enumerate(pairs)]
    for copy in copies:
        copy.start()
    copies[0].wait()
    for at, w_ref in enumerate((wk_ref, wv_ref)):
        total = jnp.zeros((REACH, 256), F32)
        for i, rows in enumerate(halves):
            copies[1 + 2 * at + i].wait()
            total += dot(x_ref[:, rows], w_ref[rows])
        tail_ref[:, 256 * at : 256 * (at + 1)] = total.astype(BF16)


def proj_kernel(x_hbm, wq_hbm, wk_ref, wv_ref, x_tail, tail_ref, q_ref, k_ref, v_ref, x_ref, wq_s, sem):
    top = 1024 - REACH
    pairs = [(x_hbm.at[c : c + REACH], x_ref.at[c : c + REACH]) for c in range(0, top, REACH)]
    pairs += [(wq_hbm, wq_s)]
    copies = [pltpu.make_async_copy(src, dst, sem.at[i]) for i, (src, dst) in enumerate(pairs)]
    for copy in copies:
        copy.start()
    x_ref[top:] = x_tail[...]
    k_ref[top:] = tail_ref[:, :256]
    v_ref[top:] = tail_ref[:, 256:]
    for i, c in enumerate(range(0, top, REACH)):
        copies[i].wait()
        x = x_ref[c : c + REACH]
        k_ref[c : c + REACH] = dot(x, wk_ref[...]).astype(BF16)
        v_ref[c : c + REACH] = dot(x, wv_ref[...]).astype(BF16)
    copies[-1].wait()
    q_ref[...] = dot(x_ref[...], wq_s[...]).astype(BF16)


def tiles(which, q_ref, k_ref, v_ref, og_ref, bias_ref, kt_s, vt_s, pat_ref, dq_ref, dq_at, ka_s, va_s, acc_at):
    for tile in which:
        rows = slice(REACH + tile * TILE, REACH + (tile + 1) * TILE)
        band = slice(tile * TILE, tile * TILE + BAND)
        to = slice(band.start - acc_at, band.stop - acc_at)
        for h in range(2):
            cols = slice(h * HDIM, (h + 1) * HDIM)
            score_grad, query_part, key_part, value_part = tile_grads(
                q_ref[rows, cols], og_ref[rows, cols], k_ref[band, cols], v_ref[band, cols],
                kt_s[cols, to], vt_s[cols, to], bias_ref[h],
            )
            pat_ref[h] += score_grad
            dq_ref[rows.start - dq_at : rows.stop - dq_at, cols] = query_part.astype(BF16)
            ka_s[to, cols] += key_part
            va_s[to, cols] += value_part


def late_kernel(
    q_ref, k_ref, v_ref, og_ref, rel_ref,
    dq_ref, acc_ref, bias_ref, pat_ref,
    kt_s, vt_s, ka_s, va_s,
):
    u = lax.broadcasted_iota(jnp.int32, (BAND, TILE), 0)
    col = lax.broadcasted_iota(jnp.int32, (BAND, TILE), 1)
    low = jnp.where(col < SEG, 0, SEG)
    inside = (u >= low) & (u < low + REACH + SEG)
    for h in range(2):
        table = rel_ref[h : h + 1, :]
        far = jnp.concatenate([table[:, :256], jnp.broadcast_to(table[:, 256:257], (1, 256))], axis=1)
        far = jnp.broadcast_to(far, (BAND, 512))
        skew = pltpu.roll(far, 0, 1, stride=1, stride_axis=0)[:, BAND:]
        bias_ref[h] = jnp.where(inside, skew, -jnp.inf)
    pat_ref[...] = jnp.zeros_like(pat_ref)
    kt_s[...] = k_ref[LATE:].T
    vt_s[...] = v_ref[LATE:].T
    ka_s[...] = jnp.zeros_like(ka_s)
    va_s[...] = jnp.zeros_like(va_s)
    tiles(
        range(LATE // TILE, 6), q_ref, k_ref, v_ref, og_ref, bias_ref, kt_s, vt_s, pat_ref, dq_ref, LATE + REACH,
        ka_s, va_s, LATE,
    )
    acc_ref[:, :256] = ka_s[...]
    acc_ref[:, 256:] = va_s[...]


def first_kernel(
    q_ref, k_ref, v_ref, halo_ref, og_ref, bias_ref, pat_in,
    dq_ref, edge_ref, back_ref, pat_ref,
    k_s, v_s, kt_s, vt_s, ka_s, va_s,
):
    k_s[:REACH] = halo_ref[:, :256]
    v_s[:REACH] = halo_ref[:, 256:]
    k_s[REACH:] = k_ref[...]
    v_s[REACH:] = v_ref[...]
    kt_s[...] = k_s[...].T
    vt_s[...] = v_s[...].T
    ka_s[...] = jnp.zeros_like(ka_s)
    va_s[...] = jnp.zeros_like(va_s)
    pat_ref[...] = pat_in[...]
    outside = (lax.axis_index("sp_0") == 0) & (lax.axis_index("sp_1") == 0)
    u = lax.broadcasted_iota(jnp.int32, (BAND, TILE), 0)
    for t in range(2):
        rows = slice(t * TILE, (t + 1) * TILE)
        band = slice(t * TILE, t * TILE + BAND)
        for h in range(2):
            cols = slice(h * HDIM, (h + 1) * HDIM)
            bias = jnp.where(outside & (u < REACH - t * TILE), -jnp.inf, bias_ref[h])
            score_grad, query_part, key_part, value_part = tile_grads(
                q_ref[rows, cols], og_ref[rows, cols], k_s[band, cols], v_s[band, cols],
                kt_s[cols, band], vt_s[cols, band], bias,
            )
            pat_ref[h] += score_grad
            dq_ref[rows, cols] = query_part.astype(BF16)
            ka_s[band, cols] += key_part
            va_s[band, cols] += value_part
    edge_ref[:, :256] = ka_s[REACH:]
    edge_ref[:, 256:] = va_s[REACH:]
    back_ref[:, :256] = ka_s[:REACH].astype(BF16)
    back_ref[:, 256:] = va_s[:REACH].astype(BF16)


def attn_kernel(
    q_ref, k_ref, v_ref, og_ref, bias_ref, pat_in, edge_in, acc_in, dq_in, dq_late,
    near_ref, kg_ref, vg_ref, edge_ref, pat_ref,
    kt_s, vt_s, ka_s, va_s,
):
    kt_s[...] = k_ref[: LATE + REACH].T
    vt_s[...] = v_ref[: LATE + REACH].T
    ka_s[:REACH] = edge_in[:, :256]
    va_s[:REACH] = edge_in[:, 256:]
    if LATE > REACH:
        ka_s[REACH:LATE] = jnp.zeros((LATE - REACH, 256), F32)
        va_s[REACH:LATE] = jnp.zeros((LATE - REACH, 256), F32)
    ka_s[LATE:] = acc_in[: LATE + REACH - LATE, :256]
    va_s[LATE:] = acc_in[: LATE + REACH - LATE, 256:]
    pat_ref[...] = pat_in[...]
    near_ref[:REACH] = dq_in[...]
    near_ref[LATE + REACH :] = dq_late[...]
    tiles(range(LATE // TILE), q_ref, k_ref, v_ref, og_ref, bias_ref, kt_s, vt_s, pat_ref, near_ref, 0, ka_s, va_s, 0)
    last = LATE + REACH
    kg_ref[:last] = ka_s[...].astype(BF16)
    vg_ref[:last] = va_s[...].astype(BF16)
    kg_ref[last:] = acc_in[last - LATE : 768 - LATE, :256].astype(BF16)
    vg_ref[last:] = acc_in[last - LATE : 768 - LATE, 256:].astype(BF16)
    edge_ref[...] = acc_in[768 - LATE :]


def finish_kernel(kg_in, vg_in, edge_ref, back_ref, own_ref, swap_ref):
    core = lax.axis_index("core")
    key = (edge_ref[:, :256] + back_ref[:, :256].astype(F32)).astype(BF16)
    value = (edge_ref[:, 256:] + back_ref[:, 256:].astype(F32)).astype(BF16)

    def put(to_key, to_value):
        to_key[:768] = kg_in[...]
        to_value[:768] = vg_in[...]
        to_key[768:] = key
        to_value[768:] = value

    @pl.when(core == 0)
    def _():
        put(own_ref, swap_ref)

    @pl.when(core == 1)
    def _():
        put(swap_ref, own_ref)


def emit_kernel(dq_in, own_in, swap_in, dq_ref, kg_ref, vg_ref, sem):
    core = lax.axis_index("core")
    query = pltpu.make_async_copy(dq_in, dq_ref, sem.at[0])
    query.start()

    @pl.when(core == 0)
    def _():
        copy_out([(own_in, kg_ref), (swap_in, vg_ref)], sem.at[1:])

    @pl.when(core == 1)
    def _():
        copy_out([(swap_in, kg_ref), (own_in, vg_ref)], sem.at[1:])

    query.wait()


def store_units(value, chunk, places, out_s):
    units = WIDTH // ROWS
    for i in range(units):
        at = pl.multiple_of(places[chunk * units + i] * ROWS, ROWS)
        out_s[pl.ds(at, ROWS), :] = value[i * ROWS : (i + 1) * ROWS].astype(BF16)


def placed_product(x_ref, grad_ref, out_s):
    places = unit_places()
    for c in range(CHUNKS):
        cols = slice(c * WIDTH, (c + 1) * WIDTH)
        store_units(dot(x_ref[:, cols], grad_ref[...], ((0,), (0,))), c, places, out_s)


def three_parts(table):
    high = table.astype(BF16).astype(F32)
    mid = (table - high).astype(BF16).astype(F32)
    low = table - high - mid
    rest = jnp.zeros((EXTRA - 12, table.shape[1]), F32)
    return jnp.concatenate([high, mid, low, rest], axis=0).astype(BF16)


def table_of(parts):
    parts = parts.astype(F32)
    return parts[0:4] + parts[4:8] + parts[8:12]


def copy_out(pairs, sem):
    copies = [pltpu.make_async_copy(src, dst, sem.at[i]) for i, (src, dst) in enumerate(pairs)]
    for copy in copies:
        copy.start()
    for copy in copies:
        copy.wait()


def query_kernel(
    x_ref, grad_ref, pat_ref, m0_hbm, m1_hbm, m2_hbm, keep_hbm, table_ref, out_s, parts_s, diag_s, sem
):
    placed_product(x_ref, grad_ref, out_s)
    for h in range(2):
        diag_s[...] = jnp.zeros_like(diag_s)
        for a in range(BAND // 8):
            off = BAND - 8 * a
            diag_s[:, off : off + TILE] += pat_ref[h, 8 * a : 8 * a + 8, :]
        total = jnp.zeros((1, 512), F32)
        for s in range(8):
            total += diag_s[s : s + 1, s : s + 512]
        far = jnp.sum(total[:, 256:], axis=1, keepdims=True)
        table_ref[h : h + 1, :] = total[:, :256]
        table_ref[2 + h : 3 + h, :] = jnp.broadcast_to(far, (1, 256))
    parts_s[...] = three_parts(table_ref[...])
    pairs = [(out_s.at[1536:], keep_hbm)]
    for i, m in enumerate((m0_hbm, m1_hbm, m2_hbm)):
        pairs += [(out_s.at[512 * i : 512 * (i + 1)], m.at[:512]), (parts_s, m.at[512:])]
    copy_out(pairs, sem)


def own_kernel(x_ref, grad_ref, out_ref):
    placed_product(x_ref, grad_ref, out_ref)


def other_kernel(x_ref, grad_ref, own_hbm, m0_hbm, m1_hbm, m2_hbm, keep_hbm, out_s, sem, sem2):
    pairs = []
    for i, m in enumerate((m0_hbm, m1_hbm, m2_hbm, keep_hbm)):
        rows = slice(512 * i, 512 * (i + 1))
        pairs.append(pltpu.make_async_copy(own_hbm.at[rows], m.at[:, :256], sem2.at[i]))
        pairs[-1].start()
    placed_product(x_ref, grad_ref, out_s)
    copy_out(
        [
            (out_s.at[512 * i : 512 * (i + 1)], m.at[:, 256:])
            for i, m in enumerate((m0_hbm, m1_hbm, m2_hbm, keep_hbm))
        ],
        sem,
    )
    for copy in pairs:
        copy.wait()


def summed(keep_ref, got_refs, rows):
    total = keep_ref[rows].astype(F32)
    for got in got_refs:
        total += got[rows].astype(F32)
    return total


def summed_table(table_in, got_refs, n):
    total = table_in[...]
    for got in got_refs:
        total += table_of(got[n:, :256])
    return total


def merge_kernel(
    keep_ref, a0, a1, a2, keep2_ref, b0, b1, b2, table_in, m0_ref, m1_ref, m2_ref, next_ref, table_ref
):
    total = summed_table(table_in, (a0, a1, a2), 512)
    table_ref[...] = total
    parts = three_parts(total)
    for i, out in enumerate((m0_ref, m1_ref, m2_ref, next_ref)):
        rows = slice(128 * i, 128 * (i + 1))
        out[:128, :256] = summed(keep_ref, (a0, a1, a2), rows).astype(BF16)
        out[:128, 256:] = summed(keep2_ref, (b0, b1, b2), rows).astype(BF16)
        if i < 3:
            out[128:, :256] = parts
            out[128:, 256:] = jnp.zeros((EXTRA, 512), BF16)


def split_kernel(keep_ref, g0, g1, g2, table_in, one_ref, two_ref, three_ref, own_ref, table_ref):
    n = own_ref.shape[0]
    total = summed_table(table_in, (g0, g1, g2), 2 * n)
    table_ref[...] = total
    far = summed(keep_ref, (g0, g1, g2), slice(0, n))
    one_ref[:n] = far[:, :512].astype(BF16)
    one_ref[n:, :256] = three_parts(total)
    one_ref[n:, 256:] = jnp.zeros((EXTRA, 256), BF16)
    two_ref[...] = far[:, 512:].astype(BF16)
    near = summed(keep_ref, (g0, g1, g2), slice(n, 2 * n))
    own_ref[...] = near[:, :512]
    three_ref[...] = near[:, 512:]


def output_kernel(own_ref, one_ref, two_ref, three_ref, table_in, q_ref, k_ref, v_ref, table_ref):
    core = lax.axis_index("core")
    n = own_ref.shape[0]
    table = table_in[...] + table_of(one_ref[n:, :256])
    table_ref[:, :256] = table[:2]
    table_ref[:, 256:] = table[2:, :1]
    own = own_ref[...] + one_ref[:n].astype(F32)
    got = three_ref[...] + two_ref[...].astype(F32)
    q_ref[...] = own[:, :256]

    @pl.when(core == 0)
    def _():
        k_ref[...] = own[:, 256:]
        v_ref[...] = got

    @pl.when(core == 1)
    def _():
        v_ref[...] = own[:, 256:]
        k_ref[...] = got


def sds(shape, dtype):
    return jax.ShapeDtypeStruct(shape, dtype)


def whole(shape):
    return pl.BlockSpec(shape, lambda *_: (0,) * len(shape))


def cost(flops, byte_count):
    return pl.CostEstimate(flops=flops, bytes_accessed=byte_count, transcendentals=0)


def params(limit=None):
    return pltpu.CompilerParams(dimension_semantics=("arbitrary",), vmem_limit_bytes=limit or VMEM_LIMIT)


def call(kernel, operands, outs, scratch=(), grid=(1,), flops=1 << 20, blocks=None, any_outs=(), any_ins=(), limit=None):
    specs = [pl.BlockSpec(memory_space=pltpu.HBM) if i in any_ins else whole(x.shape) for i, x in enumerate(operands)]
    for at, shape in (blocks or {}).items():
        specs[at] = whole(shape)
    out_specs = [pl.BlockSpec(memory_space=pl.ANY) if i in any_outs else whole(x.shape) for i, x in enumerate(outs)]
    moved = sum(x.size * x.dtype.itemsize for x in (*operands, *outs))
    return pl.pallas_call(
        kernel,
        grid=grid,
        in_specs=specs,
        out_specs=out_specs,
        out_shape=list(outs),
        scratch_shapes=list(scratch),
        compiler_params=params(limit),
        cost_estimate=cost(flops, moved),
    )(*operands)


def neighbour(block, distance):
    count = NZ * NX
    route = [(i, i + distance) for i in range(count) if 0 <= i + distance < count]
    return lax.ppermute(block, SP, route)


def staged(inputs, w_query, w_key, w_value, rel_table, out_grad):
    f32, b16 = (lambda *s: sds(s, F32)), (lambda *s: sds(s, BF16))
    v32, v16 = (lambda *s: pltpu.VMEM(s, F32)), (lambda *s: pltpu.VMEM(s, BF16))
    tile_flops = 6 * 2 * TILE * BAND * HDIM
    x_hbm, wq_hbm, wk_hbm, wv_hbm = (
        pltpu.with_memory_space_constraint(v, pltpu.HBM) for v in (inputs, w_query, w_key, w_value)
    )
    dma = pltpu.SemaphoreType.DMA
    tail, wk, wv, x_tail = call(
        load_kernel, (x_hbm, wk_hbm, wv_hbm),
        (b16(REACH, 512), b16(2048, 256), b16(2048, 256), b16(REACH, 2048)),
        (dma((5,)),), flops=2 * 256 * 2048 * 512, any_ins=(0, 1, 2),
    )
    halo = neighbour(tail, 1)
    query, key, value, x = call(
        proj_kernel, (x_hbm, wq_hbm, wk, wv, x_tail, tail),
        (b16(1024, 256),) * 3 + (b16(1024, 2048),), (v16(2048, 256), dma((4,))),
        flops=2 * 1024 * 2048 * 768, any_ins=(0, 1),
    )
    block = (REACH, 256)
    span = 1024 - LATE
    pattern = f32(2, BAND, TILE)
    dq_late, acc, bias, pat = call(
        late_kernel, (query, key, value, out_grad, rel_table),
        (b16(span - REACH, 256), f32(span, 512), pattern, pattern),
        (v16(256, span), v16(256, span), v32(span, 256), v32(span, 256)), flops=6 * tile_flops,
    )
    dq0, edge, back, pat = call(
        first_kernel, (query, key, value, halo, out_grad, bias, pat),
        (b16(REACH, 256), f32(REACH, 512), b16(REACH, 512), pattern),
        (v16(512, 256), v16(512, 256), v16(256, 512), v16(256, 512), v32(512, 256), v32(512, 256)),
        flops=4 * tile_flops, blocks={0: block, 1: block, 2: block, 4: block},
    )
    back = neighbour(back, -1)
    dq, kg, vg, edge, pat = call(
        attn_kernel, (query, key, value, out_grad, bias, pat, edge, acc, dq0, dq_late),
        (b16(1024, 256), b16(768, 256), b16(768, 256), f32(REACH, 512), pattern),
        (v16(256, LATE + REACH), v16(256, LATE + REACH), v32(LATE + REACH, 256), v32(LATE + REACH, 256)), flops=6 * tile_flops,
    )
    product = 2 * 1024 * 2048 * 256
    *send, keep, table = call(
        query_kernel, (x, dq, pat), (b16(512 + EXTRA, 256),) * 3 + (b16(512, 256), f32(4, 256)),
        (v16(2048, 256), v16(EXTRA, 256), v32(8, 640), dma((7,))), flops=product, any_outs=(0, 1, 2, 3),
    )
    a = exchange_quarters(send, 0)
    own, swap = call(finish_kernel, (kg, vg, edge, back), (b16(1024, 256),) * 2)
    got = core_swap(swap)
    (placed,) = call(own_kernel, (x, own), (b16(2048, 256),), flops=product)
    *send2, keep2 = call(
        other_kernel, (x, got, placed), (b16(512, 512),) * 4,
        (v16(2048, 256), dma((4,)), dma((4,))), flops=product, any_outs=(0, 1, 2, 3), any_ins=(2,),
    )
    b = exchange_quarters(send2, 0)
    dq, kg, vg = call(
        emit_kernel, (dq, own, swap), (b16(1024, 256),) * 3, (dma((3,)),),
        any_ins=(0, 1, 2), any_outs=(0, 1, 2),
    )
    *send, keep, table = call(
        merge_kernel, (keep, *a, keep2, *b, table),
        (b16(128 + EXTRA, 768),) * 3 + (b16(128, 768), f32(4, 256)),
    )
    c = exchange_quarters(send, 2)
    one, two, three, own, table = call(
        split_kernel, (keep, *c, table),
        (b16(64 + EXTRA, 512), b16(64, 256), f32(64, 256), f32(64, 512), f32(4, 256)),
    )
    one = exchange(one, (4,))
    two = exchange(two, (4,), across=1)
    three = core_swap(three)
    dwq, dwk, dwv, table = call(
        output_kernel, (own, one, two, three, table), (f32(64, 256),) * 3 + (f32(*rel_table.shape),)
    )
    return dq, kg, vg, dwq, dwk, dwv, table


def solution(mesh):
    torus = Mesh(mesh.devices.reshape(NZ, NX, -1, 2), SP + ("row", "core"))
    tp = ("row", "core")
    in_specs = (P(SP, None), P(None, tp), P(None, tp), P(None, tp), P(tp, None), P(SP, tp))
    out_specs = (P(SP, tp),) * 6 + (P(tp, None),)
    return jax.shard_map(staged, mesh=torus, in_specs=in_specs, out_specs=out_specs, check_vma=False)
```
